256 devices in a mesh: sp: 32 (over z, y), tp: 8 (over x, core).
Axes of the slice: x: 4, y: 4, z: 8, core: 2. Of those that a mesh axis runs over, the one named last changes fastest.
Arguments:
- grouped_head_inputs: bfloat16 [32768, 2, 1024], P('sp', None, 'tp'), may hold values from -6 to 6
- head_gate_inputs: bfloat16 [32768, 2, 1024], P('sp', None, 'tp'), may hold values from -6 to 6
- unsmoothed_step: float32 [32768, 2, 16], P('sp', None, 'tp'), may hold values from -3.8 to 3.8
- head_decay_rate: float32 [2, 16], P(None, 'tp'), may hold values from 3.0517578e-06 to 0.04761905
- extra_log_decay: float32 [32768, 2, 16], P('sp', None, 'tp'), may hold values from -1.4 to 0
- first_group_keys: bfloat16 [32768, 128], P('sp'), may hold values from -6 to 6
- first_group_queries: bfloat16 [32768, 128], P('sp'), may hold values from -6 to 6
- second_group_keys: bfloat16 [32768, 64], P('sp'), may hold values from -6 to 6
- second_group_queries: bfloat16 [32768, 64], P('sp'), may hold values from -6 to 6
- head_input_filter: float32 [4, 2, 1024], P(None, None, 'tp'), may hold values from -3 to 3
- first_group_filter: float32 [4, 2, 128], replicated, may hold values from -3 to 3
- second_group_filter: float32 [4, 2, 64], replicated, may hold values from -3 to 3
- head_norm_gain: float32 [2, 1024], P(None, 'tp'), may hold values from 0.1 to 1.9
- output_weight: bfloat16 [2, 1024, 2048], P(None, None, 'tp'), may hold values from -0.125 to 0.125
- residual: bfloat16 [32768, 2048], P('sp', 'tp'), may hold values from -37 to 37
- channel_norm_gain: float32 [2048], replicated, may hold values from 0.1 to 1.9
- channel_gate_weight: bfloat16 [2048, 5120], P('sp', 'tp'), may hold values from -0.125 to 0.125
- channel_up_weight: bfloat16 [2048, 5120], P('sp', 'tp'), may hold values from -0.125 to 0.125
- channel_down_weight: bfloat16 [2048, 5120], P('sp', 'tp'), may hold values from -0.078125 to 0.078125
Outputs:
- layer_output: bfloat16 [32768, 2048], P('sp', 'tp')
The draws below stay inside these ranges and needn't reach their ends.
All inputs are finite; a program needn't handle non-finite values.
Results may differ from the reference program's by a relative error of at most 0.007.
Values may be sent and summed in bfloat16 or wider, within the bound.
A program may use at most 128 MiB of HBM per device.

```python
import math
import jax
import jax.numpy as jnp
from jax import lax

D = 2048
GROUP_HEADS = 16
HEAD = 64
STATE_ONE = 128
STATE_TWO = 64
FF = 5120
CONV = 4
BLOCK = 128
TOKENS = 32768
CHANNELS = 1024
N_TP = 8


def draw_unsmoothed_step(key, part):
    noise_key = jax.random.fold_in(key, 11)
    block_key = jax.random.fold_in(key, 12)
    block_total = TOKENS // BLOCK
    offsets = jax.random.uniform(block_key, (block_total, 1, 1, 1), jnp.float32, -1.0, 1.0)
    noise = 0.7 * jax.random.truncated_normal(noise_key, -4.0, 4.0, (block_total, BLOCK, 2, GROUP_HEADS), jnp.float32)
    return (noise + offsets).reshape(TOKENS, 2, GROUP_HEADS)


def draw_head_decay_rate(key, part):
    choose_key = jax.random.fold_in(key, 21)
    fast_key = jax.random.fold_in(key, 22)
    slow_key = jax.random.fold_in(key, 23)
    share = 0.5
    quick = jax.random.uniform(choose_key, (2, GROUP_HEADS), jnp.float32) < share
    fast = jnp.exp(jax.random.uniform(fast_key, (2, GROUP_HEADS), jnp.float32, math.log(1.0 / 70.0), math.log(1.0 / 21.0)))
    slow = jnp.exp(jax.random.uniform(slow_key, (2, GROUP_HEADS), jnp.float32, math.log(0.1), math.log(0.6))) / TOKENS
    return jnp.where(quick, fast, slow)


def draw_extra_log_decay(key, part):
    place_key = jax.random.fold_in(key, 31)
    loss_key = jax.random.fold_in(key, 32)
    places = jax.random.randint(place_key, (2, 2, GROUP_HEADS), 0, TOKENS)
    losses = jax.random.uniform(loss_key, (2, 2, GROUP_HEADS), jnp.float32, 0.2, 0.5)
    positions = jnp.arange(TOKENS, dtype=jnp.int32)[:, None, None, None]
    struck = positions == places[None]
    return jnp.sum(jnp.where(struck, jnp.log(1.0 - losses)[None], 0.0), axis=1)


def draw_residual(key, part):
    row_key = jax.random.fold_in(key, 41)
    column_key = jax.random.fold_in(key, 42)
    noise_key = jax.random.fold_in(key, 43)
    row_scale = jnp.exp(jax.random.uniform(row_key, (TOKENS, 1), jnp.float32, math.log(0.3), math.log(3.0)))
    column_scale = jnp.exp(jax.random.uniform(column_key, (1, D), jnp.float32, math.log(0.3), math.log(3.0)))
    noise = jax.random.truncated_normal(noise_key, -4.0, 4.0, (TOKENS, D), jnp.float32)
    return (noise * row_scale * column_scale).astype(jnp.bfloat16)


def level_of(own_key, dims, cuts, least, high):
    def one(axis_at, parts):
        heights = jax.random.uniform(jax.random.fold_in(jax.random.fold_in(own_key, 6), axis_at), (parts,), jnp.float32, least / len(cuts), high / len(cuts))
        return jnp.repeat(jnp.exp(heights), dims[axis_at] // parts).reshape((-1,) + (1,) * (len(dims) - axis_at - 1))

    gain = one(*cuts[0])
    for cut in cuts[1:]:
        gain = gain * one(*cut)
    return gain


def normal_values(own_key, dims, width, bound, cuts=(), kind=jnp.bfloat16):
    level = level_of(own_key, dims, cuts, -0.22, 0.18) if cuts else 1.0
    entries = jax.random.normal(own_key, dims, jnp.float32) * width * level
    return jnp.minimum(jnp.maximum(entries, -bound), bound).astype(kind)


def setup_inputs(seed: int = 0) -> dict:
    key_list = jax.random.split(jax.random.key(seed), 20)
    grouped_head_inputs = normal_values(key_list[0], (TOKENS, 2, CHANNELS), 1.0, 6.0, ((0, 32), (2, 8)))
    head_gate_inputs = normal_values(key_list[1], (TOKENS, 2, CHANNELS), 1.0, 6.0, ((0, 32), (2, 8)))
    unsmoothed_step = draw_unsmoothed_step(jax.random.fold_in(key_list[19], 71), 0)
    head_decay_rate = draw_head_decay_rate(jax.random.fold_in(key_list[19], 71), 0)
    extra_log_decay = draw_extra_log_decay(jax.random.fold_in(key_list[19], 71), 0)
    first_group_keys = normal_values(key_list[5], (TOKENS, STATE_ONE), 1.0, 6.0, ((0, 32),))
    first_group_queries = normal_values(key_list[6], (TOKENS, STATE_ONE), 1.0, 6.0, ((0, 32),))
    second_group_keys = normal_values(key_list[7], (TOKENS, STATE_TWO), 1.0, 6.0, ((0, 32),))
    second_group_queries = normal_values(key_list[8], (TOKENS, STATE_TWO), 1.0, 6.0, ((0, 32),))
    head_input_filter = normal_values(key_list[9], (CONV, 2, CHANNELS), 0.5, 3.0, ((2, 8),), jnp.float32)
    first_group_filter = normal_values(key_list[10], (CONV, 2, STATE_ONE), 0.5, 3.0, (), jnp.float32)
    second_group_filter = normal_values(key_list[11], (CONV, 2, STATE_TWO), 0.5, 3.0, (), jnp.float32)
    head_norm_gain = jnp.clip(1.0 + 0.18 * jax.random.normal(key_list[12], (2, CHANNELS), jnp.float32), 0.1, 1.9)
    output_weight = normal_values(key_list[13], (2, CHANNELS, D), (2 * CHANNELS) ** -0.5, 0.125, ((2, 8),))
    residual = draw_residual(jax.random.fold_in(key_list[19], 71), 0)
    channel_norm_gain = jnp.clip(1.0 + 0.18 * jax.random.normal(key_list[15], (D,), jnp.float32), 0.1, 1.9)
    channel_gate_weight = normal_values(key_list[16], (D, FF), D ** -0.5, 0.125, ((0, 32), (1, 8)))
    channel_up_weight = normal_values(key_list[17], (D, FF), D ** -0.5, 0.125, ((0, 32), (1, 8)))
    channel_down_weight = normal_values(key_list[18], (D, FF), FF ** -0.5, 0.078125, ((0, 32), (1, 8)))
    return dict(grouped_head_inputs=grouped_head_inputs, head_gate_inputs=head_gate_inputs, unsmoothed_step=unsmoothed_step, head_decay_rate=head_decay_rate, extra_log_decay=extra_log_decay, first_group_keys=first_group_keys, first_group_queries=first_group_queries, second_group_keys=second_group_keys, second_group_queries=second_group_queries, head_input_filter=head_input_filter, first_group_filter=first_group_filter, second_group_filter=second_group_filter, head_norm_gain=head_norm_gain, output_weight=output_weight, residual=residual, channel_norm_gain=channel_norm_gain, channel_gate_weight=channel_gate_weight, channel_up_weight=channel_up_weight, channel_down_weight=channel_down_weight)


EPSILON = 1e-06
PRECISE = lax.Precision.HIGHEST

def causal_taps(values, taps):
    length = values.shape[0]
    zeros_rows = jnp.zeros((CONV - 1,) + values.shape[1:], jnp.float32)
    padded = jnp.concatenate([zeros_rows, values.astype(jnp.float32)], axis=0)
    running = jnp.zeros(values.shape, jnp.float32)
    for offset in range(CONV):
        running = running + taps[offset].astype(jnp.float32) * padded[offset:offset + length]
    return jax.nn.silu(running)

def block_pass(current, value_rows, log_rows, key_rows, query_rows):
    cumulative = jnp.cumsum(log_rows, axis=0)
    length = value_rows.shape[0]
    causal = jnp.arange(length)[:, None] >= jnp.arange(length)[None, :]
    scores = jnp.dot(query_rows, key_rows.T, precision=PRECISE)
    span_logs = jnp.where(causal[:, :, None], cumulative[:, None, :] - cumulative[None, :, :], -jnp.inf)
    weights = jnp.exp(span_logs) * scores[:, :, None]
    inside = jnp.einsum('lsh,shp->lhp', weights, value_rows, precision=PRECISE)
    carried = jnp.einsum('ls,hps->lhp', query_rows, current, precision=PRECISE) * jnp.exp(cumulative)[:, :, None]
    to_end = jnp.exp(cumulative[-1][None, :] - cumulative)
    update = jnp.einsum('lhp,ls->hps', value_rows * to_end[:, :, None], key_rows, precision=PRECISE)
    new_state = current * jnp.exp(cumulative[-1])[:, None, None] + update
    return (new_state, inside + carried)

def scan_group(value_rows, log_rows, key_rows, query_rows):
    length, head_count, head_width = value_rows.shape
    block_count = length // BLOCK
    initial = jnp.zeros((head_count, head_width, key_rows.shape[1]), jnp.float32)
    blocks = (value_rows.reshape(block_count, BLOCK, head_count, head_width), log_rows.reshape(block_count, BLOCK, head_count), key_rows.reshape(block_count, BLOCK, -1), query_rows.reshape(block_count, BLOCK, -1))

    def advance(current, pieces):
        return block_pass(current, pieces[0], pieces[1], pieces[2], pieces[3])
    final_state, outputs = lax.scan(advance, initial, blocks)
    return outputs.reshape(length, head_count, head_width)

def reference(grouped_head_inputs, head_gate_inputs, unsmoothed_step, head_decay_rate, extra_log_decay, first_group_keys, first_group_queries, second_group_keys, second_group_queries, head_input_filter, first_group_filter, second_group_filter, head_norm_gain, output_weight, residual, channel_norm_gain, channel_gate_weight, channel_up_weight, channel_down_weight):
    length = grouped_head_inputs.shape[0]
    conv_heads = causal_taps(grouped_head_inputs, head_input_filter)
    keys_one = causal_taps(first_group_keys, first_group_filter[:, 0])
    queries_one = causal_taps(first_group_queries, first_group_filter[:, 1])
    keys_two = causal_taps(second_group_keys, second_group_filter[:, 0])
    queries_two = causal_taps(second_group_queries, second_group_filter[:, 1])
    head_step_size = jax.nn.softplus(unsmoothed_step.astype(jnp.float32))
    decay_logarithm = extra_log_decay.astype(jnp.float32) - head_step_size * head_decay_rate.astype(jnp.float32)[None]
    values = conv_heads.reshape(length, 2, GROUP_HEADS, HEAD) * head_step_size[:, :, :, None]
    first = scan_group(values[:, 0], decay_logarithm[:, 0], keys_one, queries_one)
    second = scan_group(values[:, 1], decay_logarithm[:, 1], keys_two, queries_two)
    mixer = jnp.stack([first, second], axis=1)
    gated = mixer * jax.nn.silu(head_gate_inputs.astype(jnp.float32)).reshape(length, 2, GROUP_HEADS, HEAD)
    scaled = gated * lax.rsqrt(lax.optimization_barrier(jnp.mean(gated * gated, axis=3, keepdims=True)) + EPSILON)
    mixed = (scaled.reshape(length, 2, CHANNELS) * head_norm_gain.astype(jnp.float32)[None]).astype(jnp.bfloat16)
    projected = jnp.dot(mixed.reshape(length, 2 * CHANNELS), output_weight.reshape(2 * CHANNELS, D), preferred_element_type=jnp.float32)
    stream = (residual.astype(jnp.float32) + projected).astype(jnp.bfloat16)
    stream_wide = stream.astype(jnp.float32)
    normed = (stream_wide * lax.rsqrt(lax.optimization_barrier(jnp.mean(stream_wide * stream_wide, axis=1, keepdims=True)) + EPSILON) * channel_norm_gain.astype(jnp.float32)[None]).astype(jnp.bfloat16)
    gate = jnp.dot(normed, channel_gate_weight, preferred_element_type=jnp.float32)
    upward = jnp.dot(normed, channel_up_weight, preferred_element_type=jnp.float32)
    hidden = (jax.nn.silu(gate) * upward).astype(jnp.bfloat16)
    block_width = FF // N_TP
    summed = jnp.zeros((length, D), jnp.float32)
    for index in range(N_TP):
        piece = hidden[:, index * block_width:(index + 1) * block_width]
        columns = channel_down_weight[:, index * block_width:(index + 1) * block_width]
        partial_value = lax.dot_general(piece, columns, (((1,), (1,)), ((), ())), preferred_element_type=jnp.float32)
        rounded = lax.optimization_barrier(partial_value.astype(jnp.bfloat16))
        summed = summed + rounded.astype(jnp.float32)
    return (stream_wide + 0.5 * summed).astype(jnp.bfloat16)
```

```python
import functools

import jax
import jax.numpy as jnp
from jax import lax
from jax.experimental import pallas as pl
from jax.experimental.pallas import tpu as pltpu
from jax.sharding import PartitionSpec as P

HEAD = 64
CONV = 4
BLOCK = 128
EPSILON = 1e-06
MESH = pl.DeviceIdType.MESH
F32 = jnp.float32
BF16 = jnp.bfloat16
NY = 4
NZ = 8
QROWS = 48
MROWS = 64


def silu(v):
    return v * (1.0 / (1.0 + jnp.exp(-v)))


def halves(lane_low, a, b):
    return jnp.where(lane_low, a, b)


def dot(a, b, ca, cb):
    return lax.dot_general(a, b, (((ca,), (cb,)), ((), ())), preferred_element_type=F32)


def split_three(v):
    hi = v.astype(BF16)
    rest = v - hi.astype(F32)
    mid = rest.astype(BF16)
    low = (rest - mid.astype(F32)).astype(BF16)
    return hi.astype(F32), mid.astype(F32), low.astype(F32)


def log_rows(l0, l1):
    rows = []
    for part0, part1 in zip(split_three(l0), split_three(l1)):
        rows += [part0, part1]
    rows.append(jnp.zeros((10, 128), F32))
    return jnp.concatenate(rows, axis=0).astype(BF16)


def read_logs(rows):
    v = rows.astype(F32)
    return v[0:1] + v[2:3] + v[4:5], v[1:2] + v[3:4] + v[5:6]


def front_kernel(
    xs, gs, k1, q1, kq2, table, head_taps, taps1, taps2, gain,
    mixed,
    rim, keys, queries, values, local, cols, erun, state, starts,
    msg1, buf1, msg2, buf2, msg3, enter,
    rim_send, rim_recv, send1, recv1, send2, recv2, send3, recv3,
):
    sp = lax.axis_index("sp")
    y = lax.rem(sp, NY)
    z = sp // NY
    n_sp = NY * NZ
    blocks = xs.shape[1] // BLOCK
    right = lax.rem(sp + 1, n_sp)
    left = lax.rem(sp + n_sp - 1, n_sp)
    y_peers = [z * NY + lax.rem(y + j, NY) for j in range(1, NY)]
    z_peers = [lax.rem(z + j, NZ) * NY + y for j in range(1, NZ)]

    barrier = pltpu.get_barrier_semaphore()
    for peer in [right, left] + y_peers + z_peers:
        pl.semaphore_signal(barrier, inc=1, device_id={"sp": peer}, device_id_type=MESH)
    pl.semaphore_wait(barrier, 2 + (NY - 1) + (NZ - 1))

    tail = pl.ds(xs.shape[1] - 16, 16)
    rim_copies = []
    for n, src in enumerate([xs.at[0, tail], xs.at[1, tail], k1.at[tail], q1.at[tail], kq2.at[tail]]):
        copy = pltpu.make_async_remote_copy(
            src_ref=src, dst_ref=rim.at[n], send_sem=rim_send.at[n], recv_sem=rim_recv.at[n],
            device_id={"sp": right}, device_id_type=MESH)
        copy.start()
        rim_copies.append(copy)

    lane = lax.broadcasted_iota(jnp.int32, (8, 128), 1)
    row8 = lax.broadcasted_iota(jnp.int32, (8, 128), 0)
    low = lax.broadcasted_iota(jnp.int32, (BLOCK, 128), 1) < HEAD
    low1 = lax.broadcasted_iota(jnp.int32, (1, 128), 1) < HEAD
    causal = lax.broadcasted_iota(jnp.int32, (BLOCK, BLOCK), 0) >= lax.broadcasted_iota(
        jnp.int32, (BLOCK, BLOCK), 1)

    state[...] = jnp.zeros_like(state)
    for copy in rim_copies:
        copy.wait()
    has_left = sp > 0
    tails = tuple(
        jnp.where(has_left, rim[n].astype(F32)[8:16], 0.0) for n in range(5))

    def conv(block, before, taps):
        full = jnp.concatenate([before, block], axis=0)
        total = taps[0] * full[5 : 5 + BLOCK]
        for k in range(1, CONV):
            total = total + taps[k] * full[5 + k : 5 + k + BLOCK]
        return silu(total)

    def first(b, carry):
        before, offs = carry[:5], carry[5]
        at = pl.ds(pl.multiple_of(b * BLOCK, BLOCK), BLOCK)
        r = table[b]
        c = r
        for s in (1, 2, 4, 8, 16, 32, 64):
            c = c + jnp.where(lane >= s, pltpu.roll(c, s, 1), 0.0)
        t = jnp.where(row8 < 4, c, r).T
        cols[b] = t
        erun[b] = jnp.exp(jnp.where(row8 < 4, c + offs, 0.0)).T
        raw = [xs[0, at].astype(F32), xs[1, at].astype(F32), k1[at].astype(F32),
               q1[at].astype(F32), kq2[at].astype(F32)]
        key_one = conv(raw[2], before[2], [taps1[k, 0:1] for k in range(CONV)])
        query_one = conv(raw[3], before[3], [taps1[k, 1:2] for k in range(CONV)])
        both = conv(raw[4], before[4], [taps2[k : k + 1] for k in range(CONV)])
        key_two = jnp.where(low, both, 0.0)
        query_two = jnp.where(low, pltpu.roll(both, 64, 1), 0.0)
        for g, (key, query) in enumerate([(key_one, query_one), (key_two, query_two)]):
            u = conv(raw[g], before[g], [head_taps[k, g : g + 1] for k in range(CONV)])
            h = 2 * g
            v = u * halves(low, t[:, 4 + h : 5 + h], t[:, 5 + h : 6 + h])
            cum = halves(low, t[:, h : h + 1], t[:, h + 1 : h + 2])
            total = halves(low1, c[h : h + 1, 127:128], c[h + 1 : h + 2, 127:128])
            to_end = jnp.exp(total - cum)
            kb = key.astype(BF16)
            keys[g, at] = kb
            queries[g, at] = query.astype(BF16)
            values[g, at] = v.astype(BF16)
            old = state[g]
            starts[g, b] = old.astype(BF16)
            state[g] = old * jnp.exp(total) + dot(kb, (v * to_end).astype(BF16), 0, 0)
        offs = offs + jnp.broadcast_to(c[:, 127:128], (8, 128))
        return tuple(v[BLOCK - 8 :] for v in raw) + (offs,)

    carry = lax.fori_loop(0, blocks, first, tails + (jnp.zeros((8, 128), F32),))
    offs = carry[5]
    log0 = halves(low1, offs[0:1], offs[1:2])
    log1 = halves(low1, offs[2:3], offs[3:4])

    logs = log_rows(log0, log1)
    full_state = jnp.concatenate([state[0], state[1][0:64]], axis=0).astype(BF16)
    for q in range(NY):
        msg1[q, 0:QROWS] = full_state[q * QROWS : (q + 1) * QROWS]
        msg1[q, QROWS:MROWS] = logs
    copies1 = []
    for j in range(1, NY):
        to = lax.rem(y + j, NY)
        copy = pltpu.make_async_remote_copy(
            src_ref=msg1.at[to], dst_ref=buf1.at[y], send_sem=send1.at[j - 1],
            recv_sem=recv1.at[j - 1], device_id={"sp": z * NY + to}, device_id_type=MESH)
        copy.start()
        copies1.append(copy)
    buf1[y] = msg1[y]

    def inside(b, carry):
        at = pl.ds(pl.multiple_of(b * BLOCK, BLOCK), BLOCK)
        t = cols[b]
        crow = t.T
        for g in range(2):
            h = 2 * g
            qb, kb, v = queries[g, at], keys[g, at], values[g, at]
            scores = dot(qb, kb, 1, 1)
            weights = []
            for j in range(2):
                span = t[:, h + j : h + j + 1] - crow[h + j : h + j + 1]
                weights.append((jnp.exp(jnp.where(causal, span, -jnp.inf)) * scores).astype(BF16))
            zero = jnp.zeros_like(v)
            two = jnp.concatenate([jnp.where(low, v, zero), jnp.where(low, zero, v)], axis=0)
            out = dot(jnp.concatenate(weights, axis=1), two, 1, 0)
            cum = halves(low, t[:, h : h + 1], t[:, h + 1 : h + 2])
            local[g, at] = out + dot(qb, starts[g, b], 1, 0) * jnp.exp(cum)
        return carry

    lax.fori_loop(0, blocks // 2, inside, 0)

    for copy in copies1:
        copy.wait()
    rows = y * QROWS + lax.broadcasted_iota(jnp.int32, (QROWS, 128), 0)
    group_one = rows < 128

    def factor(f0, f1):
        return jnp.where(group_one, f0, f1)

    prefix, befores = [], []
    run = jnp.zeros((QROWS, 128), F32)
    sum0 = jnp.zeros((1, 128), F32)
    sum1 = jnp.zeros((1, 128), F32)
    for j in range(NY):
        prefix.append(run)
        befores.append((sum0, sum1))
        l0, l1 = read_logs(buf1[j, QROWS:MROWS])
        run = run * factor(jnp.exp(l0), jnp.exp(l1)) + buf1[j, 0:QROWS].astype(F32)
        sum0, sum1 = sum0 + l0, sum1 + l1
    msg2[0:QROWS] = run.astype(BF16)
    msg2[QROWS:MROWS] = log_rows(sum0, sum1)
    copies2 = []
    for j in range(1, NZ):
        copy = pltpu.make_async_remote_copy(
            src_ref=msg2, dst_ref=buf2.at[z], send_sem=send2.at[j - 1],
            recv_sem=recv2.at[j - 1], device_id={"sp": lax.rem(z + j, NZ) * NY + y},
            device_id_type=MESH)
        copy.start()
        copies2.append(copy)
    buf2[z] = msg2[...]

    lax.fori_loop(blocks // 2, blocks, inside, 0)

    for copy in copies2:
        copy.wait()
    run = jnp.zeros((QROWS, 128), F32)
    for j in range(NZ):
        l0, l1 = read_logs(buf2[j, QROWS:MROWS])
        new = run * factor(jnp.exp(l0), jnp.exp(l1)) + buf2[j, 0:QROWS].astype(F32)
        run = jnp.where(j < z, new, run)
    for j in range(NY):
        l0, l1 = befores[j]
        msg3[j] = (run * factor(jnp.exp(l0), jnp.exp(l1)) + prefix[j]).astype(BF16)
    mine = pl.ds(pl.multiple_of(y * QROWS, 16), QROWS)
    copies3 = []
    for j in range(1, NY):
        to = lax.rem(y + j, NY)
        copy = pltpu.make_async_remote_copy(
            src_ref=msg3.at[to], dst_ref=enter.at[mine], send_sem=send3.at[j - 1],
            recv_sem=recv3.at[j - 1], device_id={"sp": z * NY + to}, device_id_type=MESH)
        copy.start()
        copies3.append(copy)
    enter[mine] = msg3[y]
    for copy in copies3:
        copy.wait()

    enter_one = enter[0:128]
    enter_two = jnp.concatenate([enter[128:192], jnp.zeros((64, 128), BF16)], axis=0)

    def finish(b, carry):
        at = pl.ds(pl.multiple_of(b * BLOCK, BLOCK), BLOCK)
        e = erun[b]
        for g, entering in enumerate([enter_one, enter_two]):
            h = 2 * g
            m = local[g, at] + dot(queries[g, at], entering, 1, 0) * halves(
                low, e[:, h : h + 1], e[:, h + 1 : h + 2])
            m = m * silu(gs[g, at].astype(F32))
            square = m * m
            s0 = jnp.sum(jnp.where(low, square, 0.0), axis=1, keepdims=True)
            s1 = jnp.sum(jnp.where(low, 0.0, square), axis=1, keepdims=True)
            scale = lax.rsqrt(halves(low, s0, s1) * (1.0 / HEAD) + EPSILON)
            mixed[g, at] = (m * scale * gain[g : g + 1]).astype(BF16)
        return carry

    lax.fori_loop(0, blocks, finish, 0)


def front(xs, gs, k1, q1, kq2, table, head_taps, taps1, taps2, gain):
    length = xs.shape[1]
    blocks = length // BLOCK
    vmem = pl.BlockSpec(memory_space=pltpu.VMEM)
    dma = pltpu.SemaphoreType.DMA
    return pl.pallas_call(
        front_kernel,
        out_shape=jax.ShapeDtypeStruct((2, length, 128), BF16),
        in_specs=[vmem] * 10,
        out_specs=vmem,
        scratch_shapes=[
            pltpu.VMEM((5, 16, 128), BF16),
            pltpu.VMEM((2, length, 128), BF16),
            pltpu.VMEM((2, length, 128), BF16),
            pltpu.VMEM((2, length, 128), BF16),
            pltpu.VMEM((2, length, 128), F32),
            pltpu.VMEM((blocks, BLOCK, 8), F32),
            pltpu.VMEM((blocks, BLOCK, 8), F32),
            pltpu.VMEM((2, 128, 128), F32),
            pltpu.VMEM((2, blocks, 128, 128), BF16),
            pltpu.VMEM((NY, MROWS, 128), BF16),
            pltpu.VMEM((NY, MROWS, 128), BF16),
            pltpu.VMEM((MROWS, 128), BF16),
            pltpu.VMEM((NZ, MROWS, 128), BF16),
            pltpu.VMEM((NY, QROWS, 128), BF16),
            pltpu.VMEM((NY * QROWS, 128), BF16),
            dma((5,)), dma((5,)),
            dma((NY - 1,)), dma((NY - 1,)),
            dma((NZ - 1,)), dma((NZ - 1,)),
            dma((NY - 1,)), dma((NY - 1,)),
        ],
        compiler_params=pltpu.CompilerParams(
            collective_id=0, has_side_effects=True, vmem_limit_bytes=24 * 1024 * 1024),
        cost_estimate=pl.CostEstimate(
            flops=4_000_000_000, bytes_accessed=4_000_000, transcendentals=4_000_000),
        name="front",
    )(xs, gs, k1, q1, kq2, table, head_taps, taps1, taps2, gain)


def shards(
    grouped_head_inputs,
    head_gate_inputs,
    unsmoothed_step,
    head_decay_rate,
    extra_log_decay,
    first_group_keys,
    first_group_queries,
    second_group_keys,
    second_group_queries,
    head_input_filter,
    first_group_filter,
    second_group_filter,
    head_norm_gain,
    output_weight,
    residual,
    channel_norm_gain,
    channel_gate_weight,
    channel_up_weight,
    channel_down_weight,
):
    length = grouped_head_inputs.shape[0]
    blocks = length // BLOCK
    step = jax.nn.softplus(unsmoothed_step)
    log_decay = extra_log_decay - step * head_decay_rate[None]
    table = jnp.stack([log_decay, step]).reshape(2, blocks, BLOCK, 4)
    table = table.transpose(1, 0, 3, 2).reshape(blocks, 8, BLOCK)
    mixed = front(
        grouped_head_inputs.transpose(1, 0, 2),
        head_gate_inputs.transpose(1, 0, 2),
        first_group_keys,
        first_group_queries,
        jnp.concatenate([second_group_keys, second_group_queries], axis=1),
        table,
        head_input_filter,
        first_group_filter,
        second_group_filter.reshape(CONV, 128),
        head_norm_gain,
    )
    whole = lax.all_gather(mixed, "tp", axis=0)
    projected = lax.dot_general(
        whole,
        output_weight.reshape(2, 8, 128, output_weight.shape[2]),
        (((0, 1, 3), (1, 0, 2)), ((), ())),
        preferred_element_type=F32,
    )
    stream = (residual.astype(F32) + projected).astype(BF16)
    full_rows = lax.all_gather(stream, "tp", axis=1, tiled=True).astype(F32)
    normed = (
        full_rows
        * lax.rsqrt(jnp.mean(full_rows * full_rows, axis=1, keepdims=True) + EPSILON)
        * channel_norm_gain[None]
    ).astype(BF16)
    width = channel_gate_weight.shape[1]
    weights = lax.all_gather(
        jnp.concatenate([channel_gate_weight, channel_up_weight, channel_down_weight], axis=1),
        "sp", axis=0, tiled=True)
    gate = jnp.dot(normed, weights[:, :width], preferred_element_type=F32)
    upward = jnp.dot(normed, weights[:, width : 2 * width], preferred_element_type=F32)
    hidden = (jax.nn.silu(gate) * upward).astype(BF16)
    partial = dot(weights[:, 2 * width :], hidden, 1, 1).astype(BF16)
    summed = lax.psum_scatter(partial, "tp", scatter_dimension=0, tiled=True).astype(F32).T
    return (stream.astype(F32) + 0.5 * summed).astype(BF16)


def solution(mesh):
    return jax.shard_map(
        shards,
        mesh=mesh,
        in_specs=(
            P("sp", None, "tp"),
            P("sp", None, "tp"),
            P("sp", None, "tp"),
            P(None, "tp"),
            P("sp", None, "tp"),
            P("sp", None),
            P("sp", None),
            P("sp", None),
            P("sp", None),
            P(None, None, "tp"),
            P(),
            P(),
            P(None, "tp"),
            P(None, None, "tp"),
            P("sp", "tp"),
            P(),
            P("sp", "tp"),
            P("sp", "tp"),
            P("sp", "tp"),
        ),
        out_specs=P("sp", "tp"),
        check_vma=False,
    )
```

```python
import functools

import jax
import jax.numpy as jnp
from jax import lax
from jax.experimental import pallas as pl
from jax.experimental.pallas import tpu as pltpu
from jax.sharding import PartitionSpec as P

HEAD = 64
CONV = 4
BLOCK = 128
EPSILON = 1e-06
MESH = pl.DeviceIdType.MESH
F32 = jnp.float32
BF16 = jnp.bfloat16
NY = 4
NZ = 8
QROWS = 48
MROWS = 64
NX = 4
NTP = 8
CHUNKS = 2
N_PUT = 160


def silu(v):
    return v * (1.0 / (1.0 + jnp.exp(-v)))


def halves(lane_low, a, b):
    return jnp.where(lane_low, a, b)


def dot(a, b, ca, cb):
    return lax.dot_general(a, b, (((ca,), (cb,)), ((), ())), preferred_element_type=F32)


def split_three(v):
    hi = v.astype(BF16)
    rest = v - hi.astype(F32)
    mid = rest.astype(BF16)
    low = (rest - mid.astype(F32)).astype(BF16)
    return hi.astype(F32), mid.astype(F32), low.astype(F32)


def log_rows(l0, l1):
    rows = []
    for part0, part1 in zip(split_three(l0), split_three(l1)):
        rows += [part0, part1]
    rows.append(jnp.zeros((10, 128), F32))
    return jnp.concatenate(rows, axis=0).astype(BF16)


def read_logs(rows):
    v = rows.astype(F32)
    return v[0:1] + v[2:3] + v[4:5], v[1:2] + v[3:4] + v[5:6]


class Net:
    def __init__(self, send, recv):
        self.send, self.recv, self.count, self.sent = send, recv, 0, []

    def make(self, src, dst, to, index):
        return pltpu.make_async_remote_copy(
            src_ref=src, dst_ref=dst, send_sem=self.send.at[index], recv_sem=self.recv.at[index],
            device_id=to, device_id_type=MESH)

    def put(self, src, dst, to):
        copy = self.make(src, dst, to, self.count)
        self.count += 1
        copy.start()
        self.sent.append(copy)
        return copy

    def reserve(self, n):
        at = self.count
        self.count += n
        return at


def layer_kernel(
    xs, gs, k1, q1, kq2, table, head_taps, taps1, taps2, gain, channel_gain,
    out_w, resid, gate_w, up_w, down_w,
    out,
    rim, keys, queries, values, local, cols, erun, state, starts,
    msg1, buf1, msg2, buf2, msg3, enter,
    gu, dn, wo, res, mix_send, mix, stm, feat, nb, hidden, ps, pr, po, relay_l, relay_r,
    qs, from_l, from_r,
    local_sem, send_sem, recv_sem,
):
    sp = lax.axis_index("sp")
    tp = lax.axis_index("tp")
    y = lax.rem(sp, NY)
    z = sp // NY
    core = lax.rem(tp, 2)
    x = tp // 2
    n_sp = NY * NZ
    blocks = xs.shape[1] // BLOCK
    width = gate_w.shape[1]
    right = lax.rem(sp + 1, n_sp)
    left = lax.rem(sp + n_sp - 1, n_sp)

    def zmod(v):
        return lax.rem(v + NZ, NZ)

    def ymod(v):
        return lax.rem(v + NY, NY)

    y_peers = [{"sp": z * NY + ymod(y + j)} for j in range(1, NY)]
    z_peers = [{"sp": zmod(z + j) * NY + y} for j in range(1, NZ)]
    tp_peers = [{"tp": lax.rem(tp + j, NTP)} for j in range(1, NTP)]
    up_y, down_y = {"sp": z * NY + ymod(y + 1)}, {"sp": z * NY + ymod(y - 1)}
    up_z, down_z = {"sp": zmod(z + 1) * NY + y}, {"sp": zmod(z - 1) * NY + y}
    slot_l = lax.rem(x + NX - 1, NX) * 2 + core
    slot_r = lax.rem(x + 1, NX) * 2 + core
    slot_o = lax.rem(x + 2, NX) * 2 + core
    partner_slot = x * 2 + 1 - core
    partner, x_right, x_left = {"tp": partner_slot}, {"tp": slot_r}, {"tp": slot_l}

    own = [
        pltpu.make_async_copy(gate_w, gu.at[z, y, :, 0:width], local_sem.at[0]),
        pltpu.make_async_copy(up_w, gu.at[z, y, :, width:], local_sem.at[1]),
        pltpu.make_async_copy(down_w, dn.at[z, y], local_sem.at[2]),
        pltpu.make_async_copy(out_w, wo.at[tp], local_sem.at[3]),
        pltpu.make_async_copy(resid.at[tp], res.at[tp], local_sem.at[4]),
    ]
    for copy in own:
        copy.start()

    barrier = pltpu.get_barrier_semaphore()
    greet = [{"sp": right}, {"sp": left}] + y_peers + z_peers + tp_peers
    for peer in greet:
        pl.semaphore_signal(barrier, inc=1, device_id=peer, device_id_type=MESH)
    pl.semaphore_wait(barrier, len(greet))

    net = Net(send_sem, recv_sem)
    tail = pl.ds(xs.shape[1] - 16, 16)
    rims = [net.put(src, rim.at[n], {"sp": right}) for n, src in enumerate(
        [xs.at[0, tail], xs.at[1, tail], k1.at[tail], q1.at[tail], kq2.at[tail]])]

    def both(ref_a, ref_b, to_a, to_b):
        return net.put(ref_a, ref_a, to_a), net.put(ref_b, ref_b, to_b)

    def arrive(pair):
        for copy in pair:
            copy.wait_recv()

    def gu_z(r):
        a, b = zmod(z - (r - 1)), zmod(z + (r - 1))
        if r == 4:
            return both(gu.at[a, y, :, 0:width], gu.at[b, y, :, width:], up_z, down_z)
        return both(gu.at[a, y], gu.at[b, y], up_z, down_z)

    def gu_y(k):
        zz = zmod(z + k)
        return both(gu.at[zz, y], gu.at[zz, y], up_y, down_y)

    def gu_y_relay(k):
        zz = zmod(z + k)
        return both(gu.at[zz, ymod(y - 1), :, 0:width], gu.at[zz, ymod(y + 1), :, width:], up_y, down_y)

    def dn_z(r):
        a, b = zmod(z - (r - 1)), zmod(z + (r - 1))
        if r == 4:
            return both(dn.at[a, 0:2], dn.at[b, 2:4], up_z, down_z)
        return both(dn.at[a], dn.at[b], up_z, down_z)

    def wo_first(g):
        ref = wo.at[tp, g]
        return net.put(ref, ref, x_right), net.put(ref, ref, x_left), net.put(ref, ref, partner)

    def gather_second(ref_l, ref_r, half):
        a, b = ref_l.at[0:half], ref_r.at[half:]
        return (net.put(a, a, x_right), net.put(b, b, x_left),
                net.put(ref_l, ref_l, partner), net.put(ref_r, ref_r, partner))

    for copy in own[:3]:
        copy.wait()
    gz1 = gu_z(1)
    gy = {0: gu_y(0)}
    gr = {}
    dy = both(dn.at[z, y], dn.at[z, y], up_y, down_y)
    resid_puts = []
    for j in range(1, NTP):
        to = lax.rem(tp + j, NTP)
        resid_puts.append(net.put(resid.at[to], res.at[tp], {"tp": to}))
    own[3].wait()
    own[4].wait()
    wo_a = [wo_first(0), wo_first(1)]
    wo_b, wo_c = [], []

    def pump_wo(g):
        arrive(wo_a[g][:2])
        wo_b.append(gather_second(wo.at[slot_l, g], wo.at[slot_r, g], wo.shape[2] // 2))

    def pump_wo_last(g):
        arrive(wo_b[g][:2])
        ref = wo.at[slot_o, g]
        wo_c.append(net.put(ref, ref, partner))

    lane = lax.broadcasted_iota(jnp.int32, (8, 128), 1)
    row8 = lax.broadcasted_iota(jnp.int32, (8, 128), 0)
    low = lax.broadcasted_iota(jnp.int32, (BLOCK, 128), 1) < HEAD
    low1 = lax.broadcasted_iota(jnp.int32, (1, 128), 1) < HEAD
    causal = lax.broadcasted_iota(jnp.int32, (BLOCK, BLOCK), 0) >= lax.broadcasted_iota(
        jnp.int32, (BLOCK, BLOCK), 1)

    state[...] = jnp.zeros_like(state)
    for copy in rims:
        copy.wait_recv()
    has_left = sp > 0
    tails = tuple(
        jnp.where(has_left, rim[n].astype(F32)[8:16], 0.0) for n in range(5))

    def conv(block, before, taps):
        full = jnp.concatenate([before, block], axis=0)
        total = taps[0] * full[5 : 5 + BLOCK]
        for k in range(1, CONV):
            total = total + taps[k] * full[5 + k : 5 + k + BLOCK]
        return silu(total)

    def first(b, carry):
        before, offs = carry[:5], carry[5]
        at = pl.ds(pl.multiple_of(b * BLOCK, BLOCK), BLOCK)
        r = table[b]
        c = r
        for s in (1, 2, 4, 8, 16, 32, 64):
            c = c + jnp.where(lane >= s, pltpu.roll(c, s, 1), 0.0)
        t = jnp.where(row8 < 4, c, r).T
        cols[b] = t
        erun[b] = jnp.exp(jnp.where(row8 < 4, c + offs, 0.0)).T
        raw = [xs[0, at].astype(F32), xs[1, at].astype(F32), k1[at].astype(F32),
               q1[at].astype(F32), kq2[at].astype(F32)]
        key_one = conv(raw[2], before[2], [taps1[k, 0:1] for k in range(CONV)])
        query_one = conv(raw[3], before[3], [taps1[k, 1:2] for k in range(CONV)])
        both = conv(raw[4], before[4], [taps2[k : k + 1] for k in range(CONV)])
        key_two = jnp.where(low, both, 0.0)
        query_two = jnp.where(low, pltpu.roll(both, 64, 1), 0.0)
        for g, (key, query) in enumerate([(key_one, query_one), (key_two, query_two)]):
            u = conv(raw[g], before[g], [head_taps[k, g : g + 1] for k in range(CONV)])
            h = 2 * g
            v = u * halves(low, t[:, 4 + h : 5 + h], t[:, 5 + h : 6 + h])
            cum = halves(low, t[:, h : h + 1], t[:, h + 1 : h + 2])
            total = halves(low1, c[h : h + 1, 127:128], c[h + 1 : h + 2, 127:128])
            to_end = jnp.exp(total - cum)
            kb = key.astype(BF16)
            keys[g, at] = kb
            queries[g, at] = query.astype(BF16)
            values[g, at] = v.astype(BF16)
            old = state[g]
            starts[g, b] = old.astype(BF16)
            state[g] = old * jnp.exp(total) + dot(kb, (v * to_end).astype(BF16), 0, 0)
        offs = offs + jnp.broadcast_to(c[:, 127:128], (8, 128))
        return tuple(v[BLOCK - 8 :] for v in raw) + (offs,)

    carry = lax.fori_loop(
        0, blocks // 2, first, tails + (jnp.zeros((8, 128), F32),))

    arrive(gz1)
    gz2 = gu_z(2)
    gy[1], gy[-1] = gu_y(1), gu_y(-1)
    arrive(dy)
    dy2 = both(dn.at[z, ymod(y - 1), 0:32], dn.at[z, ymod(y + 1), 32:64], up_y, down_y)

    carry = lax.fori_loop(blocks // 2, blocks, first, carry)
    offs = carry[5]
    log0 = halves(low1, offs[0:1], offs[1:2])
    log1 = halves(low1, offs[2:3], offs[3:4])

    logs = log_rows(log0, log1)
    full_state = jnp.concatenate([state[0], state[1][0:64]], axis=0).astype(BF16)
    for q in range(NY):
        msg1[q, 0:QROWS] = full_state[q * QROWS : (q + 1) * QROWS]
        msg1[q, QROWS:MROWS] = logs
    copies1 = []
    for j in range(1, NY):
        to = ymod(y + j)
        copies1.append(net.put(msg1.at[to], buf1.at[y], {"sp": z * NY + to}))
    buf1[y] = msg1[y]

    arrive(gz2)
    gz3 = gu_z(3)
    arrive(gy[0])
    gr[0] = gu_y_relay(0)
    pump_wo(0)

    def inside(b, carry):
        at = pl.ds(pl.multiple_of(b * BLOCK, BLOCK), BLOCK)
        t = cols[b]
        crow = t.T
        for g in range(2):
            h = 2 * g
            qb, kb, v = queries[g, at], keys[g, at], values[g, at]
            scores = dot(qb, kb, 1, 1)
            weights = []
            for j in range(2):
                span = t[:, h + j : h + j + 1] - crow[h + j : h + j + 1]
                weights.append((jnp.exp(jnp.where(causal, span, -jnp.inf)) * scores).astype(BF16))
            zero = jnp.zeros_like(v)
            two = jnp.concatenate([jnp.where(low, v, zero), jnp.where(low, zero, v)], axis=0)
            out = dot(jnp.concatenate(weights, axis=1), two, 1, 0)
            cum = halves(low, t[:, h : h + 1], t[:, h + 1 : h + 2])
            local[g, at] = out + dot(qb, starts[g, b], 1, 0) * jnp.exp(cum)
        return carry

    lax.fori_loop(0, blocks // 2, inside, 0)

    arrive(copies1)
    rows = y * QROWS + lax.broadcasted_iota(jnp.int32, (QROWS, 128), 0)
    group_one = rows < 128

    def factor(f0, f1):
        return jnp.where(group_one, f0, f1)

    prefix, befores = [], []
    run = jnp.zeros((QROWS, 128), F32)
    sum0 = jnp.zeros((1, 128), F32)
    sum1 = jnp.zeros((1, 128), F32)
    for j in range(NY):
        prefix.append(run)
        befores.append((sum0, sum1))
        l0, l1 = read_logs(buf1[j, QROWS:MROWS])
        run = run * factor(jnp.exp(l0), jnp.exp(l1)) + buf1[j, 0:QROWS].astype(F32)
        sum0, sum1 = sum0 + l0, sum1 + l1
    msg2[0:QROWS] = run.astype(BF16)
    msg2[QROWS:MROWS] = log_rows(sum0, sum1)
    copies2 = []
    for j in range(1, NZ):
        copies2.append(net.put(msg2, buf2.at[z], {"sp": zmod(z + j) * NY + y}))
    buf2[z] = msg2[...]

    arrive(gz3)
    gz4 = gu_z(4)
    arrive(dy2)
    dz1 = dn_z(1)

    lax.fori_loop(blocks // 2, blocks, inside, 0)

    arrive(copies2)
    run = jnp.zeros((QROWS, 128), F32)
    for j in range(NZ):
        l0, l1 = read_logs(buf2[j, QROWS:MROWS])
        new = run * factor(jnp.exp(l0), jnp.exp(l1)) + buf2[j, 0:QROWS].astype(F32)
        run = jnp.where(j < z, new, run)
    for j in range(NY):
        l0, l1 = befores[j]
        msg3[j] = (run * factor(jnp.exp(l0), jnp.exp(l1)) + prefix[j]).astype(BF16)
    mine = pl.ds(pl.multiple_of(y * QROWS, 16), QROWS)
    copies3 = []
    for j in range(1, NY):
        to = ymod(y + j)
        copies3.append(net.put(msg3.at[to], enter.at[mine], {"sp": z * NY + to}))
    enter[mine] = msg3[y]

    gy[2], gy[-2] = gu_y(2), gu_y(-2)
    arrive(gy[1])
    gr[1] = gu_y_relay(1)
    arrive(gy[-1])
    gr[-1] = gu_y_relay(-1)
    pump_wo(1)
    arrive(copies3)

    enter_one = enter[0:128]
    enter_two = jnp.concatenate([enter[128:192], jnp.zeros((64, 128), BF16)], axis=0)

    mix_at = net.reserve(NTP - 1)

    def mix_copy(i):
        to = lax.rem(tp + 1 + i, NTP)
        return net.make(mix_send.at[to], mix.at[tp], {"tp": to}, mix_at + i)

    def finish(i, carry):
        b = lax.rem(tp + 1 + i, NTP)
        at = pl.ds(pl.multiple_of(b * BLOCK, BLOCK), BLOCK)
        e = erun[b]
        for g, entering in enumerate([enter_one, enter_two]):
            h = 2 * g
            m = local[g, at] + dot(queries[g, at], entering, 1, 0) * halves(
                low, e[:, h : h + 1], e[:, h + 1 : h + 2])
            m = m * silu(gs[g, at].astype(F32))
            square = m * m
            s0 = jnp.sum(jnp.where(low, square, 0.0), axis=1, keepdims=True)
            s1 = jnp.sum(jnp.where(low, 0.0, square), axis=1, keepdims=True)
            scale = lax.rsqrt(halves(low, s0, s1) * (1.0 / HEAD) + EPSILON)
            mix_send[b, g] = (m * scale * gain[g : g + 1]).astype(BF16)

        @pl.when(i < NTP - 1)
        def _():
            mix_copy(i).start()

        return carry

    lax.fori_loop(0, NTP, finish, 0)
    mix[tp] = mix_send[tp]

    arrive(dz1)
    dz2 = dn_z(2)
    arrive(gz4)
    gy[3], gy[-3] = gu_y(3), gu_y(-3)
    gy[4] = gu_y(4)
    pump_wo_last(0)
    arrive(resid_puts)
    pump_wo_last(1)
    for i in range(NTP - 1):
        mix_copy(i).wait_recv()
    for g in range(2):
        wo_a[g][2].wait_recv()
        arrive(wo_b[g][2:])
        wo_c[g].wait_recv()

    lhs = jnp.concatenate([mix[t, g] for g in range(2) for t in range(NTP)], axis=1)
    depth = lhs.shape[1]
    square = jnp.zeros((BLOCK, 1), F32)
    for s in range(NTP):
        row = dot(lhs, wo[s].reshape(depth, 256), 1, 0) + res[s].astype(F32)
        row = row.astype(BF16)
        stm[s] = row
        wide = row.astype(F32)
        square = square + jnp.sum(wide * wide, axis=1, keepdims=True)
    scale = lax.rsqrt(square * (1.0 / depth) + EPSILON)
    tokens = BLOCK // CHUNKS
    for s in range(NTP):
        cut = slice(s * 256, (s + 1) * 256)
        normed = (stm[s].astype(F32) * scale * channel_gain[:, cut]).astype(BF16)
        for h in range(CHUNKS):
            nb[h, tp, :, cut] = normed[h * tokens : (h + 1) * tokens]

    arrive(dz2)
    dz3 = dn_z(3)
    ag_a, ag_b, ag_c = [], [], []
    for h in range(CHUNKS):
        ref = nb.at[h, tp]
        ag_a.append((net.put(ref, ref, x_right), net.put(ref, ref, x_left), net.put(ref, ref, partner)))
    arrive(gy[2])
    gr[2] = gu_y_relay(2)
    arrive(gy[-2])
    gr[-2] = gu_y_relay(-2)

    def ag_second(h):
        arrive(ag_a[h][:2])
        ag_b.append(gather_second(nb.at[h, slot_l], nb.at[h, slot_r], tokens // 2))

    def ag_third(h):
        arrive(ag_b[h][:2])
        ref = nb.at[h, slot_o]
        ag_c.append(net.put(ref, ref, partner))

    def ag_done(h):
        ag_a[h][2].wait_recv()
        arrive(ag_b[h][2:])
        ag_c[h].wait_recv()

    ag_second(0)
    arrive(gy[3])
    gr[3] = gu_y_relay(3)
    arrive(gy[-3])
    gr[-3] = gu_y_relay(-3)
    arrive(gy[4])
    gr[4] = gu_y_relay(4)
    arrive(dz3)
    dz4 = dn_z(4)
    ag_third(0)
    feat_puts = []
    ag_second(1)
    for j in range(1, NTP):
        to = lax.rem(tp + j, NTP)
        feat_puts.append(net.put(stm.at[to], feat.at[tp], {"tp": to}))
    feat[tp] = stm[tp]
    for k in (0, 1, -1, 2, -2, 3, -3, 4):
        arrive(gr[k])
    ag_done(0)

    n_rows = NTP * tokens
    order = (2, 3, 1, 0)
    dests = {k: lax.rem(x + k, NX) * 2 for k in order}

    def hid(h):
        for m in range(2):
            rows_in = nb[h, 4 * m : 4 * m + 4].reshape(4 * tokens, depth)
            both_up = dot(rows_in, gu[...].reshape(depth, 2 * width), 1, 0)
            g, u = both_up[:, :width], both_up[:, width:]
            hidden[4 * tokens * m : 4 * tokens * (m + 1)] = (silu(g) * u).astype(BF16)

    def down(d):
        return dot(hidden[...], dn[d].reshape(256, width), 1, 1).astype(BF16)

    ps_puts, rl_puts, out_puts = {}, {}, {}

    def down_partner(h):
        for k in order:
            ps[h, k] = down(dests[k] + 1 - core)
            ps_puts[h, k] = net.put(ps.at[h, k], pr.at[h, k], partner)

    def down_own(h):
        for k in order:
            po[h, k] = down(dests[k] + core)

    def pair_sum(h, k):
        ps_puts[h, k].wait_recv()
        return po[h, k].astype(F32) + pr[h, k].astype(F32)

    mid = n_rows // 2

    def rs_first(h):
        qs[h, 2] = pair_sum(h, 2).astype(BF16)
        rl_puts[h] = (net.put(qs.at[h, 2, 0:mid], relay_r.at[h], x_left),
                      net.put(qs.at[h, 2, mid:], relay_l.at[h], x_right))

    def rs_second(h):
        to_left, to_right = pair_sum(h, 3), pair_sum(h, 1)
        arrive(rl_puts[h])
        qs[h, 3, 0:mid] = (to_left[0:mid] + relay_r[h].astype(F32)).astype(BF16)
        qs[h, 3, mid:] = to_left[mid:].astype(BF16)
        qs[h, 1, 0:mid] = to_right[0:mid].astype(BF16)
        qs[h, 1, mid:] = (to_right[mid:] + relay_l[h].astype(F32)).astype(BF16)
        out_puts[h] = (net.put(qs.at[h, 3], from_r.at[h], x_left),
                       net.put(qs.at[h, 1], from_l.at[h], x_right))

    def rs_third(h):
        total = pair_sum(h, 0)
        arrive(out_puts[h])
        total = total + from_l[h].astype(F32) + from_r[h].astype(F32)
        at = slice(h * tokens, (h + 1) * tokens)
        stream = feat[:, at].astype(F32)
        out[:, at] = (stream + 0.5 * total.reshape(NTP, tokens, 256)).astype(BF16)

    hid(0)
    ag_third(1)
    for pair in (dz4,):
        arrive(pair)
    down_partner(0)
    down_own(0)
    rs_first(0)
    ag_done(1)
    hid(1)
    rs_second(0)
    down_partner(1)
    down_own(1)
    rs_first(1)
    arrive(feat_puts)
    rs_third(0)
    rs_second(1)
    rs_third(1)

    for copy in net.sent:
        copy.wait_send()
    for i in range(NTP - 1):
        mix_copy(i).wait_send()


def layer(args, hbm_args):
    length = args[0].shape[1]
    blocks = length // BLOCK
    tokens = BLOCK // CHUNKS
    n_rows = NTP * tokens
    vmem = pl.BlockSpec(memory_space=pltpu.VMEM)
    hbm = pl.BlockSpec(memory_space=pl.ANY)
    dma = pltpu.SemaphoreType.DMA
    width = hbm_args[2].shape[1]
    return pl.pallas_call(
        layer_kernel,
        out_shape=jax.ShapeDtypeStruct((NTP, BLOCK, 256), BF16),
        in_specs=[vmem] * len(args) + [hbm] * len(hbm_args),
        out_specs=vmem,
        scratch_shapes=[
            pltpu.VMEM((5, 16, 128), BF16),
            pltpu.VMEM((2, length, 128), BF16),
            pltpu.VMEM((2, length, 128), BF16),
            pltpu.VMEM((2, length, 128), BF16),
            pltpu.VMEM((2, length, 128), F32),
            pltpu.VMEM((blocks, BLOCK, 8), F32),
            pltpu.VMEM((blocks, BLOCK, 8), F32),
            pltpu.VMEM((2, 128, 128), F32),
            pltpu.VMEM((2, blocks, 128, 128), BF16),
            pltpu.VMEM((NY, MROWS, 128), BF16),
            pltpu.VMEM((NY, MROWS, 128), BF16),
            pltpu.VMEM((MROWS, 128), BF16),
            pltpu.VMEM((NZ, MROWS, 128), BF16),
            pltpu.VMEM((NY, QROWS, 128), BF16),
            pltpu.VMEM((NY * QROWS, 128), BF16),
            pltpu.VMEM((NZ, NY, 64, 2 * width), BF16),
            pltpu.VMEM((NZ, NY, 64, width), BF16),
            pltpu.VMEM((NTP, 2, 1024, 256), BF16),
            pltpu.VMEM((NTP, BLOCK, 256), BF16),
            pltpu.VMEM((NTP, 2, BLOCK, 128), BF16),
            pltpu.VMEM((NTP, 2, BLOCK, 128), BF16),
            pltpu.VMEM((NTP, BLOCK, 256), BF16),
            pltpu.VMEM((NTP, BLOCK, 256), BF16),
            pltpu.VMEM((CHUNKS, NTP, tokens, 2048), BF16),
            pltpu.VMEM((n_rows, width), BF16),
            pltpu.VMEM((CHUNKS, NX, n_rows, 256), BF16),
            pltpu.VMEM((CHUNKS, NX, n_rows, 256), BF16),
            pltpu.VMEM((CHUNKS, NX, n_rows, 256), BF16),
            pltpu.VMEM((CHUNKS, n_rows // 2, 256), BF16),
            pltpu.VMEM((CHUNKS, n_rows // 2, 256), BF16),
            pltpu.VMEM((CHUNKS, NX, n_rows, 256), BF16),
            pltpu.VMEM((CHUNKS, n_rows, 256), BF16),
            pltpu.VMEM((CHUNKS, n_rows, 256), BF16),
            dma((5,)), dma((N_PUT,)), dma((N_PUT,)),
        ],
        compiler_params=pltpu.CompilerParams(
            collective_id=0, has_side_effects=True, vmem_limit_bytes=58 * 1024 * 1024),
        cost_estimate=pl.CostEstimate(
            flops=12_000_000_000, bytes_accessed=8_000_000, transcendentals=4_000_000),
        name="layer",
    )(*args, *hbm_args)


def shards(
    grouped_head_inputs,
    head_gate_inputs,
    unsmoothed_step,
    head_decay_rate,
    extra_log_decay,
    first_group_keys,
    first_group_queries,
    second_group_keys,
    second_group_queries,
    head_input_filter,
    first_group_filter,
    second_group_filter,
    head_norm_gain,
    output_weight,
    residual,
    channel_norm_gain,
    channel_gate_weight,
    channel_up_weight,
    channel_down_weight,
):
    length = grouped_head_inputs.shape[0]
    blocks = length // BLOCK
    step = jax.nn.softplus(unsmoothed_step)
    log_decay = extra_log_decay - step * head_decay_rate[None]
    table = jnp.stack([log_decay, step]).reshape(2, blocks, BLOCK, 4)
    table = table.transpose(1, 0, 3, 2).reshape(blocks, 8, BLOCK)
    out = layer(
        (
            grouped_head_inputs.transpose(1, 0, 2),
            head_gate_inputs.transpose(1, 0, 2),
            first_group_keys,
            first_group_queries,
            jnp.concatenate([second_group_keys, second_group_queries], axis=1),
            table,
            head_input_filter,
            first_group_filter,
            second_group_filter.reshape(CONV, 128),
            head_norm_gain,
            channel_norm_gain[None],
        ),
        (
            output_weight,
            residual.reshape(NTP, BLOCK, 256),
            channel_gate_weight,
            channel_up_weight,
            channel_down_weight,
        ),
    )
    return out.reshape(length, 256)


def solution(mesh):
    return jax.shard_map(
        shards,
        mesh=mesh,
        in_specs=(
            P("sp", None, "tp"),
            P("sp", None, "tp"),
            P("sp", None, "tp"),
            P(None, "tp"),
            P("sp", None, "tp"),
            P("sp", None),
            P("sp", None),
            P("sp", None),
            P("sp", None),
            P(None, None, "tp"),
            P(),
            P(),
            P(None, "tp"),
            P(None, None, "tp"),
            P("sp", "tp"),
            P(),
            P("sp", "tp"),
            P("sp", "tp"),
            P("sp", "tp"),
        ),
        out_specs=P("sp", "tp"),
        check_vma=False,
    )
```

```python
import functools

import jax
import jax.numpy as jnp
from jax import lax
from jax.experimental import pallas as pl
from jax.experimental.pallas import tpu as pltpu
from jax.sharding import PartitionSpec as P

HEAD = 64
CONV = 4
BLOCK = 128
EPSILON = 1e-06
MESH = pl.DeviceIdType.MESH
F32 = jnp.float32
BF16 = jnp.bfloat16
NY = 4
NZ = 8
NX = 4
NTP = 8
QROWS = 48
MROWS = 64
CHUNKS = 4
N_PUT = 176
STEPS = (
    "bA", "bB", "b0", "s1", "gy1", "gz2", "ia", "ib", "s2", "dy2", "gz3", "dz1", "s3", "gy2",
    "gr-1", "gr0", "gr1", "gz4", "gy3", "fin0", "Ai0", "fin1", "Ai1", "fin2", "fin3", "gr2",
    "dz2", "Ai2", "Ar0", "gr-2", "gy4", "Ar1", "Ai3", "Ar2", "Af0", "Af1", "P0", "Bi0", "dz3",
    "P1", "Bi1", "gr3", "Ar3", "Af2", "gr-3", "P2", "Bi2", "Br0", "Br1", "dz4", "Af3", "gr4",
    "P3", "Bi3", "Br2", "Bf0", "Bf1", "H0", "D0", "H1", "Bf2", "Br3", "D1", "E0", "C10", "E1",
    "H2", "Bf3", "C11", "D2", "C20", "E2", "H3", "C12", "C21", "D3", "E3", "C30", "C13", "C22",
    "C31", "C23", "C32", "C33",
)


def mark(name):
    pass


def silu(v):
    return v * (0.5 * jnp.tanh(0.5 * v) + 0.5)


def halves(lane_low, a, b):
    return jnp.where(lane_low, a, b)


def dot(a, b, ca, cb):
    return lax.dot_general(a, b, (((ca,), (cb,)), ((), ())), preferred_element_type=F32)


def split_three(v):
    hi = v.astype(BF16)
    rest = v - hi.astype(F32)
    mid = rest.astype(BF16)
    low = (rest - mid.astype(F32)).astype(BF16)
    return hi, mid, low


def log_rows(l0, l1):
    rows = []
    for part0, part1 in zip(split_three(l0), split_three(l1)):
        rows += [part0.astype(F32), part1.astype(F32)]
    rows.append(jnp.zeros((10, 128), F32))
    return jnp.concatenate(rows, axis=0).astype(BF16)


def read_logs(rows):
    v = rows.astype(F32)
    return v[0:1] + v[2:3] + v[4:5], v[1:2] + v[3:4] + v[5:6]


class Net:
    def __init__(self, send, recv):
        self.send, self.recv, self.sent = send, recv, []

    def put(self, src, dst, to):
        index = len(self.sent)
        copy = pltpu.make_async_remote_copy(
            src_ref=src, dst_ref=dst, send_sem=self.send.at[index], recv_sem=self.recv.at[index],
            device_id=to, device_id_type=MESH)
        copy.start()
        self.sent.append(copy)
        return copy


def arrive(copies):
    for copy in copies:
        copy.wait_recv()


def layer_kernel(
    step_in, extra, head_taps, taps1, taps2, gain, channel_gain, rate,
    hx, hg, k1, q1, k2t, q2t, out_w, resid, gate_w, up_w, down_w,
    out,
    raw_x, raw_g, raw_k, raw_q, raw_t, xf, gf, pad, rim_x, rim_k, rim_q, rim_t,
    ctab, cols, keys, queries, values, local, gates, upd, starts,
    msg1, buf1, msg2, buf2, msg3, enter,
    gu, dn, wo, res, mx, st, nb, hidden, ps, pr, po, relay_l, relay_r, qs, from_l, from_r,
    local_sem, send_sem, recv_sem,
):
    sp = lax.axis_index("sp")
    tp = lax.axis_index("tp")
    y = lax.rem(sp, NY)
    z = sp // NY
    core = lax.rem(tp, 2)
    x = tp // 2
    n_sp = NY * NZ
    length = k1.shape[0]
    blocks = length // BLOCK
    width = gate_w.shape[1]
    depth = wo.shape[0]
    right = lax.rem(sp + 1, n_sp)
    left = lax.rem(sp + n_sp - 1, n_sp)

    def zmod(v):
        return lax.rem(v + NZ, NZ)

    def ymod(v):
        return lax.rem(v + NY, NY)

    y_peers = [{"sp": z * NY + ymod(y + j)} for j in range(1, NY)]
    z_peers = [{"sp": zmod(z + j) * NY + y} for j in range(1, NZ)]
    up_y, down_y = {"sp": z * NY + ymod(y + 1)}, {"sp": z * NY + ymod(y - 1)}
    up_z, down_z = {"sp": zmod(z + 1) * NY + y}, {"sp": zmod(z - 1) * NY + y}
    slot_l = lax.rem(x + NX - 1, NX) * 2 + core
    slot_r = lax.rem(x + 1, NX) * 2 + core
    slot_o = lax.rem(x + 2, NX) * 2 + core
    partner, x_right, x_left = {"tp": x * 2 + 1 - core}, {"tp": slot_r}, {"tp": slot_l}

    mark("barrier")
    wanted = [
        (gate_w, gu.at[z, y, :, 0:width]),
        (up_w, gu.at[z, y, :, width:]),
        (down_w, dn.at[z, y]),
        (hx, raw_x),
        (k1, raw_k),
        (q1, raw_q),
        (k2t, raw_t.at[0:64]),
        (q2t, raw_t.at[64:128]),
        (hg, raw_g),
        (out_w, wo),
        (resid, res),
    ]
    own = [pltpu.make_async_copy(a, b, local_sem.at[n]) for n, (a, b) in enumerate(wanted)]
    for copy in own:
        copy.start()

    barrier = pltpu.get_barrier_semaphore()
    greet = [{"sp": right}, {"sp": left}] + y_peers + z_peers + [partner, x_right, x_left]
    for peer in greet:
        pl.semaphore_signal(barrier, inc=1, device_id=peer, device_id_type=MESH)

    mark("tables")
    row8 = lax.broadcasted_iota(jnp.int32, (8, 128), 0)
    low = lax.broadcasted_iota(jnp.int32, (BLOCK, 128), 1) < HEAD
    low1 = lax.broadcasted_iota(jnp.int32, (1, 128), 1) < HEAD
    at_row = lax.broadcasted_iota(jnp.int32, (BLOCK, BLOCK), 0)
    at_col = lax.broadcasted_iota(jnp.int32, (BLOCK, BLOCK), 1)
    causal = at_row >= at_col
    upper = jnp.where(at_row <= at_col, 1.0, 0.0).astype(BF16)
    first_head = lax.broadcasted_iota(jnp.int32, (2, length), 0) == 0
    steps = [jax.nn.softplus(step_in[g]) for g in range(2)]
    logs = [extra[g] - steps[g] * jnp.where(first_head, rate[g, 0], rate[g, 1]) for g in range(2)]
    table = jnp.concatenate(
        [v[:, b * BLOCK : (b + 1) * BLOCK] for b in range(blocks) for v in logs + steps], axis=0)
    rows = table.shape[0]
    sums = dot(jnp.concatenate(split_three(table), axis=0), upper, 1, 0)
    sums = sums[0:rows] + sums[rows : 2 * rows] + sums[2 * rows :]
    offs = jnp.zeros((8, 1), F32)
    for b in range(blocks):
        cut = slice(8 * b, 8 * b + 8)
        c8 = jnp.where(row8 < 4, sums[cut], table[cut])
        ctab[b] = c8
        e8 = jnp.exp(jnp.where(row8 < 4, c8 + offs, 0.0))
        cols[b] = jnp.concatenate([c8, e8], axis=0).T
        offs = offs + c8[:, 127:128]
    log0 = halves(low1, offs[0:1], offs[1:2])
    log1 = halves(low1, offs[2:3], offs[3:4])
    my_logs = log_rows(log0, log1)
    for q in range(NY):
        msg1[q, QROWS:MROWS] = my_logs

    mark("barwait")
    for copy in own[:8]:
        copy.wait()
    pl.semaphore_wait(barrier, len(greet))

    net = Net(send_sem, recv_sem)
    got = {}
    have = {("gz", 0)}

    def need(*key):
        if key not in have:
            have.add(key)
            arrive(got[key])

    tail = pl.ds(length - 16, 16)
    rims = [
        net.put(raw_x.at[pl.ds(2 * length - 16, 16)], rim_x, {"sp": right}),
        net.put(raw_k.at[tail], rim_k, {"sp": right}),
        net.put(raw_q.at[tail], rim_q, {"sp": right}),
        net.put(raw_t.at[:, pl.ds(length - BLOCK, BLOCK)], rim_t, {"sp": right}),
    ]

    def both(ref_a, ref_b, to_a, to_b):
        return net.put(ref_a, ref_a, to_a), net.put(ref_b, ref_b, to_b)

    def gu_z(r):
        need("gz", r - 1)
        a, b = zmod(z - (r - 1)), zmod(z + (r - 1))
        if r == 4:
            got["gz", r] = both(gu.at[a, y, :, 0:width], gu.at[b, y, :, width:], up_z, down_z)
        else:
            got["gz", r] = both(gu.at[a, y], gu.at[b, y], up_z, down_z)

    def gu_y(*ks):
        for k in ks:
            need("gz", abs(k))
            zz = zmod(z + k)
            got["gy", k] = both(gu.at[zz, y], gu.at[zz, y], up_y, down_y)

    def gu_y_relay(k):
        arrive(got["gy", k])
        zz = zmod(z + k)
        got["gr", k] = both(
            gu.at[zz, ymod(y - 1), :, 0:width], gu.at[zz, ymod(y + 1), :, width:], up_y, down_y)

    def dn_y(r):
        if r == 1:
            got["dy", 1] = both(dn.at[z, y], dn.at[z, y], up_y, down_y)
        else:
            arrive(got["dy", 1])
            got["dy", 2] = both(
                dn.at[z, ymod(y - 1), 0:32], dn.at[z, ymod(y + 1), 32:64], up_y, down_y)

    def dn_z(r):
        arrive(got["dz", r - 1] if r > 1 else got["dy", 2])
        a, b = zmod(z - (r - 1)), zmod(z + (r - 1))
        if r == 4:
            got["dz", r] = both(dn.at[a, 0:2], dn.at[b, 2:4], up_z, down_z)
        else:
            got["dz", r] = both(dn.at[a], dn.at[b], up_z, down_z)

    def tp_first(buf, key, k):
        ref = buf.at[k, tp]
        got[key, k, 0] = (net.put(ref, ref, x_right), net.put(ref, ref, x_left))
        got[key, k, 1] = [net.put(ref, ref, partner)]

    def tp_second(buf, key, k):
        arrive(got[key, k, 0])
        ref_l, ref_r = buf.at[k, slot_l], buf.at[k, slot_r]
        half = buf.shape[2] // 2
        a, b = ref_l.at[0:half], ref_r.at[half:]
        got[key, k, 2] = (net.put(a, a, x_right), net.put(b, b, x_left))
        got[key, k, 1] += [net.put(ref_l, ref_l, partner), net.put(ref_r, ref_r, partner)]

    def tp_third(buf, key, k):
        arrive(got[key, k, 2])
        ref = buf.at[k, slot_o]
        got[key, k, 1] += [net.put(ref, ref, partner)]

    def tp_done(key, k):
        arrive(got[key, k, 1])

    mark("start")
    gu_z(1)
    gu_y(0)
    dn_y(1)

    mark("spread")
    xf[...] = raw_x[...].astype(F32)
    for g in range(2):
        pad[g, 8 : 8 + length] = xf[pl.ds(g, length, stride=2)]
    pad[2, 8 : 8 + length] = raw_k[...].astype(F32)
    pad[3, 8 : 8 + length] = raw_q[...].astype(F32)
    for b in range(blocks):
        pad[4, 8 + b * BLOCK : 8 + (b + 1) * BLOCK] = raw_t[:, b * BLOCK : (b + 1) * BLOCK].astype(F32).T
    second_taps = [jnp.concatenate([taps2[k, 0:1], taps2[k, 1:2]], axis=1) for k in range(CONV)]
    all_taps = [
        [head_taps[k, 0:1] for k in range(CONV)],
        [head_taps[k, 1:2] for k in range(CONV)],
        [taps1[k, 0:1] for k in range(CONV)],
        [taps1[k, 1:2] for k in range(CONV)],
        second_taps,
    ]

    def conv(n, b):
        full = pad[n, pl.ds(pl.multiple_of(b * BLOCK, BLOCK), BLOCK + 8)]
        taps = all_taps[n]
        total = taps[0] * full[5 : 5 + BLOCK]
        for k in range(1, CONV):
            total = total + taps[k] * full[5 + k : 5 + k + BLOCK]
        return silu(total)

    def block(b, carry):
        at = pl.ds(pl.multiple_of(b * BLOCK, BLOCK), BLOCK)
        c = ctab[b]
        t = cols[b]
        key_one, query_one, mix_two = conv(2, b), conv(3, b), conv(4, b)
        key_two = jnp.where(low, mix_two, 0.0)
        query_two = jnp.where(low, pltpu.roll(mix_two, 64, 1), 0.0)
        for g, (key, query) in enumerate([(key_one, query_one), (key_two, query_two)]):
            h = 2 * g
            v = conv(g, b) * halves(low, t[:, 4 + h : 5 + h], t[:, 5 + h : 6 + h])
            cum = halves(low, t[:, h : h + 1], t[:, h + 1 : h + 2])
            total = halves(low1, c[h : h + 1, 127:128], c[h + 1 : h + 2, 127:128])
            kb = key.astype(BF16)
            keys[g, at] = kb
            queries[g, at] = query.astype(BF16)
            values[g, at] = v.astype(BF16)
            upd[g, b] = dot(kb, (v * jnp.exp(total - cum)).astype(BF16), 0, 0)
        return carry

    def run_blocks(lo, hi):
        lax.fori_loop(lo, hi, block, 0, unroll=2)

    def last_block():
        block(blocks - 1, 0)
        arrive(rims)
        has_left = sp > 0
        xf[0:16] = rim_x[...].astype(F32)
        for g in range(2):
            pad[g, 0:8] = jnp.where(has_left, xf[pl.ds(g, 8, stride=2)], 0.0)
        pad[2, 0:8] = jnp.where(has_left, rim_k[...].astype(F32)[8:16], 0.0)
        pad[3, 0:8] = jnp.where(has_left, rim_q[...].astype(F32)[8:16], 0.0)
        pad[4, 0:8] = jnp.where(has_left, rim_t[...].astype(F32).T[BLOCK - 8 :], 0.0)
        block(0, 0)
        ends = []
        for g in range(2):
            h = 2 * g
            state = jnp.zeros((BLOCK, 128), F32)
            for b in range(blocks):
                c = ctab[b]
                total = halves(low1, c[h : h + 1, 127:128], c[h + 1 : h + 2, 127:128])
                starts[g, b] = state.astype(BF16)
                state = state * jnp.exp(total) + upd[g, b]
            ends.append(state)
        full = jnp.concatenate([ends[0], ends[1][0:64]], axis=0).astype(BF16)
        for q in range(NY):
            msg1[q, 0:QROWS] = full[q * QROWS : (q + 1) * QROWS]

    quarter = y * QROWS + lax.broadcasted_iota(jnp.int32, (QROWS, 128), 0)
    group_one = quarter < 128

    def factor(l0, l1):
        return jnp.where(group_one, jnp.exp(l0), jnp.exp(l1))

    def stage1():
        got["s1"] = []
        for j in range(1, NY):
            to = ymod(y + j)
            got["s1"].append(net.put(msg1.at[to], buf1.at[y], {"sp": z * NY + to}))
        buf1[y] = msg1[y]

    before = []

    def stage2():
        arrive(got["s1"])
        run = jnp.zeros((QROWS, 128), F32)
        sum0 = jnp.zeros((1, 128), F32)
        sum1 = jnp.zeros((1, 128), F32)
        for j in range(NY):
            before.append((run, sum0, sum1))
            l0, l1 = read_logs(buf1[j, QROWS:MROWS])
            run = run * factor(l0, l1) + buf1[j, 0:QROWS].astype(F32)
            sum0, sum1 = sum0 + l0, sum1 + l1
        msg2[0:QROWS] = run.astype(BF16)
        msg2[QROWS:MROWS] = log_rows(sum0, sum1)
        got["s2"] = []
        for j in range(1, NZ):
            got["s2"].append(net.put(msg2, buf2.at[z], {"sp": zmod(z + j) * NY + y}))
        buf2[z] = msg2[...]

    def stage3():
        arrive(got["s2"])
        run = jnp.zeros((QROWS, 128), F32)
        for j in range(NZ):
            l0, l1 = read_logs(buf2[j, QROWS:MROWS])
            new = run * factor(l0, l1) + buf2[j, 0:QROWS].astype(F32)
            run = jnp.where(j < z, new, run)
        for j in range(NY):
            part, l0, l1 = before[j]
            msg3[j] = (run * factor(l0, l1) + part).astype(BF16)
        mine = pl.ds(pl.multiple_of(y * QROWS, 16), QROWS)
        got["s3"] = []
        for j in range(1, NY):
            to = ymod(y + j)
            got["s3"].append(net.put(msg3.at[to], enter.at[mine], {"sp": z * NY + to}))
        enter[mine] = msg3[y]

    def inside(b, carry):
        at = pl.ds(pl.multiple_of(b * BLOCK, BLOCK), BLOCK)
        t = cols[b]
        c = ctab[b]
        for g in range(2):
            h = 2 * g
            qb, v = queries[g, at], values[g, at]
            scores = dot(qb, keys[g, at], 1, 1)
            weights = []
            for j in range(2):
                span = t[:, h + j : h + j + 1] - c[h + j : h + j + 1]
                weights.append((jnp.exp(jnp.where(causal, span, -jnp.inf)) * scores).astype(BF16))
            zero = jnp.zeros_like(v)
            two = jnp.concatenate([jnp.where(low, v, zero), jnp.where(low, zero, v)], axis=0)
            cum = halves(low, t[:, h : h + 1], t[:, h + 1 : h + 2])
            local[g, at] = dot(jnp.concatenate(weights, axis=1), two, 1, 0) + dot(
                qb, starts[g, b], 1, 0) * jnp.exp(cum)
        return carry

    def inside_a():
        own[8].wait()
        gf[...] = raw_g[...].astype(F32)
        for g in range(2):
            gates[g] = silu(gf[pl.ds(g, length, stride=2)])
        lax.fori_loop(0, blocks // 2, inside, 0, unroll=2)

    def inside_b():
        lax.fori_loop(blocks // 2, blocks, inside, 0, unroll=2)

    per = blocks // CHUNKS
    tokens = BLOCK * per

    def finish(k):
        if k == 0:
            arrive(got["s3"])
        for i in range(per):
            b = k * per + i
            at = slice(b * BLOCK, (b + 1) * BLOCK)
            t = cols[b]
            for g in range(2):
                h = 8 + 2 * g
                if g == 0:
                    entering = enter[0:128]
                else:
                    entering = jnp.concatenate([enter[128:192], jnp.zeros((64, 128), BF16)], axis=0)
                m = local[g, at] + dot(queries[g, at], entering, 1, 0) * halves(
                    low, t[:, h : h + 1], t[:, h + 1 : h + 2])
                m = m * gates[g, at]
                square = m * m
                s0 = jnp.sum(jnp.where(low, square, 0.0), axis=1, keepdims=True)
                s1 = jnp.sum(jnp.where(low, 0.0, square), axis=1, keepdims=True)
                scale = lax.rsqrt(halves(low, s0, s1) * (1.0 / HEAD) + EPSILON)
                mx[k, tp, i * BLOCK : (i + 1) * BLOCK, g * 128 : (g + 1) * 128] = (
                    m * scale * gain[g : g + 1]).astype(BF16)

    def project(k):
        if k == 0:
            own[9].wait()
            own[10].wait()
        tp_done("A", k)
        lhs = jnp.concatenate(
            [mx[k, s, :, g * 128 : (g + 1) * 128] for g in range(2) for s in range(NTP)], axis=1)
        row = dot(lhs, wo[...], 1, 0) + res[k * tokens : (k + 1) * tokens].astype(F32)
        st[k, tp] = row.astype(BF16)

    def norm_hidden(k):
        tp_done("B", k)
        if k == 0:
            for j in (0, 1, -1, 2, -2, 3, -3, 4):
                arrive(got["gr", j])
        square = jnp.zeros((tokens, 128), F32)
        for s in range(NTP):
            v = st[k, s].astype(F32)
            square = square + v[:, :128] * v[:, :128] + v[:, 128:] * v[:, 128:]
        scale = lax.rsqrt(jnp.sum(square, axis=1, keepdims=True) * (1.0 / depth) + EPSILON)
        for s in range(NTP):
            cut = slice(s * 256, (s + 1) * 256)
            nb[:, cut] = (st[k, s].astype(F32) * scale * channel_gain[:, cut]).astype(BF16)
        pair = dot(nb[...], gu[...].reshape(depth, 2 * width), 1, 0)
        hidden[k] = (silu(pair[:, :width]) * pair[:, width:]).astype(BF16)

    order = (2, 3, 1, 0)
    dests = {k: lax.rem(x + k, NX) * 2 for k in order}

    def down(k, d):
        return dot(hidden[k], dn[d].reshape(256, width), 1, 1).astype(BF16)

    def down_partner(k):
        if k == 0:
            arrive(got["dz", 4])
        for j in order:
            ps[k, j] = down(k, dests[j] + 1 - core)
            got["P", k, j] = net.put(ps.at[k, j], pr.at[k, j], partner)

    def down_own(k):
        for j in order:
            po[k, j] = down(k, dests[j] + core)

    def pair_sum(k, j):
        got["P", k, j].wait_recv()
        return po[k, j].astype(F32) + pr[k, j].astype(F32)

    mid = tokens // 2

    def sum_first(k):
        qs[k, 2] = pair_sum(k, 2).astype(BF16)
        got["C1", k] = (net.put(qs.at[k, 2, 0:mid], relay_r.at[k], x_left),
                        net.put(qs.at[k, 2, mid:], relay_l.at[k], x_right))

    def sum_second(k):
        to_left, to_right = pair_sum(k, 3), pair_sum(k, 1)
        arrive(got["C1", k])
        qs[k, 3, 0:mid] = (to_left[0:mid] + relay_r[k].astype(F32)).astype(BF16)
        qs[k, 3, mid:] = to_left[mid:].astype(BF16)
        qs[k, 1, 0:mid] = to_right[0:mid].astype(BF16)
        qs[k, 1, mid:] = (to_right[mid:] + relay_l[k].astype(F32)).astype(BF16)
        got["C2", k] = (net.put(qs.at[k, 3], from_r.at[k], x_left),
                        net.put(qs.at[k, 1], from_l.at[k], x_right))

    def sum_third(k):
        total = pair_sum(k, 0)
        arrive(got["C2", k])
        total = total + from_l[k].astype(F32) + from_r[k].astype(F32)
        out[k * tokens : (k + 1) * tokens] = (st[k, tp].astype(F32) + 0.5 * total).astype(BF16)

    run = {
        "bA": lambda: run_blocks(1, 5),
        "bB": lambda: run_blocks(5, 7),
        "b0": last_block,
        "s1": stage1,
        "s2": stage2,
        "s3": stage3,
        "ia": inside_a,
        "ib": inside_b,
        "gy1": lambda: gu_y(1, -1),
        "gy2": lambda: gu_y(2, -2),
        "gy3": lambda: gu_y(3, -3),
        "gy4": lambda: gu_y(4),
        "dy2": lambda: dn_y(2),
    }
    for r in (2, 3, 4):
        run[f"gz{r}"] = functools.partial(gu_z, r)
    for r in (1, 2, 3, 4):
        run[f"dz{r}"] = functools.partial(dn_z, r)
    for k in (0, 1, -1, 2, -2, 3, -3, 4):
        run[f"gr{k}"] = functools.partial(gu_y_relay, k)
    for k in range(CHUNKS):
        run[f"fin{k}"] = functools.partial(finish, k)
        run[f"P{k}"] = functools.partial(project, k)
        run[f"H{k}"] = functools.partial(norm_hidden, k)
        run[f"D{k}"] = functools.partial(down_partner, k)
        run[f"E{k}"] = functools.partial(down_own, k)
        run[f"C1{k}"] = functools.partial(sum_first, k)
        run[f"C2{k}"] = functools.partial(sum_second, k)
        run[f"C3{k}"] = functools.partial(sum_third, k)
        for key, buf in (("A", mx), ("B", st)):
            run[f"{key}i{k}"] = functools.partial(tp_first, buf, key, k)
            run[f"{key}r{k}"] = functools.partial(tp_second, buf, key, k)
            run[f"{key}f{k}"] = functools.partial(tp_third, buf, key, k)
    for name in STEPS:
        mark(name)
        run.pop(name)()
    assert not run

    mark("sends")
    for copy in net.sent:
        copy.wait_send()


def layer(vmem_args, smem_arg, hbm_args):
    length = hbm_args[2].shape[0]
    blocks = length // BLOCK
    tokens = length // CHUNKS
    width = hbm_args[8].shape[1]
    vmem = pl.BlockSpec(memory_space=pltpu.VMEM)
    dma = pltpu.SemaphoreType.DMA

    def bf(*shape):
        return pltpu.VMEM(shape, BF16)

    def fl(*shape):
        return pltpu.VMEM(shape, F32)

    return pl.pallas_call(
        layer_kernel,
        out_shape=jax.ShapeDtypeStruct((length, 256), BF16),
        in_specs=[vmem] * len(vmem_args)
        + [pl.BlockSpec(memory_space=pltpu.SMEM)]
        + [pl.BlockSpec(memory_space=pl.ANY)] * len(hbm_args),
        out_specs=vmem,
        scratch_shapes=[
            bf(2 * length, 128), bf(2 * length, 128), bf(length, 128), bf(length, 128),
            bf(128, length), fl(2 * length, 128), fl(2 * length, 128), fl(5, length + 8, 128),
            bf(16, 128), bf(16, 128), bf(16, 128), bf(128, 128),
            fl(blocks, 8, 128), fl(blocks, BLOCK, 16),
            bf(2, length, 128), bf(2, length, 128), bf(2, length, 128),
            fl(2, length, 128), fl(2, length, 128),
            fl(2, blocks, 128, 128), bf(2, blocks, 128, 128),
            bf(NY, MROWS, 128), bf(NY, MROWS, 128), bf(MROWS, 128), bf(NZ, MROWS, 128),
            bf(NY, QROWS, 128), bf(NY * QROWS, 128),
            bf(NZ, NY, 64, 2 * width), bf(NZ, NY, 64, width), bf(2048, 256), bf(length, 256),
            bf(CHUNKS, NTP, tokens, 256), bf(CHUNKS, NTP, tokens, 256),
            bf(tokens, 2048), bf(CHUNKS, tokens, width),
            bf(CHUNKS, NX, tokens, 256), bf(CHUNKS, NX, tokens, 256), bf(CHUNKS, NX, tokens, 256),
            bf(CHUNKS, tokens // 2, 256), bf(CHUNKS, tokens // 2, 256),
            bf(CHUNKS, NX, tokens, 256), bf(CHUNKS, tokens, 256), bf(CHUNKS, tokens, 256),
            dma((11,)), dma((N_PUT,)), dma((N_PUT,)),
        ],
        compiler_params=pltpu.CompilerParams(
            collective_id=0, has_side_effects=True, vmem_limit_bytes=58 * 1024 * 1024),
        cost_estimate=pl.CostEstimate(
            flops=12_000_000_000, bytes_accessed=8_000_000, transcendentals=4_000_000),
        name="layer",
    )(*vmem_args, smem_arg, *hbm_args)


def shards(
    grouped_head_inputs,
    head_gate_inputs,
    unsmoothed_step,
    head_decay_rate,
    extra_log_decay,
    first_group_keys,
    first_group_queries,
    second_group_keys,
    second_group_queries,
    head_input_filter,
    first_group_filter,
    second_group_filter,
    head_norm_gain,
    output_weight,
    residual,
    channel_norm_gain,
    channel_gate_weight,
    channel_up_weight,
    channel_down_weight,
):
    length = grouped_head_inputs.shape[0]
    return layer(
        (
            unsmoothed_step.transpose(1, 2, 0),
            extra_log_decay.transpose(1, 2, 0),
            head_input_filter,
            first_group_filter,
            second_group_filter,
            head_norm_gain,
            channel_norm_gain[None],
        ),
        head_decay_rate,
        (
            grouped_head_inputs.reshape(2 * length, 128),
            head_gate_inputs.reshape(2 * length, 128),
            first_group_keys,
            first_group_queries,
            second_group_keys.T,
            second_group_queries.T,
            output_weight.reshape(-1, output_weight.shape[2]),
            residual,
            channel_gate_weight,
            channel_up_weight,
            channel_down_weight,
        ),
    )


def solution(mesh):
    return jax.shard_map(
        shards,
        mesh=mesh,
        in_specs=(
            P("sp", None, "tp"),
            P("sp", None, "tp"),
            P("sp", None, "tp"),
            P(None, "tp"),
            P("sp", None, "tp"),
            P("sp", None),
            P("sp", None),
            P("sp", None),
            P("sp", None),
            P(None, None, "tp"),
            P(),
            P(),
            P(None, "tp"),
            P(None, None, "tp"),
            P("sp", "tp"),
            P(),
            P("sp", "tp"),
            P("sp", "tp"),
            P("sp", "tp"),
        ),
        out_specs=P("sp", "tp"),
        check_vma=False,
    )
```

```python
import functools

import jax
import jax.numpy as jnp
from jax import lax
from jax.experimental import pallas as pl
from jax.experimental.pallas import tpu as pltpu
from jax.sharding import PartitionSpec as P

HEAD = 64
CONV = 4
BLOCK = 128
EPSILON = 1e-06
MESH = pl.DeviceIdType.MESH
F32 = jnp.float32
BF16 = jnp.bfloat16
NY = 4
NZ = 8
NX = 4
NTP = 8
QROWS = 48
MROWS = 64
CHUNKS = 4
N_PUT = 224
STEPS = (
    "gz1", "spread", "dz1", "uy1", "gy0", "bA", "bB", "b0", "s1", "gz2", "gy1", "dz2", "share",
    "s2", "uy2", "gr0", "ia", "gy2", "gz3", "ib", "gr1", "dz3", "gr-1", "u21", "gr2", "gz4", "s3",
    "dz4", "gy3", "u31", "fin0", "Ai0", "dy1", "u11", "u01", "gy4", "fin1", "u32", "u22", "fin2",
    "Ai2", "fin3", "u12", "Ar0", "Ai1", "Ar2", "u02", "Af0", "u33", "gr-3", "gr-2", "dy0", "Ai3",
    "Ar1", "P0", "Bi0", "Af2", "u23", "gr4", "P2", "u13", "Bi2", "u03", "Af1", "gr3", "Ar3",
    "u24", "Br0", "u14", "dr1", "Br2", "P1", "Af3", "u04", "Bi1", "u34", "P3", "dr0", "Bf2",
    "Bi3", "Bf0", "H2", "Br1", "H0", "Br3", "D0", "E0", "Bf1", "D2", "C10", "E2", "H1", "C12",
    "Bf3", "D1", "C20", "E1", "H3", "C11", "C22", "D3", "C30", "E3", "C13", "C21", "C32", "C23",
    "C31", "C33",
)


def mark(name):
    pass


def silu(v):
    return v * (0.5 * jnp.tanh(0.5 * v) + 0.5)


def halves(lane_low, a, b):
    return jnp.where(lane_low, a, b)


def dot(a, b, ca, cb):
    return lax.dot_general(a, b, (((ca,), (cb,)), ((), ())), preferred_element_type=F32)


def split_three(v):
    hi = v.astype(BF16)
    rest = v - hi.astype(F32)
    mid = rest.astype(BF16)
    low = (rest - mid.astype(F32)).astype(BF16)
    return hi, mid, low


def log_rows(l0, l1):
    rows = []
    for part0, part1 in zip(split_three(l0), split_three(l1)):
        rows += [part0.astype(F32), part1.astype(F32)]
    rows.append(jnp.zeros((10, 128), F32))
    return jnp.concatenate(rows, axis=0).astype(BF16)


def read_logs(rows):
    v = rows.astype(F32)
    return v[0:1] + v[2:3] + v[4:5], v[1:2] + v[3:4] + v[5:6]


class Net:
    def __init__(self, send, recv):
        self.send, self.recv, self.sent = send, recv, []

    def put(self, src, dst, to):
        index = len(self.sent)
        copy = pltpu.make_async_remote_copy(
            src_ref=src, dst_ref=dst, send_sem=self.send.at[index], recv_sem=self.recv.at[index],
            device_id=to, device_id_type=MESH)
        copy.start()
        self.sent.append(copy)
        return copy


def arrive(copies):
    for copy in copies:
        copy.wait_recv()


def layer_kernel(
    step_in, extra, head_taps, taps1, taps2, gain, channel_gain, rate,
    hx, hg, k1, q1, k2t, q2t, out_w, resid, gate_w, up_w, down_w,
    out,
    raw_x, raw_g, raw_k, raw_q, raw_t, xf, gf, pad, rim_x, rim_k, rim_q, rim_t,
    ctab, cols, keys, queries, values, local, gates, upd, starts,
    msg1, buf1, msg2, buf2, msg3, enter,
    gu, dn, wo, res, rn, mx, st, nb, hidden, ps, pr, po, relay_l, relay_r, qs, from_l, from_r,
    local_sem, send_sem, recv_sem,
):
    sp = lax.axis_index("sp")
    tp = lax.axis_index("tp")
    y = lax.rem(sp, NY)
    z = sp // NY
    core = lax.rem(tp, 2)
    x = tp // 2
    n_sp = NY * NZ
    length = k1.shape[0]
    blocks = length // BLOCK
    width = gate_w.shape[1]
    depth = wo.shape[0]
    right = lax.rem(sp + 1, n_sp)
    left = lax.rem(sp + n_sp - 1, n_sp)

    def zmod(v):
        return lax.rem(v + NZ, NZ)

    def ymod(v):
        return lax.rem(v + NY, NY)

    y_peers = [{"sp": z * NY + ymod(y + j)} for j in range(1, NY)]
    z_peers = [{"sp": zmod(z + j) * NY + y} for j in range(1, NZ)]
    to_up_y, to_down_y = {"sp": z * NY + ymod(y + 1)}, {"sp": z * NY + ymod(y - 1)}
    to_up_z, to_down_z = {"sp": zmod(z + 1) * NY + y}, {"sp": zmod(z - 1) * NY + y}
    odd = lax.rem(x, 2)
    even = 1 - odd
    slot_l = lax.rem(x + NX - 1, NX) * 2 + core
    slot_r = lax.rem(x + 1, NX) * 2 + core
    slot_o = lax.rem(x + 2, NX) * 2 + core
    partner, x_right, x_left = {"tp": x * 2 + 1 - core}, {"tp": slot_r}, {"tp": slot_l}

    mark("barrier")
    wanted = [
        (gate_w, gu.at[z, y, :, 0:width]),
        (up_w, gu.at[z, y, :, width:]),
        (down_w, dn.at[z, y]),
        (hx, raw_x),
        (k1, raw_k),
        (q1, raw_q),
        (k2t, raw_t.at[0:64]),
        (q2t, raw_t.at[64:128]),
        (hg, raw_g),
        (out_w, wo.at[:, 0:256]),
        (resid, res),
    ]
    own = [pltpu.make_async_copy(a, b, local_sem.at[n]) for n, (a, b) in enumerate(wanted)]
    for copy in own:
        copy.start()

    barrier = pltpu.get_barrier_semaphore()
    greet = [{"sp": right}, {"sp": left}] + y_peers + z_peers + [partner, x_right, x_left]
    for peer in greet:
        pl.semaphore_signal(barrier, inc=1, device_id=peer, device_id_type=MESH)

    mark("tables")
    row8 = lax.broadcasted_iota(jnp.int32, (8, 128), 0)
    low = lax.broadcasted_iota(jnp.int32, (BLOCK, 128), 1) < HEAD
    low1 = lax.broadcasted_iota(jnp.int32, (1, 128), 1) < HEAD
    at_row = lax.broadcasted_iota(jnp.int32, (BLOCK, BLOCK), 0)
    at_col = lax.broadcasted_iota(jnp.int32, (BLOCK, BLOCK), 1)
    causal = at_row >= at_col
    upper = jnp.where(at_row <= at_col, 1.0, 0.0).astype(BF16)
    first_head = lax.broadcasted_iota(jnp.int32, (2, length), 0) == 0
    steps = [jax.nn.softplus(step_in[g]) for g in range(2)]
    logs = [extra[g] - steps[g] * jnp.where(first_head, rate[g, 0], rate[g, 1]) for g in range(2)]
    table = jnp.concatenate(
        [v[:, b * BLOCK : (b + 1) * BLOCK] for b in range(blocks) for v in logs + steps], axis=0)
    rows = table.shape[0]
    sums = dot(jnp.concatenate(split_three(table), axis=0), upper, 1, 0)
    sums = sums[0:rows] + sums[rows : 2 * rows] + sums[2 * rows :]
    offs = jnp.zeros((8, 1), F32)
    for b in range(blocks):
        cut = slice(8 * b, 8 * b + 8)
        c8 = jnp.where(row8 < 4, sums[cut], table[cut])
        ctab[b] = c8
        e8 = jnp.exp(jnp.where(row8 < 4, c8 + offs, 0.0))
        cols[b] = jnp.concatenate([c8, e8], axis=0).T
        offs = offs + c8[:, 127:128]
    log0 = halves(low1, offs[0:1], offs[1:2])
    log1 = halves(low1, offs[2:3], offs[3:4])
    my_logs = log_rows(log0, log1)
    for q in range(NY):
        msg1[q, QROWS:MROWS] = my_logs

    mark("barwait")
    for copy in own[:8]:
        copy.wait()
    pl.semaphore_wait(barrier, len(greet))

    net = Net(send_sem, recv_sem)
    got = {}
    have = {("gz", 0)}

    def need(*key):
        if key not in have:
            have.add(key)
            arrive(got[key if len(key) > 1 else key[0]])

    tail = pl.ds(length - 16, 16)
    rims = [
        net.put(raw_x.at[pl.ds(2 * length - 16, 16)], rim_x, {"sp": right}),
        net.put(raw_k.at[tail], rim_k, {"sp": right}),
        net.put(raw_q.at[tail], rim_q, {"sp": right}),
        net.put(raw_t.at[:, pl.ds(length - BLOCK, BLOCK)], rim_t, {"sp": right}),
    ]

    def both(ref_a, ref_b, to_a, to_b):
        return net.put(ref_a, ref_a, to_a), net.put(ref_b, ref_b, to_b)

    def gate_z(r):
        need("gz", r - 1)
        a, b = zmod(z - (r - 1)), zmod(z + (r - 1))
        if r == 4:
            got["gz", r] = both(
                gu.at[a, y, 0:32, 0:width], gu.at[b, y, 32:64, 0:width], to_up_z, to_down_z)
        else:
            got["gz", r] = both(
                gu.at[a, y, :, 0:width], gu.at[b, y, :, 0:width], to_up_z, to_down_z)

    def gate_y(*ks):
        for k in ks:
            need("gz", abs(k))
            ref = gu.at[zmod(z + k), y, :, 0:width]
            got["gy", k] = both(ref, ref, to_up_y, to_down_y)

    def gate_relay(k):
        arrive(got["gy", k])
        zz = zmod(z + k)
        got["gr", k] = both(
            gu.at[zz, ymod(y - 1), 0:32, 0:width], gu.at[zz, ymod(y + 1), 32:64, 0:width],
            to_up_y, to_down_y)

    def up_y(r):
        if r == 1:
            ref = gu.at[z, y, :, width:]
            got["uy", 1] = both(ref, ref, to_up_y, to_down_y)
        else:
            need("uy", 1)
            got["uy", 2] = both(
                gu.at[z, ymod(y - 1), 0:32, width:], gu.at[z, ymod(y + 1), 32:64, width:],
                to_up_y, to_down_y)

    def up_z(c, r):
        if r > 1:
            arrive(got["uz", c, r - 1])
        elif c > 0:
            need("uy", 2 if c == 3 else 1)
        col = ymod(y + (0, -1, 1, 2)[c])
        a, b = zmod(z - (r - 1)), zmod(z + (r - 1))
        if r == 4:
            got["uz", c, r] = both(
                gu.at[a, col, 0:32, width:], gu.at[b, col, 32:64, width:], to_up_z, to_down_z)
        else:
            got["uz", c, r] = both(
                gu.at[a, col, :, width:], gu.at[b, col, :, width:], to_up_z, to_down_z)

    def down_z(r):
        if r > 1:
            arrive(got["dz", r - 1])
        a, b = zmod(z - (r - 1)), zmod(z + (r - 1))
        if r == 4:
            got["dz", r] = both(dn.at[a, y, 0:32], dn.at[b, y, 32:64], to_up_z, to_down_z)
        else:
            got["dz", r] = both(dn.at[a, y], dn.at[b, y], to_up_z, to_down_z)

    def down_y(h):
        need("dz", 4)
        ref = dn.at[4 * h : 4 * h + 4, y]
        got["dy", h] = both(ref, ref, to_up_y, to_down_y)

    def down_relay(h):
        arrive(got["dy", h])
        got["dr", h] = both(
            dn.at[4 * h : 4 * h + 4, ymod(y - 1), 0:32], dn.at[4 * h : 4 * h + 4, ymod(y + 1), 32:64],
            to_up_y, to_down_y)

    def share():
        own[9].wait()
        own[10].wait()
        got["share"] = (
            net.put(res.at[:, even, :, 0:128], rn.at[0], x_left),
            net.put(res.at[:, even, :, 128:256], rn.at[1], x_right),
            net.put(wo.at[:, 0:128], wo.at[:, 256:384], x_left),
            net.put(wo.at[:, 128:256], wo.at[:, 384:512], x_right),
        )

    def mix_first(k):
        a, b = mx.at[k, tp, odd, 0:64], mx.at[k, tp, odd, 64:128]
        ref = mx.at[k, tp, even]
        got["A", k, 0] = (net.put(a, a, x_right), net.put(b, b, x_left),
                          net.put(ref, ref, x_right), net.put(ref, ref, x_left))
        ref = mx.at[k, tp, odd]
        got["A", k, 1] = [net.put(ref, ref, partner)]

    def mix_second(k):
        arrive(got["A", k, 0])
        a, b = mx.at[k, slot_l, even, 0:64], mx.at[k, slot_r, even, 64:128]
        got["A", k, 2] = (net.put(a, a, x_right), net.put(b, b, x_left))
        for slot in (slot_l, slot_r):
            ref = mx.at[k, slot, odd]
            got["A", k, 1] += [net.put(ref, ref, partner)]

    def mix_third(k):
        arrive(got["A", k, 2])
        ref = mx.at[k, slot_o, odd]
        got["A", k, 1] += [net.put(ref, ref, partner)]

    def tp_first(buf, key, k):
        ref = buf.at[k, tp]
        got[key, k, 0] = (net.put(ref, ref, x_right), net.put(ref, ref, x_left))
        got[key, k, 1] = [net.put(ref, ref, partner)]

    def tp_second(buf, key, k):
        arrive(got[key, k, 0])
        ref_l, ref_r = buf.at[k, slot_l], buf.at[k, slot_r]
        half = buf.shape[2] // 2
        a, b = ref_l.at[0:half], ref_r.at[half:]
        got[key, k, 2] = (net.put(a, a, x_right), net.put(b, b, x_left))
        got[key, k, 1] += [net.put(ref_l, ref_l, partner), net.put(ref_r, ref_r, partner)]

    def tp_third(buf, key, k):
        arrive(got[key, k, 2])
        ref = buf.at[k, slot_o]
        got[key, k, 1] += [net.put(ref, ref, partner)]

    def tp_done(key, k):
        arrive(got[key, k, 1])

    def spread():
        xf[...] = raw_x[...].astype(F32)
        for g in range(2):
            pad[g, 8 : 8 + length] = xf[pl.ds(g, length, stride=2)]
        pad[2, 8 : 8 + length] = raw_k[...].astype(F32)
        pad[3, 8 : 8 + length] = raw_q[...].astype(F32)
        for b in range(blocks):
            pad[4, 8 + b * BLOCK : 8 + (b + 1) * BLOCK] = raw_t[:, b * BLOCK : (b + 1) * BLOCK].astype(F32).T

    second_taps = [jnp.concatenate([taps2[k, 0:1], taps2[k, 1:2]], axis=1) for k in range(CONV)]
    all_taps = [
        [head_taps[k, 0:1] for k in range(CONV)],
        [head_taps[k, 1:2] for k in range(CONV)],
        [taps1[k, 0:1] for k in range(CONV)],
        [taps1[k, 1:2] for k in range(CONV)],
        second_taps,
    ]

    def conv(n, b):
        full = pad[n, pl.ds(pl.multiple_of(b * BLOCK, BLOCK), BLOCK + 8)]
        taps = all_taps[n]
        total = taps[0] * full[5 : 5 + BLOCK]
        for k in range(1, CONV):
            total = total + taps[k] * full[5 + k : 5 + k + BLOCK]
        return silu(total)

    def block(b, carry):
        at = pl.ds(pl.multiple_of(b * BLOCK, BLOCK), BLOCK)
        c = ctab[b]
        t = cols[b]
        key_one, mix_two = conv(2, b), conv(4, b)
        key_two = jnp.where(low, mix_two, 0.0)
        queries[1, at] = jnp.where(low, pltpu.roll(mix_two, 64, 1), 0.0).astype(BF16)
        for g, key in enumerate([key_one, key_two]):
            h = 2 * g
            v = conv(g, b) * halves(low, t[:, 4 + h : 5 + h], t[:, 5 + h : 6 + h])
            cum = halves(low, t[:, h : h + 1], t[:, h + 1 : h + 2])
            total = halves(low1, c[h : h + 1, 127:128], c[h + 1 : h + 2, 127:128])
            kb = key.astype(BF16)
            keys[g, at] = kb
            values[g, at] = v.astype(BF16)
            upd[g, b] = dot(kb, (v * jnp.exp(total - cum)).astype(BF16), 0, 0)
        return carry

    def run_blocks(lo, hi):
        lax.fori_loop(lo, hi, block, 0, unroll=2)

    def last_block():
        block(blocks - 1, 0)
        arrive(rims)
        has_left = sp > 0
        xf[0:16] = rim_x[...].astype(F32)
        for g in range(2):
            pad[g, 0:8] = jnp.where(has_left, xf[pl.ds(g, 8, stride=2)], 0.0)
        pad[2, 0:8] = jnp.where(has_left, rim_k[...].astype(F32)[8:16], 0.0)
        pad[3, 0:8] = jnp.where(has_left, rim_q[...].astype(F32)[8:16], 0.0)
        pad[4, 0:8] = jnp.where(has_left, rim_t[...].astype(F32).T[BLOCK - 8 :], 0.0)
        block(0, 0)
        ends = []
        for g in range(2):
            h = 2 * g
            state = jnp.zeros((BLOCK, 128), F32)
            for b in range(blocks):
                c = ctab[b]
                total = halves(low1, c[h : h + 1, 127:128], c[h + 1 : h + 2, 127:128])
                starts[g, b] = state.astype(BF16)
                state = state * jnp.exp(total) + upd[g, b]
            ends.append(state)
        full = jnp.concatenate([ends[0], ends[1][0:64]], axis=0).astype(BF16)
        for q in range(NY):
            msg1[q, 0:QROWS] = full[q * QROWS : (q + 1) * QROWS]

    quarter = y * QROWS + lax.broadcasted_iota(jnp.int32, (QROWS, 128), 0)
    group_one = quarter < 128

    def factor(l0, l1):
        return jnp.where(group_one, jnp.exp(l0), jnp.exp(l1))

    def stage1():
        got["s1"] = []
        for j in range(1, NY):
            to = ymod(y + j)
            got["s1"].append(net.put(msg1.at[to], buf1.at[y], {"sp": z * NY + to}))
        buf1[y] = msg1[y]

    before = []

    def stage2():
        arrive(got["s1"])
        run = jnp.zeros((QROWS, 128), F32)
        sum0 = jnp.zeros((1, 128), F32)
        sum1 = jnp.zeros((1, 128), F32)
        for j in range(NY):
            before.append((run, sum0, sum1))
            l0, l1 = read_logs(buf1[j, QROWS:MROWS])
            run = run * factor(l0, l1) + buf1[j, 0:QROWS].astype(F32)
            sum0, sum1 = sum0 + l0, sum1 + l1
        msg2[0:QROWS] = run.astype(BF16)
        msg2[QROWS:MROWS] = log_rows(sum0, sum1)
        got["s2"] = []
        for j in range(1, NZ):
            got["s2"].append(net.put(msg2, buf2.at[z], {"sp": zmod(z + j) * NY + y}))
        buf2[z] = msg2[...]

    def stage3():
        arrive(got["s2"])
        run = jnp.zeros((QROWS, 128), F32)
        for j in range(NZ):
            l0, l1 = read_logs(buf2[j, QROWS:MROWS])
            new = run * factor(l0, l1) + buf2[j, 0:QROWS].astype(F32)
            run = jnp.where(j < z, new, run)
        for j in range(NY):
            part, l0, l1 = before[j]
            msg3[j] = (run * factor(l0, l1) + part).astype(BF16)
        mine = pl.ds(pl.multiple_of(y * QROWS, 16), QROWS)
        got["s3"] = []
        for j in range(1, NY):
            to = ymod(y + j)
            got["s3"].append(net.put(msg3.at[to], enter.at[mine], {"sp": z * NY + to}))
        enter[mine] = msg3[y]

    def inside(b, carry):
        at = pl.ds(pl.multiple_of(b * BLOCK, BLOCK), BLOCK)
        t = cols[b]
        c = ctab[b]
        queries[0, at] = conv(3, b).astype(BF16)
        for g in range(2):
            h = 2 * g
            qb, v = queries[g, at], values[g, at]
            scores = dot(qb, keys[g, at], 1, 1)
            weights = []
            for j in range(2):
                span = t[:, h + j : h + j + 1] - c[h + j : h + j + 1]
                weights.append((jnp.exp(jnp.where(causal, span, -jnp.inf)) * scores).astype(BF16))
            zero = jnp.zeros_like(v)
            two = jnp.concatenate([jnp.where(low, v, zero), jnp.where(low, zero, v)], axis=0)
            cum = halves(low, t[:, h : h + 1], t[:, h + 1 : h + 2])
            local[g, at] = dot(jnp.concatenate(weights, axis=1), two, 1, 0) + dot(
                qb, starts[g, b], 1, 0) * jnp.exp(cum)
        return carry

    def inside_a():
        own[8].wait()
        gf[...] = raw_g[...].astype(F32)
        for g in range(2):
            gates[g] = silu(gf[pl.ds(g, length, stride=2)])
        lax.fori_loop(0, blocks // 2, inside, 0, unroll=2)

    def inside_b():
        lax.fori_loop(blocks // 2, blocks, inside, 0, unroll=2)

    per = blocks // CHUNKS
    tokens = BLOCK * per

    def finish(k):
        need("s3")
        for i in range(per):
            b = k * per + i
            at = slice(b * BLOCK, (b + 1) * BLOCK)
            t = cols[b]
            for g in range(2):
                h = 8 + 2 * g
                if g == 0:
                    entering = enter[0:128]
                else:
                    entering = jnp.concatenate([enter[128:192], jnp.zeros((64, 128), BF16)], axis=0)
                m = local[g, at] + dot(queries[g, at], entering, 1, 0) * halves(
                    low, t[:, h : h + 1], t[:, h + 1 : h + 2])
                m = m * gates[g, at]
                square = m * m
                s0 = jnp.sum(jnp.where(low, square, 0.0), axis=1, keepdims=True)
                s1 = jnp.sum(jnp.where(low, 0.0, square), axis=1, keepdims=True)
                scale = lax.rsqrt(halves(low, s0, s1) * (1.0 / HEAD) + EPSILON)
                mx[k, tp, i, :, g * 128 : (g + 1) * 128] = (
                    m * scale * gain[g : g + 1]).astype(BF16)

    def project(k):
        need("share")
        tp_done("A", k)
        lhs = jnp.concatenate(
            [mx[k, s, odd, :, g * 128 : (g + 1) * 128] for g in range(2) for s in range(NTP)], axis=1)
        base = jnp.concatenate([res[k, odd], rn[0, k], rn[1, k]], axis=1)
        st[k, tp] = (dot(lhs, wo[...], 1, 0) + base.astype(F32)).astype(BF16)

    def stream_of(k, q, xx, cc):
        if xx % 2 == q:
            return st[k, 2 * xx + cc, :, 0:256]
        return jnp.concatenate(
            [st[k, 2 * ((xx - 1) % NX) + cc, :, 256:384], st[k, 2 * ((xx + 1) % NX) + cc, :, 384:512]],
            axis=1)

    def norm_hidden(k):
        tp_done("B", k)
        for j in (0, 1, -1, 2, -2, 3, -3, 4):
            need("gr", j)
        for c in range(NY):
            need("uz", c, 4)
        for q in range(2):
            square = jnp.zeros((BLOCK, 128), F32)
            for slot in (2 * q, 2 * q + 1, 2 * q + 4, 2 * q + 5):
                v = st[k, slot].astype(F32)
                for c in range(4):
                    piece = v[:, c * 128 : (c + 1) * 128]
                    square = square + piece * piece
            scale = lax.rsqrt(jnp.sum(square, axis=1, keepdims=True) * (1.0 / depth) + EPSILON)
            for slot in range(NTP):
                cut = slice(slot * 256, (slot + 1) * 256)
                v = stream_of(k, q, slot // 2, slot % 2).astype(F32)
                nb[q * BLOCK : (q + 1) * BLOCK, cut] = (v * scale * channel_gain[:, cut]).astype(BF16)
        pair = dot(nb[...], gu[...].reshape(depth, 2 * width), 1, 0)
        hidden[k] = (silu(pair[:, :width]) * pair[:, width:]).astype(BF16)

    order = (2, 3, 1, 0)
    dests = {k: lax.rem(x + k, NX) * 2 for k in order}

    def down(k, d):
        return dot(hidden[k], dn[d].reshape(256, width), 1, 1).astype(BF16)

    def down_partner(k):
        need("dr", 0)
        need("dr", 1)
        for j in order:
            ps[k, j] = down(k, dests[j] + 1 - core)
            got["P", k, j] = net.put(ps.at[k, j], pr.at[k, j], partner)

    def down_own(k):
        for j in order:
            po[k, j] = down(k, dests[j] + core)

    def pair_sum(k, j):
        got["P", k, j].wait_recv()
        return po[k, j].astype(F32) + pr[k, j].astype(F32)

    mid = tokens // 2

    def sum_first(k):
        qs[k, 2] = pair_sum(k, 2).astype(BF16)
        got["C1", k] = (net.put(qs.at[k, 2, 0:mid], relay_r.at[k], x_left),
                        net.put(qs.at[k, 2, mid:], relay_l.at[k], x_right))

    def sum_second(k):
        to_left, to_right = pair_sum(k, 3), pair_sum(k, 1)
        arrive(got["C1", k])
        qs[k, 3, 0:mid] = (to_left[0:mid] + relay_r[k].astype(F32)).astype(BF16)
        qs[k, 3, mid:] = to_left[mid:].astype(BF16)
        qs[k, 1, 0:mid] = to_right[0:mid].astype(BF16)
        qs[k, 1, mid:] = (to_right[mid:] + relay_l[k].astype(F32)).astype(BF16)
        got["C2", k] = (net.put(qs.at[k, 3], from_r.at[k], x_left),
                        net.put(qs.at[k, 1], from_l.at[k], x_right))

    def sum_third(k):
        total = pair_sum(k, 0)
        arrive(got["C2", k])
        total = total + from_l[k].astype(F32) + from_r[k].astype(F32)
        mine = st[k, tp, :, 0:256].astype(F32)
        other = jnp.concatenate(
            [st[k, slot_l, :, 256:384], st[k, slot_r, :, 384:512]], axis=1).astype(F32)
        for q in range(2):
            at = k * tokens + q * BLOCK
            stream = jnp.where(odd == q, mine, other)
            out[at : at + BLOCK] = (
                stream + 0.5 * total[q * BLOCK : (q + 1) * BLOCK]).astype(BF16)

    run = {
        "spread": spread,
        "bA": lambda: run_blocks(1, 5),
        "bB": lambda: run_blocks(5, 7),
        "b0": last_block,
        "s1": stage1,
        "s2": stage2,
        "s3": stage3,
        "ia": inside_a,
        "ib": inside_b,
        "gy0": lambda: gate_y(0),
        "gy1": lambda: gate_y(1, -1),
        "gy2": lambda: gate_y(2, -2),
        "gy3": lambda: gate_y(3, -3),
        "gy4": lambda: gate_y(4),
        "uy1": lambda: up_y(1),
        "uy2": lambda: up_y(2),
        "dy0": lambda: down_y(0),
        "dy1": lambda: down_y(1),
        "dr0": lambda: down_relay(0),
        "dr1": lambda: down_relay(1),
        "share": share,
    }
    for r in (1, 2, 3, 4):
        run[f"gz{r}"] = functools.partial(gate_z, r)
        for c in range(NY):
            run[f"u{c}{r}"] = functools.partial(up_z, c, r)
        run[f"dz{r}"] = functools.partial(down_z, r)
    for k in (0, 1, -1, 2, -2, 3, -3, 4):
        run[f"gr{k}"] = functools.partial(gate_relay, k)
    for k in range(CHUNKS):
        run[f"fin{k}"] = functools.partial(finish, k)
        run[f"P{k}"] = functools.partial(project, k)
        run[f"H{k}"] = functools.partial(norm_hidden, k)
        run[f"D{k}"] = functools.partial(down_partner, k)
        run[f"E{k}"] = functools.partial(down_own, k)
        run[f"C1{k}"] = functools.partial(sum_first, k)
        run[f"C2{k}"] = functools.partial(sum_second, k)
        run[f"C3{k}"] = functools.partial(sum_third, k)
        run[f"Ai{k}"] = functools.partial(mix_first, k)
        run[f"Ar{k}"] = functools.partial(mix_second, k)
        run[f"Af{k}"] = functools.partial(mix_third, k)
        run[f"Bi{k}"] = functools.partial(tp_first, st, "B", k)
        run[f"Br{k}"] = functools.partial(tp_second, st, "B", k)
        run[f"Bf{k}"] = functools.partial(tp_third, st, "B", k)
    for name in STEPS:
        mark(name)
        run.pop(name)()
    assert not run

    mark("sends")
    for copy in net.sent:
        copy.wait_send()


def layer(vmem_args, smem_arg, hbm_args):
    length = hbm_args[2].shape[0]
    blocks = length // BLOCK
    tokens = length // CHUNKS
    width = hbm_args[8].shape[1]
    vmem = pl.BlockSpec(memory_space=pltpu.VMEM)
    dma = pltpu.SemaphoreType.DMA

    def bf(*shape):
        return pltpu.VMEM(shape, BF16)

    def fl(*shape):
        return pltpu.VMEM(shape, F32)

    return pl.pallas_call(
        layer_kernel,
        out_shape=jax.ShapeDtypeStruct((length, 256), BF16),
        in_specs=[vmem] * len(vmem_args)
        + [pl.BlockSpec(memory_space=pltpu.SMEM)]
        + [pl.BlockSpec(memory_space=pl.ANY)] * len(hbm_args),
        out_specs=vmem,
        scratch_shapes=[
            bf(2 * length, 128), bf(2 * length, 128), bf(length, 128), bf(length, 128),
            bf(128, length), fl(2 * length, 128), fl(2 * length, 128), fl(5, length + 8, 128),
            bf(16, 128), bf(16, 128), bf(16, 128), bf(128, 128),
            fl(blocks, 8, 128), fl(blocks, BLOCK, 16),
            bf(2, length, 128), bf(2, length, 128), bf(2, length, 128),
            fl(2, length, 128), fl(2, length, 128),
            fl(2, blocks, 128, 128), bf(2, blocks, 128, 128),
            bf(NY, MROWS, 128), bf(NY, MROWS, 128), bf(MROWS, 128), bf(NZ, MROWS, 128),
            bf(NY, QROWS, 128), bf(NY * QROWS, 128),
            bf(NZ, NY, 64, 2 * width), bf(NZ, NY, 64, width), bf(2048, 512),
            bf(CHUNKS, 2, BLOCK, 256), bf(2, CHUNKS, BLOCK, 128),
            bf(CHUNKS, NTP, 2, BLOCK, 256), bf(CHUNKS, NTP, BLOCK, 512),
            bf(tokens, 2048), bf(CHUNKS, tokens, width),
            bf(CHUNKS, NX, tokens, 256), bf(CHUNKS, NX, tokens, 256), bf(CHUNKS, NX, tokens, 256),
            bf(CHUNKS, tokens // 2, 256), bf(CHUNKS, tokens // 2, 256),
            bf(CHUNKS, NX, tokens, 256), bf(CHUNKS, tokens, 256), bf(CHUNKS, tokens, 256),
            dma((11,)), dma((N_PUT,)), dma((N_PUT,)),
        ],
        compiler_params=pltpu.CompilerParams(
            collective_id=0, has_side_effects=True, vmem_limit_bytes=58 * 1024 * 1024),
        cost_estimate=pl.CostEstimate(
            flops=12_000_000_000, bytes_accessed=8_000_000, transcendentals=4_000_000),
        name="layer",
    )(*vmem_args, smem_arg, *hbm_args)


def shards(
    grouped_head_inputs,
    head_gate_inputs,
    unsmoothed_step,
    head_decay_rate,
    extra_log_decay,
    first_group_keys,
    first_group_queries,
    second_group_keys,
    second_group_queries,
    head_input_filter,
    first_group_filter,
    second_group_filter,
    head_norm_gain,
    output_weight,
    residual,
    channel_norm_gain,
    channel_gate_weight,
    channel_up_weight,
    channel_down_weight,
):
    length = grouped_head_inputs.shape[0]
    return layer(
        (
            unsmoothed_step.transpose(1, 2, 0),
            extra_log_decay.transpose(1, 2, 0),
            head_input_filter,
            first_group_filter,
            second_group_filter,
            head_norm_gain,
            channel_norm_gain[None],
        ),
        head_decay_rate,
        (
            grouped_head_inputs.reshape(2 * length, 128),
            head_gate_inputs.reshape(2 * length, 128),
            first_group_keys,
            first_group_queries,
            second_group_keys.T,
            second_group_queries.T,
            output_weight.reshape(-1, output_weight.shape[2]),
            residual.reshape(CHUNKS, 2, BLOCK, residual.shape[1]),
            channel_gate_weight,
            channel_up_weight,
            channel_down_weight,
        ),
    )


def solution(mesh):
    return jax.shard_map(
        shards,
        mesh=mesh,
        in_specs=(
            P("sp", None, "tp"),
            P("sp", None, "tp"),
            P("sp", None, "tp"),
            P(None, "tp"),
            P("sp", None, "tp"),
            P("sp", None),
            P("sp", None),
            P("sp", None),
            P("sp", None),
            P(None, None, "tp"),
            P(),
            P(),
            P(None, "tp"),
            P(None, None, "tp"),
            P("sp", "tp"),
            P(),
            P("sp", "tp"),
            P("sp", "tp"),
            P("sp", "tp"),
        ),
        out_specs=P("sp", "tp"),
        check_vma=False,
    )
```

```python
import functools

import jax
import jax.numpy as jnp
from jax import lax
from jax.experimental import pallas as pl
from jax.experimental.pallas import tpu as pltpu
from jax.sharding import PartitionSpec as P

HEAD = 64
CONV = 4
BLOCK = 128
EPSILON = 1e-06
MESH = pl.DeviceIdType.MESH
F32 = jnp.float32
BF16 = jnp.bfloat16
NY = 4
NZ = 8
NX = 4
NTP = 8
QROWS = 48
MROWS = 64
CHUNKS = 4
N_PUT = 236
SPLIT = 512
STEPS = (
    "gz1", "ey1", "dz1", "spread", "gy0", "uy1", "u01", "bA", "bB", "b0", "share", "gz2", "s1",
    "dz2", "ey2", "gr0", "gy1", "s2", "ia", "dz3", "gz3", "ez1", "uy2", "gy2", "gr1", "u21", "ib",
    "dz4", "u02", "s3", "gr-1", "u11", "gy3", "fin0", "Ai0", "fin1", "fin2", "dy1", "gr-2", "u22",
    "fin3", "gr2", "u31", "dy0", "Ai1", "Ar0", "Ai2", "gr3", "gz4", "gr-3", "u12", "Ar1", "u03",
    "Ai3", "ez2", "Af0", "P0", "Ar2", "u32", "Bi0", "gy4", "Af1", "u23", "P1", "Af2", "Bi1",
    "Ar3", "dr1", "u13", "u33", "Br0", "u24", "P2", "Br1", "u14", "Bi2", "ez3", "u04", "Af3",
    "gr4", "P3", "dr0", "u34", "Bi3", "Bf0", "Bf1", "ez4", "N0", "N1", "Br2", "H1", "D1", "Br3",
    "H0", "Bf2", "D0", "E1", "C11", "N2", "E0", "Bf3", "C10", "H2", "D2", "C21", "N3", "E2",
    "C12", "H3", "C20", "D3", "C31", "E3", "C13", "C22", "C30", "C23", "C32", "C33",
)


def mark(name):
    pass


def silu(v):
    return v * (0.5 * jnp.tanh(0.5 * v) + 0.5)


def halves(lane_low, a, b):
    return jnp.where(lane_low, a, b)


def dot(a, b, ca, cb):
    return lax.dot_general(a, b, (((ca,), (cb,)), ((), ())), preferred_element_type=F32)


def split_three(v):
    hi = v.astype(BF16)
    rest = v - hi.astype(F32)
    mid = rest.astype(BF16)
    low = (rest - mid.astype(F32)).astype(BF16)
    return hi, mid, low


def log_rows(l0, l1):
    rows = []
    for part0, part1 in zip(split_three(l0), split_three(l1)):
        rows += [part0.astype(F32), part1.astype(F32)]
    rows.append(jnp.zeros((10, 128), F32))
    return jnp.concatenate(rows, axis=0).astype(BF16)


def read_logs(rows):
    v = rows.astype(F32)
    return v[0:1] + v[2:3] + v[4:5], v[1:2] + v[3:4] + v[5:6]


class Net:
    def __init__(self, send, recv):
        self.send, self.recv, self.sent = send, recv, []

    def put(self, src, dst, to):
        index = len(self.sent)
        copy = pltpu.make_async_remote_copy(
            src_ref=src, dst_ref=dst, send_sem=self.send.at[index], recv_sem=self.recv.at[index],
            device_id=to, device_id_type=MESH)
        copy.start()
        self.sent.append(copy)
        return copy


def arrive(copies):
    for copy in copies:
        copy.wait_recv()


def layer_kernel(
    step_in, extra, head_taps, taps1, taps2, gain, channel_gain, rate,
    hx, hg, k1, q1, k2t, q2t, out_w, resid, gate_w, up_w, down_w,
    out,
    raw_x, raw_g, raw_k, raw_q, raw_t, xf, gf, pad, rim_x, rim_k, rim_q, rim_t,
    ctab, cols, keys, queries, values, local, gates, upd, starts,
    msg1, buf1, msg2, buf2, msg3, enter,
    gu, dn, wo, res, rn, mx, st, nb, hidden, ps, pr, po, relay_l, relay_r, qs, from_l, from_r,
    local_sem, send_sem, recv_sem,
):
    sp = lax.axis_index("sp")
    tp = lax.axis_index("tp")
    y = lax.rem(sp, NY)
    z = sp // NY
    core = lax.rem(tp, 2)
    x = tp // 2
    n_sp = NY * NZ
    length = k1.shape[0]
    blocks = length // BLOCK
    width = gate_w.shape[1]
    depth = wo.shape[0]
    right = lax.rem(sp + 1, n_sp)
    left = lax.rem(sp + n_sp - 1, n_sp)

    def zmod(v):
        return lax.rem(v + NZ, NZ)

    def ymod(v):
        return lax.rem(v + NY, NY)

    y_peers = [{"sp": z * NY + ymod(y + j)} for j in range(1, NY)]
    z_peers = [{"sp": zmod(z + j) * NY + y} for j in range(1, NZ)]
    to_up_y, to_down_y = {"sp": z * NY + ymod(y + 1)}, {"sp": z * NY + ymod(y - 1)}
    to_up_z, to_down_z = {"sp": zmod(z + 1) * NY + y}, {"sp": zmod(z - 1) * NY + y}
    odd = lax.rem(x, 2)
    even = 1 - odd
    slot_l = lax.rem(x + NX - 1, NX) * 2 + core
    slot_r = lax.rem(x + 1, NX) * 2 + core
    slot_o = lax.rem(x + 2, NX) * 2 + core
    partner, x_right, x_left = {"tp": x * 2 + 1 - core}, {"tp": slot_r}, {"tp": slot_l}

    mark("barrier")
    wanted = [
        (gate_w, gu.at[z, y, :, 0:width]),
        (up_w, gu.at[z, y, :, width:]),
        (down_w, dn.at[z, y]),
        (hx, raw_x),
        (k1, raw_k),
        (q1, raw_q),
        (k2t, raw_t.at[0:64]),
        (q2t, raw_t.at[64:128]),
        (hg, raw_g),
        (out_w, wo.at[:, 0:256]),
        (resid, res),
    ]
    own = [pltpu.make_async_copy(a, b, local_sem.at[n]) for n, (a, b) in enumerate(wanted)]
    for copy in own:
        copy.start()

    barrier = pltpu.get_barrier_semaphore()
    greet = [{"sp": right}, {"sp": left}] + y_peers + z_peers + [partner, x_right, x_left]
    for peer in greet:
        pl.semaphore_signal(barrier, inc=1, device_id=peer, device_id_type=MESH)

    mark("tables")
    row8 = lax.broadcasted_iota(jnp.int32, (8, 128), 0)
    low = lax.broadcasted_iota(jnp.int32, (BLOCK, 128), 1) < HEAD
    low1 = lax.broadcasted_iota(jnp.int32, (1, 128), 1) < HEAD
    at_row = lax.broadcasted_iota(jnp.int32, (BLOCK, BLOCK), 0)
    at_col = lax.broadcasted_iota(jnp.int32, (BLOCK, BLOCK), 1)
    causal = at_row >= at_col
    upper = jnp.where(at_row <= at_col, 1.0, 0.0).astype(BF16)
    first_head = lax.broadcasted_iota(jnp.int32, (2, length), 0) == 0
    steps = [jax.nn.softplus(step_in[g]) for g in range(2)]
    logs = [extra[g] - steps[g] * jnp.where(first_head, rate[g, 0], rate[g, 1]) for g in range(2)]
    table = jnp.concatenate(
        [v[:, b * BLOCK : (b + 1) * BLOCK] for b in range(blocks) for v in logs + steps], axis=0)
    rows = table.shape[0]
    sums = dot(jnp.concatenate(split_three(table), axis=0), upper, 1, 0)
    sums = sums[0:rows] + sums[rows : 2 * rows] + sums[2 * rows :]
    offs = jnp.zeros((8, 1), F32)
    for b in range(blocks):
        cut = slice(8 * b, 8 * b + 8)
        c8 = jnp.where(row8 < 4, sums[cut], table[cut])
        ctab[b] = c8
        e8 = jnp.exp(jnp.where(row8 < 4, c8 + offs, 0.0))
        cols[b] = jnp.concatenate([c8, e8], axis=0).T
        offs = offs + c8[:, 127:128]
    log0 = halves(low1, offs[0:1], offs[1:2])
    log1 = halves(low1, offs[2:3], offs[3:4])
    my_logs = log_rows(log0, log1)
    for q in range(NY):
        msg1[q, QROWS:MROWS] = my_logs

    mark("barwait")
    for copy in own[:8]:
        copy.wait()
    pl.semaphore_wait(barrier, len(greet))

    net = Net(send_sem, recv_sem)
    got = {}
    have = {("gz", 0)}

    def need(*key):
        if key not in have:
            have.add(key)
            arrive(got[key if len(key) > 1 else key[0]])

    tail = pl.ds(length - 16, 16)
    rims = [
        net.put(raw_x.at[pl.ds(2 * length - 16, 16)], rim_x, {"sp": right}),
        net.put(raw_k.at[tail], rim_k, {"sp": right}),
        net.put(raw_q.at[tail], rim_q, {"sp": right}),
        net.put(raw_t.at[:, pl.ds(length - BLOCK, BLOCK)], rim_t, {"sp": right}),
    ]

    def both(ref_a, ref_b, to_a, to_b):
        return net.put(ref_a, ref_a, to_a), net.put(ref_b, ref_b, to_b)

    def gate_z(r):
        need("gz", r - 1)
        a, b = zmod(z - (r - 1)), zmod(z + (r - 1))
        if r == 4:
            got["gz", r] = both(
                gu.at[a, y, 0:32, 0:width], gu.at[b, y, 32:64, 0:width], to_up_z, to_down_z)
        else:
            got["gz", r] = both(
                gu.at[a, y, :, 0:width], gu.at[b, y, :, 0:width], to_up_z, to_down_z)

    def gate_y(*ks):
        for k in ks:
            need("gz", abs(k))
            ref = gu.at[zmod(z + k), y, :, 0:width]
            got["gy", k] = both(ref, ref, to_up_y, to_down_y)

    def gate_relay(k):
        arrive(got["gy", k])
        zz = zmod(z + k)
        got["gr", k] = both(
            gu.at[zz, ymod(y - 1), 0:32, 0:width], gu.at[zz, ymod(y + 1), 32:64, 0:width],
            to_up_y, to_down_y)

    def up_y(r):
        if r == 1:
            ref = gu.at[z, y, :, width:]
            got["uy", 1] = both(ref, ref, to_up_y, to_down_y)
        else:
            need("uy", 1)
            got["uy", 2] = both(
                gu.at[z, ymod(y - 1), 0:32, width:], gu.at[z, ymod(y + 1), 32:64, width:],
                to_up_y, to_down_y)

    def up_z(c, r):
        if r > 1:
            arrive(got["uz", c, r - 1])
        elif c > 0:
            need("uy", 2 if c == 3 else 1)
        col = ymod(y + (0, -1, 1, 2)[c])
        a, b = zmod(z - (r - 1)), zmod(z + (r - 1))
        if r == 4:
            got["uz", c, r] = both(
                gu.at[a, col, 0:32, width:], gu.at[b, col, 32:64, width:], to_up_z, to_down_z)
        else:
            got["uz", c, r] = both(
                gu.at[a, col, :, width:], gu.at[b, col, :, width:], to_up_z, to_down_z)

    def down_z(r):
        if r > 1:
            arrive(got["dz", r - 1])
        a, b = zmod(z - (r - 1)), zmod(z + (r - 1))
        if r == 4:
            got["dz", r] = both(
                dn.at[a, y, 0:32, 0:SPLIT], dn.at[b, y, 32:64, 0:SPLIT], to_up_z, to_down_z)
        else:
            got["dz", r] = both(
                dn.at[a, y, :, 0:SPLIT], dn.at[b, y, :, 0:SPLIT], to_up_z, to_down_z)

    def down_y(h):
        need("dz", 4)
        ref = dn.at[4 * h : 4 * h + 4, y, :, 0:SPLIT]
        got["dy", h] = both(ref, ref, to_up_y, to_down_y)

    def down_relay(h):
        arrive(got["dy", h])
        part = pl.ds(4 * h, 4)
        got["dr", h] = both(
            dn.at[part, ymod(y - 1), 0:32, 0:SPLIT], dn.at[part, ymod(y + 1), 32:64, 0:SPLIT],
            to_up_y, to_down_y)

    def rest_y(r):
        if r == 1:
            ref = dn.at[z, y, :, SPLIT:]
            got["ey", 1] = both(ref, ref, to_up_y, to_down_y)
        else:
            need("ey", 1)
            got["ey", 2] = both(
                dn.at[z, ymod(y - 1), 0:32, SPLIT:], dn.at[z, ymod(y + 1), 32:64, SPLIT:],
                to_up_y, to_down_y)

    def rest_z(r):
        if r == 1:
            need("ey", 2)
        else:
            arrive(got["ez", r - 1])
        a, b = zmod(z - (r - 1)), zmod(z + (r - 1))
        if r == 4:
            got["ez", r] = both(
                dn.at[a, 0:2, :, SPLIT:], dn.at[b, 2:4, :, SPLIT:], to_up_z, to_down_z)
        else:
            got["ez", r] = both(
                dn.at[a, :, :, SPLIT:], dn.at[b, :, :, SPLIT:], to_up_z, to_down_z)

    def share():
        own[9].wait()
        own[10].wait()
        got["share"] = (
            net.put(res.at[:, even, :, 0:128], rn.at[0], x_left),
            net.put(res.at[:, even, :, 128:256], rn.at[1], x_right),
            net.put(wo.at[:, 0:128], wo.at[:, 256:384], x_left),
            net.put(wo.at[:, 128:256], wo.at[:, 384:512], x_right),
        )

    def mix_first(k):
        a, b = mx.at[k, tp, odd, 0:64], mx.at[k, tp, odd, 64:128]
        ref = mx.at[k, tp, even]
        got["A", k, 0] = (net.put(a, a, x_right), net.put(b, b, x_left),
                          net.put(ref, ref, x_right), net.put(ref, ref, x_left))
        ref = mx.at[k, tp, odd]
        got["A", k, 1] = [net.put(ref, ref, partner)]

    def mix_second(k):
        arrive(got["A", k, 0])
        a, b = mx.at[k, slot_l, even, 0:64], mx.at[k, slot_r, even, 64:128]
        got["A", k, 2] = (net.put(a, a, x_right), net.put(b, b, x_left))
        for slot in (slot_l, slot_r):
            ref = mx.at[k, slot, odd]
            got["A", k, 1] += [net.put(ref, ref, partner)]

    def mix_third(k):
        arrive(got["A", k, 2])
        ref = mx.at[k, slot_o, odd]
        got["A", k, 1] += [net.put(ref, ref, partner)]

    def tp_first(buf, key, k):
        ref = buf.at[k, tp]
        got[key, k, 0] = (net.put(ref, ref, x_right), net.put(ref, ref, x_left))
        got[key, k, 1] = [net.put(ref, ref, partner)]

    def tp_second(buf, key, k):
        arrive(got[key, k, 0])
        ref_l, ref_r = buf.at[k, slot_l], buf.at[k, slot_r]
        half = buf.shape[2] // 2
        a, b = ref_l.at[0:half], ref_r.at[half:]
        got[key, k, 2] = (net.put(a, a, x_right), net.put(b, b, x_left))
        got[key, k, 1] += [net.put(ref_l, ref_l, partner), net.put(ref_r, ref_r, partner)]

    def tp_third(buf, key, k):
        arrive(got[key, k, 2])
        ref = buf.at[k, slot_o]
        got[key, k, 1] += [net.put(ref, ref, partner)]

    def tp_done(key, k):
        arrive(got[key, k, 1])

    def spread():
        xf[...] = raw_x[...].astype(F32)
        for g in range(2):
            pad[g, 8 : 8 + length] = xf[pl.ds(g, length, stride=2)]
        pad[2, 8 : 8 + length] = raw_k[...].astype(F32)
        pad[3, 8 : 8 + length] = raw_q[...].astype(F32)
        for b in range(blocks):
            pad[4, 8 + b * BLOCK : 8 + (b + 1) * BLOCK] = raw_t[:, b * BLOCK : (b + 1) * BLOCK].astype(F32).T

    second_taps = [jnp.concatenate([taps2[k, 0:1], taps2[k, 1:2]], axis=1) for k in range(CONV)]
    all_taps = [
        [head_taps[k, 0:1] for k in range(CONV)],
        [head_taps[k, 1:2] for k in range(CONV)],
        [taps1[k, 0:1] for k in range(CONV)],
        [taps1[k, 1:2] for k in range(CONV)],
        second_taps,
    ]

    def conv(n, b):
        full = pad[n, pl.ds(pl.multiple_of(b * BLOCK, BLOCK), BLOCK + 8)]
        taps = all_taps[n]
        total = taps[0] * full[5 : 5 + BLOCK]
        for k in range(1, CONV):
            total = total + taps[k] * full[5 + k : 5 + k + BLOCK]
        return silu(total)

    def block(b, carry):
        at = pl.ds(pl.multiple_of(b * BLOCK, BLOCK), BLOCK)
        c = ctab[b]
        t = cols[b]
        key_one, mix_two = conv(2, b), conv(4, b)
        key_two = jnp.where(low, mix_two, 0.0)
        queries[1, at] = jnp.where(low, pltpu.roll(mix_two, 64, 1), 0.0).astype(BF16)
        for g, key in enumerate([key_one, key_two]):
            h = 2 * g
            v = conv(g, b) * halves(low, t[:, 4 + h : 5 + h], t[:, 5 + h : 6 + h])
            cum = halves(low, t[:, h : h + 1], t[:, h + 1 : h + 2])
            total = halves(low1, c[h : h + 1, 127:128], c[h + 1 : h + 2, 127:128])
            kb = key.astype(BF16)
            keys[g, at] = kb
            values[g, at] = v.astype(BF16)
            upd[g, b] = dot(kb, (v * jnp.exp(total - cum)).astype(BF16), 0, 0)
        return carry

    def run_blocks(lo, hi):
        lax.fori_loop(lo, hi, block, 0, unroll=2)

    def last_block():
        block(blocks - 1, 0)
        arrive(rims)
        has_left = sp > 0
        xf[0:16] = rim_x[...].astype(F32)
        for g in range(2):
            pad[g, 0:8] = jnp.where(has_left, xf[pl.ds(g, 8, stride=2)], 0.0)
        pad[2, 0:8] = jnp.where(has_left, rim_k[...].astype(F32)[8:16], 0.0)
        pad[3, 0:8] = jnp.where(has_left, rim_q[...].astype(F32)[8:16], 0.0)
        pad[4, 0:8] = jnp.where(has_left, rim_t[...].astype(F32).T[BLOCK - 8 :], 0.0)
        block(0, 0)
        ends = []
        for g in range(2):
            h = 2 * g
            state = jnp.zeros((BLOCK, 128), F32)
            for b in range(blocks):
                c = ctab[b]
                total = halves(low1, c[h : h + 1, 127:128], c[h + 1 : h + 2, 127:128])
                starts[g, b] = state.astype(BF16)
                state = state * jnp.exp(total) + upd[g, b]
            ends.append(state)
        full = jnp.concatenate([ends[0], ends[1][0:64]], axis=0).astype(BF16)
        for q in range(NY):
            msg1[q, 0:QROWS] = full[q * QROWS : (q + 1) * QROWS]

    quarter = y * QROWS + lax.broadcasted_iota(jnp.int32, (QROWS, 128), 0)
    group_one = quarter < 128

    def factor(l0, l1):
        return jnp.where(group_one, jnp.exp(l0), jnp.exp(l1))

    def stage1():
        got["s1"] = []
        for j in range(1, NY):
            to = ymod(y + j)
            got["s1"].append(net.put(msg1.at[to], buf1.at[y], {"sp": z * NY + to}))
        buf1[y] = msg1[y]

    before = []

    def stage2():
        arrive(got["s1"])
        run = jnp.zeros((QROWS, 128), F32)
        sum0 = jnp.zeros((1, 128), F32)
        sum1 = jnp.zeros((1, 128), F32)
        for j in range(NY):
            before.append((run, sum0, sum1))
            l0, l1 = read_logs(buf1[j, QROWS:MROWS])
            run = run * factor(l0, l1) + buf1[j, 0:QROWS].astype(F32)
            sum0, sum1 = sum0 + l0, sum1 + l1
        msg2[0:QROWS] = run.astype(BF16)
        msg2[QROWS:MROWS] = log_rows(sum0, sum1)
        got["s2"] = []
        for j in range(1, NZ):
            got["s2"].append(net.put(msg2, buf2.at[z], {"sp": zmod(z + j) * NY + y}))
        buf2[z] = msg2[...]

    def stage3():
        arrive(got["s2"])
        run = jnp.zeros((QROWS, 128), F32)
        for j in range(NZ):
            l0, l1 = read_logs(buf2[j, QROWS:MROWS])
            new = run * factor(l0, l1) + buf2[j, 0:QROWS].astype(F32)
            run = jnp.where(j < z, new, run)
        for j in range(NY):
            part, l0, l1 = before[j]
            msg3[j] = (run * factor(l0, l1) + part).astype(BF16)
        mine = pl.ds(pl.multiple_of(y * QROWS, 16), QROWS)
        got["s3"] = []
        for j in range(1, NY):
            to = ymod(y + j)
            got["s3"].append(net.put(msg3.at[to], enter.at[mine], {"sp": z * NY + to}))
        enter[mine] = msg3[y]

    def inside(b, carry):
        at = pl.ds(pl.multiple_of(b * BLOCK, BLOCK), BLOCK)
        t = cols[b]
        c = ctab[b]
        queries[0, at] = conv(3, b).astype(BF16)
        for g in range(2):
            h = 2 * g
            qb, v = queries[g, at], values[g, at]
            scores = dot(qb, keys[g, at], 1, 1)
            weights = []
            for j in range(2):
                span = t[:, h + j : h + j + 1] - c[h + j : h + j + 1]
                weights.append((jnp.exp(jnp.where(causal, span, -jnp.inf)) * scores).astype(BF16))
            zero = jnp.zeros_like(v)
            two = jnp.concatenate([jnp.where(low, v, zero), jnp.where(low, zero, v)], axis=0)
            cum = halves(low, t[:, h : h + 1], t[:, h + 1 : h + 2])
            local[g, at] = dot(jnp.concatenate(weights, axis=1), two, 1, 0) + dot(
                qb, starts[g, b], 1, 0) * jnp.exp(cum)
        return carry

    def inside_a():
        own[8].wait()
        gf[...] = raw_g[...].astype(F32)
        for g in range(2):
            gates[g] = silu(gf[pl.ds(g, length, stride=2)])
        lax.fori_loop(0, blocks // 2, inside, 0, unroll=2)

    def inside_b():
        lax.fori_loop(blocks // 2, blocks, inside, 0, unroll=2)

    per = blocks // CHUNKS
    tokens = BLOCK * per

    def finish(k):
        need("s3")
        for i in range(per):
            b = k * per + i
            at = slice(b * BLOCK, (b + 1) * BLOCK)
            t = cols[b]
            for g in range(2):
                h = 8 + 2 * g
                if g == 0:
                    entering = enter[0:128]
                else:
                    entering = jnp.concatenate([enter[128:192], jnp.zeros((64, 128), BF16)], axis=0)
                m = local[g, at] + dot(queries[g, at], entering, 1, 0) * halves(
                    low, t[:, h : h + 1], t[:, h + 1 : h + 2])
                m = m * gates[g, at]
                square = m * m
                s0 = jnp.sum(jnp.where(low, square, 0.0), axis=1, keepdims=True)
                s1 = jnp.sum(jnp.where(low, 0.0, square), axis=1, keepdims=True)
                scale = lax.rsqrt(halves(low, s0, s1) * (1.0 / HEAD) + EPSILON)
                mx[k, tp, i, :, g * 128 : (g + 1) * 128] = (
                    m * scale * gain[g : g + 1]).astype(BF16)

    def project(k):
        need("share")
        tp_done("A", k)
        lhs = jnp.concatenate(
            [mx[k, s, odd, :, g * 128 : (g + 1) * 128] for g in range(2) for s in range(NTP)], axis=1)
        base = jnp.concatenate([res[k, odd], rn[0, k], rn[1, k]], axis=1)
        st[k, tp] = (dot(lhs, wo[...], 1, 0) + base.astype(F32)).astype(BF16)

    def stream_of(k, q, xx, cc):
        if xx % 2 == q:
            return st[k, 2 * xx + cc, :, 0:256]
        return jnp.concatenate(
            [st[k, 2 * ((xx - 1) % NX) + cc, :, 256:384], st[k, 2 * ((xx + 1) % NX) + cc, :, 384:512]],
            axis=1)

    def norm(k):
        tp_done("B", k)
        for q in range(2):
            square = jnp.zeros((BLOCK, 128), F32)
            for slot in (2 * q, 2 * q + 1, 2 * q + 4, 2 * q + 5):
                v = st[k, slot].astype(F32)
                for c in range(4):
                    piece = v[:, c * 128 : (c + 1) * 128]
                    square = square + piece * piece
            scale = lax.rsqrt(jnp.sum(square, axis=1, keepdims=True) * (1.0 / depth) + EPSILON)
            for slot in range(NTP):
                cut = slice(slot * 256, (slot + 1) * 256)
                v = stream_of(k, q, slot // 2, slot % 2).astype(F32)
                nb[k, q * BLOCK : (q + 1) * BLOCK, cut] = (v * scale * channel_gain[:, cut]).astype(BF16)

    def hidden_units(k):
        for j in (0, 1, -1, 2, -2, 3, -3, 4):
            need("gr", j)
        for c in range(NY):
            need("uz", c, 4)
        pair = dot(nb[k], gu[...].reshape(depth, 2 * width), 1, 0)
        hidden[k] = (silu(pair[:, :width]) * pair[:, width:]).astype(BF16)

    order = (2, 3, 1, 0)
    dests = {k: lax.rem(x + k, NX) * 2 for k in order}

    def down(k, d):
        return dot(hidden[k], dn[d].reshape(256, width), 1, 1).astype(BF16)

    def down_partner(k):
        need("dr", 0)
        need("dr", 1)
        need("ez", 4)
        for j in order:
            ps[k, j] = down(k, dests[j] + 1 - core)
        for j in order:
            got["P", k, j] = net.put(ps.at[k, j], pr.at[k, j], partner)

    def down_own(k):
        for j in order:
            po[k, j] = down(k, dests[j] + core)

    def pair_sum(k, j):
        got["P", k, j].wait_recv()
        return po[k, j].astype(F32) + pr[k, j].astype(F32)

    mid = tokens // 2

    def sum_first(k):
        qs[k, 2] = pair_sum(k, 2).astype(BF16)
        got["C1", k] = (net.put(qs.at[k, 2, 0:mid], relay_r.at[k], x_left),
                        net.put(qs.at[k, 2, mid:], relay_l.at[k], x_right))

    def sum_second(k):
        to_left, to_right = pair_sum(k, 3), pair_sum(k, 1)
        arrive(got["C1", k])
        qs[k, 3, 0:mid] = (to_left[0:mid] + relay_r[k].astype(F32)).astype(BF16)
        qs[k, 3, mid:] = to_left[mid:].astype(BF16)
        qs[k, 1, 0:mid] = to_right[0:mid].astype(BF16)
        qs[k, 1, mid:] = (to_right[mid:] + relay_l[k].astype(F32)).astype(BF16)
        got["C2", k] = (net.put(qs.at[k, 3], from_r.at[k], x_left),
                        net.put(qs.at[k, 1], from_l.at[k], x_right))

    def sum_third(k):
        total = pair_sum(k, 0)
        arrive(got["C2", k])
        total = total + from_l[k].astype(F32) + from_r[k].astype(F32)
        mine = st[k, tp, :, 0:256].astype(F32)
        other = jnp.concatenate(
            [st[k, slot_l, :, 256:384], st[k, slot_r, :, 384:512]], axis=1).astype(F32)
        for q in range(2):
            at = k * tokens + q * BLOCK
            stream = jnp.where(odd == q, mine, other)
            out[at : at + BLOCK] = (
                stream + 0.5 * total[q * BLOCK : (q + 1) * BLOCK]).astype(BF16)

    run = {
        "spread": spread,
        "bA": lambda: run_blocks(1, 5),
        "bB": lambda: run_blocks(5, 7),
        "b0": last_block,
        "s1": stage1,
        "s2": stage2,
        "s3": stage3,
        "ia": inside_a,
        "ib": inside_b,
        "gy0": lambda: gate_y(0),
        "gy1": lambda: gate_y(1, -1),
        "gy2": lambda: gate_y(2, -2),
        "gy3": lambda: gate_y(3, -3),
        "gy4": lambda: gate_y(4),
        "uy1": lambda: up_y(1),
        "uy2": lambda: up_y(2),
        "dy0": lambda: down_y(0),
        "dy1": lambda: down_y(1),
        "ey1": lambda: rest_y(1),
        "ey2": lambda: rest_y(2),
        "dr0": lambda: down_relay(0),
        "dr1": lambda: down_relay(1),
        "share": share,
    }
    for r in (1, 2, 3, 4):
        run[f"gz{r}"] = functools.partial(gate_z, r)
        for c in range(NY):
            run[f"u{c}{r}"] = functools.partial(up_z, c, r)
        run[f"dz{r}"] = functools.partial(down_z, r)
        run[f"ez{r}"] = functools.partial(rest_z, r)
    for k in (0, 1, -1, 2, -2, 3, -3, 4):
        run[f"gr{k}"] = functools.partial(gate_relay, k)
    for k in range(CHUNKS):
        run[f"fin{k}"] = functools.partial(finish, k)
        run[f"P{k}"] = functools.partial(project, k)
        run[f"N{k}"] = functools.partial(norm, k)
        run[f"H{k}"] = functools.partial(hidden_units, k)
        run[f"D{k}"] = functools.partial(down_partner, k)
        run[f"E{k}"] = functools.partial(down_own, k)
        run[f"C1{k}"] = functools.partial(sum_first, k)
        run[f"C2{k}"] = functools.partial(sum_second, k)
        run[f"C3{k}"] = functools.partial(sum_third, k)
        run[f"Ai{k}"] = functools.partial(mix_first, k)
        run[f"Ar{k}"] = functools.partial(mix_second, k)
        run[f"Af{k}"] = functools.partial(mix_third, k)
        run[f"Bi{k}"] = functools.partial(tp_first, st, "B", k)
        run[f"Br{k}"] = functools.partial(tp_second, st, "B", k)
        run[f"Bf{k}"] = functools.partial(tp_third, st, "B", k)
    for name in STEPS:
        mark(name)
        run.pop(name)()
    assert not run

    mark("sends")
    for copy in net.sent:
        copy.wait_send()


def layer(vmem_args, smem_arg, hbm_args):
    length = hbm_args[2].shape[0]
    blocks = length // BLOCK
    tokens = length // CHUNKS
    width = hbm_args[8].shape[1]
    vmem = pl.BlockSpec(memory_space=pltpu.VMEM)
    dma = pltpu.SemaphoreType.DMA

    def bf(*shape):
        return pltpu.VMEM(shape, BF16)

    def fl(*shape):
        return pltpu.VMEM(shape, F32)

    return pl.pallas_call(
        layer_kernel,
        out_shape=jax.ShapeDtypeStruct((length, 256), BF16),
        in_specs=[vmem] * len(vmem_args)
        + [pl.BlockSpec(memory_space=pltpu.SMEM)]
        + [pl.BlockSpec(memory_space=pl.ANY)] * len(hbm_args),
        out_specs=vmem,
        scratch_shapes=[
            bf(2 * length, 128), bf(2 * length, 128), bf(length, 128), bf(length, 128),
            bf(128, length), fl(2 * length, 128), fl(2 * length, 128), fl(5, length + 8, 128),
            bf(16, 128), bf(16, 128), bf(16, 128), bf(128, 128),
            fl(blocks, 8, 128), fl(blocks, BLOCK, 16),
            bf(2, length, 128), bf(2, length, 128), bf(2, length, 128),
            fl(2, length, 128), fl(2, length, 128),
            fl(2, blocks, 128, 128), bf(2, blocks, 128, 128),
            bf(NY, MROWS, 128), bf(NY, MROWS, 128), bf(MROWS, 128), bf(NZ, MROWS, 128),
            bf(NY, QROWS, 128), bf(NY * QROWS, 128),
            bf(NZ, NY, 64, 2 * width), bf(NZ, NY, 64, width), bf(2048, 512),
            bf(CHUNKS, 2, BLOCK, 256), bf(2, CHUNKS, BLOCK, 128),
            bf(CHUNKS, NTP, 2, BLOCK, 256), bf(CHUNKS, NTP, BLOCK, 512),
            bf(CHUNKS, tokens, 2048), bf(CHUNKS, tokens, width),
            bf(CHUNKS, NX, tokens, 256), bf(CHUNKS, NX, tokens, 256), bf(CHUNKS, NX, tokens, 256),
            bf(CHUNKS, tokens // 2, 256), bf(CHUNKS, tokens // 2, 256),
            bf(CHUNKS, NX, tokens, 256), bf(CHUNKS, tokens, 256), bf(CHUNKS, tokens, 256),
            dma((11,)), dma((N_PUT,)), dma((N_PUT,)),
        ],
        compiler_params=pltpu.CompilerParams(
            collective_id=0, has_side_effects=True, vmem_limit_bytes=58 * 1024 * 1024),
        cost_estimate=pl.CostEstimate(
            flops=12_000_000_000, bytes_accessed=8_000_000, transcendentals=4_000_000),
        name="layer",
    )(*vmem_args, smem_arg, *hbm_args)


def shards(
    grouped_head_inputs,
    head_gate_inputs,
    unsmoothed_step,
    head_decay_rate,
    extra_log_decay,
    first_group_keys,
    first_group_queries,
    second_group_keys,
    second_group_queries,
    head_input_filter,
    first_group_filter,
    second_group_filter,
    head_norm_gain,
    output_weight,
    residual,
    channel_norm_gain,
    channel_gate_weight,
    channel_up_weight,
    channel_down_weight,
):
    length = grouped_head_inputs.shape[0]
    return layer(
        (
            unsmoothed_step.transpose(1, 2, 0),
            extra_log_decay.transpose(1, 2, 0),
            head_input_filter,
            first_group_filter,
            second_group_filter,
            head_norm_gain,
            channel_norm_gain[None],
        ),
        head_decay_rate,
        (
            grouped_head_inputs.reshape(2 * length, 128),
            head_gate_inputs.reshape(2 * length, 128),
            first_group_keys,
            first_group_queries,
            second_group_keys.T,
            second_group_queries.T,
            output_weight.reshape(-1, output_weight.shape[2]),
            residual.reshape(CHUNKS, 2, BLOCK, residual.shape[1]),
            channel_gate_weight,
            channel_up_weight,
            channel_down_weight,
        ),
    )


def solution(mesh):
    return jax.shard_map(
        shards,
        mesh=mesh,
        in_specs=(
            P("sp", None, "tp"),
            P("sp", None, "tp"),
            P("sp", None, "tp"),
            P(None, "tp"),
            P("sp", None, "tp"),
            P("sp", None),
            P("sp", None),
            P("sp", None),
            P("sp", None),
            P(None, None, "tp"),
            P(),
            P(),
            P(None, "tp"),
            P(None, None, "tp"),
            P("sp", "tp"),
            P(),
            P("sp", "tp"),
            P("sp", "tp"),
            P("sp", "tp"),
        ),
        out_specs=P("sp", "tp"),
        check_vma=False,
    )
```

```python
import functools

import jax
import jax.numpy as jnp
from jax import lax
from jax.experimental import pallas as pl
from jax.experimental.pallas import tpu as pltpu
from jax.sharding import PartitionSpec as P

HEAD = 64
CONV = 4
BLOCK = 128
EPSILON = 1e-06
MESH = pl.DeviceIdType.MESH
F32 = jnp.float32
BF16 = jnp.bfloat16
NY = 4
NZ = 8
NX = 4
NTP = 8
QROWS = 48
MROWS = 64
CHUNKS = 4
N_PUT = 236
SPLIT = 512
STEPS = (
    "gz1", "ey1", "dz1", "spread", "tables", "gy0", "uy1", "u01", "bA", "bB", "b0", "share",
    "gz2", "s1", "dz2", "ey2", "gr0", "gy1", "s2", "ia", "dz3", "gz3", "ez1", "uy2", "gy2", "gr1",
    "u21", "ib", "dz4", "u02", "s3", "gr-1", "u11", "gy3", "fin0", "Ai0", "fin1", "fin2", "dy1",
    "gr-2", "u22", "fin3", "gr2", "u31", "dy0", "Ai1", "Ar0", "Ai2", "gr3", "gz4", "gr-3", "u12",
    "Ar1", "u03", "Ai3", "ez2", "Af0", "P0", "Ar2", "u32", "Bi0", "gy4", "Af1", "u23", "P1",
    "Af2", "Bi1", "Ar3", "dr1", "u13", "u33", "Br0", "u24", "P2", "Br1", "u14", "Bi2", "ez3",
    "u04", "Af3", "gr4", "P3", "dr0", "u34", "Bi3", "Bf0", "Bf1", "ez4", "N0", "N1", "Br2", "H1",
    "D1", "Br3", "H0", "Bf2", "D0", "E1", "C11", "N2", "E0", "Bf3", "C10", "H2", "D2", "C21",
    "N3", "E2", "C12", "H3", "C20", "D3", "C31", "E3", "C13", "C22", "C30", "C23", "C32", "C33",
)


def mark(name):
    pass


def silu(v):
    return v * (0.5 * jnp.tanh(0.5 * v) + 0.5)


def halves(lane_low, a, b):
    return jnp.where(lane_low, a, b)


def dot(a, b, ca, cb):
    return lax.dot_general(a, b, (((ca,), (cb,)), ((), ())), preferred_element_type=F32)


def split_three(v):
    hi = v.astype(BF16)
    rest = v - hi.astype(F32)
    mid = rest.astype(BF16)
    low = (rest - mid.astype(F32)).astype(BF16)
    return hi, mid, low


def log_rows(l0, l1):
    rows = []
    for part0, part1 in zip(split_three(l0), split_three(l1)):
        rows += [part0.astype(F32), part1.astype(F32)]
    rows.append(jnp.zeros((10, 128), F32))
    return jnp.concatenate(rows, axis=0).astype(BF16)


def read_logs(rows):
    v = rows.astype(F32)
    return v[0:1] + v[2:3] + v[4:5], v[1:2] + v[3:4] + v[5:6]


class Net:
    def __init__(self, send, recv):
        self.send, self.recv, self.sent = send, recv, []

    def put(self, src, dst, to):
        index = len(self.sent)
        copy = pltpu.make_async_remote_copy(
            src_ref=src, dst_ref=dst, send_sem=self.send.at[index], recv_sem=self.recv.at[index],
            device_id=to, device_id_type=MESH)
        copy.start()
        self.sent.append(copy)
        return copy


def arrive(copies):
    for copy in copies:
        copy.wait_recv()


def layer_kernel(
    hbm_step, hbm_extra, hbm_head, hbm_taps1, hbm_taps2, hbm_gain, hbm_channel, hbm_rate,
    hx, hg, k1, q1, k2t, q2t, out_w, resid, gate_w, up_w, down_w,
    hbm_out,
    step_in, extra, head_taps, taps1, taps2, gain, channel_gain, rate, out,
    raw_x, raw_g, raw_k, raw_q, raw_t, xf, gf, pad, rim_x, rim_k, rim_q, rim_t,
    ctab, cols, keys, queries, values, local, gates, upd, starts,
    msg1, buf1, msg2, buf2, msg3, enter,
    gu, dn, wo, res, rn, mx, st, nb, hidden, ps, pr, po, relay_l, relay_r, qs, from_l, from_r,
    local_sem, send_sem, recv_sem,
):
    sp = lax.axis_index("sp")
    tp = lax.axis_index("tp")
    y = lax.rem(sp, NY)
    z = sp // NY
    core = lax.rem(tp, 2)
    x = tp // 2
    n_sp = NY * NZ
    length = k1.shape[0]
    blocks = length // BLOCK
    width = gate_w.shape[1]
    depth = wo.shape[0]
    right = lax.rem(sp + 1, n_sp)
    left = lax.rem(sp + n_sp - 1, n_sp)

    def zmod(v):
        return lax.rem(v + NZ, NZ)

    def ymod(v):
        return lax.rem(v + NY, NY)

    y_peers = [{"sp": z * NY + ymod(y + j)} for j in range(1, NY)]
    z_peers = [{"sp": zmod(z + j) * NY + y} for j in range(1, NZ)]
    to_up_y, to_down_y = {"sp": z * NY + ymod(y + 1)}, {"sp": z * NY + ymod(y - 1)}
    to_up_z, to_down_z = {"sp": zmod(z + 1) * NY + y}, {"sp": zmod(z - 1) * NY + y}
    odd = lax.rem(x, 2)
    even = 1 - odd
    slot_l = lax.rem(x + NX - 1, NX) * 2 + core
    slot_r = lax.rem(x + 1, NX) * 2 + core
    slot_o = lax.rem(x + 2, NX) * 2 + core
    partner, x_right, x_left = {"tp": x * 2 + 1 - core}, {"tp": slot_r}, {"tp": slot_l}

    mark("barrier")
    wanted = [
        (gate_w, gu.at[z, y, :, 0:width]),
        (up_w, gu.at[z, y, :, width:]),
        (down_w, dn.at[z, y]),
        (hx, raw_x),
        (k1, raw_k),
        (q1, raw_q),
        (k2t, raw_t.at[0:64]),
        (q2t, raw_t.at[64:128]),
        (hg, raw_g),
        (out_w, wo.at[:, 0:256]),
        (resid, res),
        (hbm_step, step_in),
        (hbm_extra, extra),
        (hbm_rate, rate),
        (hbm_head, head_taps),
        (hbm_taps1, taps1),
        (hbm_taps2, taps2),
        (hbm_gain, gain),
        (hbm_channel, channel_gain),
    ]
    barrier = pltpu.get_barrier_semaphore()
    greet = [{"sp": right}, {"sp": left}] + y_peers + z_peers + [partner, x_right, x_left]
    for peer in greet:
        pl.semaphore_signal(barrier, inc=1, device_id=peer, device_id_type=MESH)

    own = [pltpu.make_async_copy(a, b, local_sem.at[n]) for n, (a, b) in enumerate(wanted)]
    for copy in own:
        copy.start()

    row8 = lax.broadcasted_iota(jnp.int32, (8, 128), 0)
    low = lax.broadcasted_iota(jnp.int32, (BLOCK, 128), 1) < HEAD
    low1 = lax.broadcasted_iota(jnp.int32, (1, 128), 1) < HEAD
    at_row = lax.broadcasted_iota(jnp.int32, (BLOCK, BLOCK), 0)
    at_col = lax.broadcasted_iota(jnp.int32, (BLOCK, BLOCK), 1)
    causal = at_row >= at_col
    upper = jnp.where(at_row <= at_col, 1.0, 0.0).astype(BF16)

    mark("barwait")
    for copy in own[:8]:
        copy.wait()
    pl.semaphore_wait(barrier, len(greet))

    net = Net(send_sem, recv_sem)
    got = {}
    have = {("gz", 0)}

    def need(*key):
        if key not in have:
            have.add(key)
            arrive(got[key if len(key) > 1 else key[0]])

    tail = pl.ds(length - 16, 16)
    rims = [
        net.put(raw_x.at[pl.ds(2 * length - 16, 16)], rim_x, {"sp": right}),
        net.put(raw_k.at[tail], rim_k, {"sp": right}),
        net.put(raw_q.at[tail], rim_q, {"sp": right}),
        net.put(raw_t.at[:, pl.ds(length - BLOCK, BLOCK)], rim_t, {"sp": right}),
    ]

    def both(ref_a, ref_b, to_a, to_b):
        return net.put(ref_a, ref_a, to_a), net.put(ref_b, ref_b, to_b)

    def gate_z(r):
        need("gz", r - 1)
        a, b = zmod(z - (r - 1)), zmod(z + (r - 1))
        if r == 4:
            got["gz", r] = both(
                gu.at[a, y, 0:32, 0:width], gu.at[b, y, 32:64, 0:width], to_up_z, to_down_z)
        else:
            got["gz", r] = both(
                gu.at[a, y, :, 0:width], gu.at[b, y, :, 0:width], to_up_z, to_down_z)

    def gate_y(*ks):
        for k in ks:
            need("gz", abs(k))
            ref = gu.at[zmod(z + k), y, :, 0:width]
            got["gy", k] = both(ref, ref, to_up_y, to_down_y)

    def gate_relay(k):
        arrive(got["gy", k])
        zz = zmod(z + k)
        got["gr", k] = both(
            gu.at[zz, ymod(y - 1), 0:32, 0:width], gu.at[zz, ymod(y + 1), 32:64, 0:width],
            to_up_y, to_down_y)

    def up_y(r):
        if r == 1:
            ref = gu.at[z, y, :, width:]
            got["uy", 1] = both(ref, ref, to_up_y, to_down_y)
        else:
            need("uy", 1)
            got["uy", 2] = both(
                gu.at[z, ymod(y - 1), 0:32, width:], gu.at[z, ymod(y + 1), 32:64, width:],
                to_up_y, to_down_y)

    def up_z(c, r):
        if r > 1:
            arrive(got["uz", c, r - 1])
        elif c > 0:
            need("uy", 2 if c == 3 else 1)
        col = ymod(y + (0, -1, 1, 2)[c])
        a, b = zmod(z - (r - 1)), zmod(z + (r - 1))
        if r == 4:
            got["uz", c, r] = both(
                gu.at[a, col, 0:32, width:], gu.at[b, col, 32:64, width:], to_up_z, to_down_z)
        else:
            got["uz", c, r] = both(
                gu.at[a, col, :, width:], gu.at[b, col, :, width:], to_up_z, to_down_z)

    def down_z(r):
        if r > 1:
            arrive(got["dz", r - 1])
        a, b = zmod(z - (r - 1)), zmod(z + (r - 1))
        if r == 4:
            got["dz", r] = both(
                dn.at[a, y, 0:32, 0:SPLIT], dn.at[b, y, 32:64, 0:SPLIT], to_up_z, to_down_z)
        else:
            got["dz", r] = both(
                dn.at[a, y, :, 0:SPLIT], dn.at[b, y, :, 0:SPLIT], to_up_z, to_down_z)

    def down_y(h):
        need("dz", 4)
        ref = dn.at[4 * h : 4 * h + 4, y, :, 0:SPLIT]
        got["dy", h] = both(ref, ref, to_up_y, to_down_y)

    def down_relay(h):
        arrive(got["dy", h])
        part = pl.ds(4 * h, 4)
        got["dr", h] = both(
            dn.at[part, ymod(y - 1), 0:32, 0:SPLIT], dn.at[part, ymod(y + 1), 32:64, 0:SPLIT],
            to_up_y, to_down_y)

    def rest_y(r):
        if r == 1:
            ref = dn.at[z, y, :, SPLIT:]
            got["ey", 1] = both(ref, ref, to_up_y, to_down_y)
        else:
            need("ey", 1)
            got["ey", 2] = both(
                dn.at[z, ymod(y - 1), 0:32, SPLIT:], dn.at[z, ymod(y + 1), 32:64, SPLIT:],
                to_up_y, to_down_y)

    def rest_z(r):
        if r == 1:
            need("ey", 2)
        else:
            arrive(got["ez", r - 1])
        a, b = zmod(z - (r - 1)), zmod(z + (r - 1))
        if r == 4:
            got["ez", r] = both(
                dn.at[a, 0:2, :, SPLIT:], dn.at[b, 2:4, :, SPLIT:], to_up_z, to_down_z)
        else:
            got["ez", r] = both(
                dn.at[a, :, :, SPLIT:], dn.at[b, :, :, SPLIT:], to_up_z, to_down_z)

    def share():
        own[9].wait()
        own[10].wait()
        got["share"] = (
            net.put(res.at[:, even, :, 0:128], rn.at[0], x_left),
            net.put(res.at[:, even, :, 128:256], rn.at[1], x_right),
            net.put(wo.at[:, 0:128], wo.at[:, 256:384], x_left),
            net.put(wo.at[:, 128:256], wo.at[:, 384:512], x_right),
        )

    def mix_first(k):
        a, b = mx.at[k, tp, odd, 0:64], mx.at[k, tp, odd, 64:128]
        ref = mx.at[k, tp, even]
        got["A", k, 0] = (net.put(a, a, x_right), net.put(b, b, x_left),
                          net.put(ref, ref, x_right), net.put(ref, ref, x_left))
        ref = mx.at[k, tp, odd]
        got["A", k, 1] = [net.put(ref, ref, partner)]

    def mix_second(k):
        arrive(got["A", k, 0])
        a, b = mx.at[k, slot_l, even, 0:64], mx.at[k, slot_r, even, 64:128]
        got["A", k, 2] = (net.put(a, a, x_right), net.put(b, b, x_left))
        for slot in (slot_l, slot_r):
            ref = mx.at[k, slot, odd]
            got["A", k, 1] += [net.put(ref, ref, partner)]

    def mix_third(k):
        arrive(got["A", k, 2])
        ref = mx.at[k, slot_o, odd]
        got["A", k, 1] += [net.put(ref, ref, partner)]

    def tp_first(buf, key, k):
        ref = buf.at[k, tp]
        got[key, k, 0] = (net.put(ref, ref, x_right), net.put(ref, ref, x_left))
        got[key, k, 1] = [net.put(ref, ref, partner)]

    def tp_second(buf, key, k):
        arrive(got[key, k, 0])
        ref_l, ref_r = buf.at[k, slot_l], buf.at[k, slot_r]
        half = buf.shape[2] // 2
        a, b = ref_l.at[0:half], ref_r.at[half:]
        got[key, k, 2] = (net.put(a, a, x_right), net.put(b, b, x_left))
        got[key, k, 1] += [net.put(ref_l, ref_l, partner), net.put(ref_r, ref_r, partner)]

    def tp_third(buf, key, k):
        arrive(got[key, k, 2])
        ref = buf.at[k, slot_o]
        got[key, k, 1] += [net.put(ref, ref, partner)]

    def tp_done(key, k):
        arrive(got[key, k, 1])

    def tables():
        for copy in own[11:]:
            copy.wait()
        first_head = lax.broadcasted_iota(jnp.int32, (2, length), 0) == 0
        steps = [jax.nn.softplus(step_in[g]) for g in range(2)]
        logs = [extra[g] - steps[g] * jnp.where(first_head, rate[g : g + 1, 0:1], rate[g : g + 1, 1:2]) for g in range(2)]
        table = jnp.concatenate(
            [v[:, b * BLOCK : (b + 1) * BLOCK] for b in range(blocks) for v in logs + steps], axis=0)
        rows = table.shape[0]
        sums = dot(jnp.concatenate(split_three(table), axis=0), upper, 1, 0)
        sums = sums[0:rows] + sums[rows : 2 * rows] + sums[2 * rows :]
        offs = jnp.zeros((8, 1), F32)
        for b in range(blocks):
            cut = slice(8 * b, 8 * b + 8)
            c8 = jnp.where(row8 < 4, sums[cut], table[cut])
            ctab[b] = c8
            e8 = jnp.exp(jnp.where(row8 < 4, c8 + offs, 0.0))
            cols[b] = jnp.concatenate([c8, e8], axis=0).T
            offs = offs + c8[:, 127:128]
        log0 = halves(low1, offs[0:1], offs[1:2])
        log1 = halves(low1, offs[2:3], offs[3:4])
        my_logs = log_rows(log0, log1)
        for q in range(NY):
            msg1[q, QROWS:MROWS] = my_logs

    def spread():
        xf[...] = raw_x[...].astype(F32)
        for g in range(2):
            pad[g, 8 : 8 + length] = xf[pl.ds(g, length, stride=2)]
        pad[2, 8 : 8 + length] = raw_k[...].astype(F32)
        pad[3, 8 : 8 + length] = raw_q[...].astype(F32)
        for b in range(blocks):
            pad[4, 8 + b * BLOCK : 8 + (b + 1) * BLOCK] = raw_t[:, b * BLOCK : (b + 1) * BLOCK].astype(F32).T

    def conv(n, b):
        full = pad[n, pl.ds(pl.multiple_of(b * BLOCK, BLOCK), BLOCK + 8)]
        if n < 2:
            taps = [head_taps[k, n : n + 1] for k in range(CONV)]
        elif n < 4:
            taps = [taps1[k, n - 2 : n - 1] for k in range(CONV)]
        else:
            taps = [jnp.concatenate([taps2[k, 0:1], taps2[k, 1:2]], axis=1) for k in range(CONV)]
        total = taps[0] * full[5 : 5 + BLOCK]
        for k in range(1, CONV):
            total = total + taps[k] * full[5 + k : 5 + k + BLOCK]
        return silu(total)

    def block(b, carry):
        at = pl.ds(pl.multiple_of(b * BLOCK, BLOCK), BLOCK)
        c = ctab[b]
        t = cols[b]
        key_one, mix_two = conv(2, b), conv(4, b)
        key_two = jnp.where(low, mix_two, 0.0)
        queries[1, at] = jnp.where(low, pltpu.roll(mix_two, 64, 1), 0.0).astype(BF16)
        for g, key in enumerate([key_one, key_two]):
            h = 2 * g
            v = conv(g, b) * halves(low, t[:, 4 + h : 5 + h], t[:, 5 + h : 6 + h])
            cum = halves(low, t[:, h : h + 1], t[:, h + 1 : h + 2])
            total = halves(low1, c[h : h + 1, 127:128], c[h + 1 : h + 2, 127:128])
            kb = key.astype(BF16)
            keys[g, at] = kb
            values[g, at] = v.astype(BF16)
            upd[g, b] = dot(kb, (v * jnp.exp(total - cum)).astype(BF16), 0, 0)
        return carry

    def run_blocks(lo, hi):
        lax.fori_loop(lo, hi, block, 0, unroll=2)

    def last_block():
        block(blocks - 1, 0)
        arrive(rims)
        has_left = sp > 0
        xf[0:16] = rim_x[...].astype(F32)
        for g in range(2):
            pad[g, 0:8] = jnp.where(has_left, xf[pl.ds(g, 8, stride=2)], 0.0)
        pad[2, 0:8] = jnp.where(has_left, rim_k[...].astype(F32)[8:16], 0.0)
        pad[3, 0:8] = jnp.where(has_left, rim_q[...].astype(F32)[8:16], 0.0)
        pad[4, 0:8] = jnp.where(has_left, rim_t[...].astype(F32).T[BLOCK - 8 :], 0.0)
        block(0, 0)
        ends = []
        for g in range(2):
            h = 2 * g
            state = jnp.zeros((BLOCK, 128), F32)
            for b in range(blocks):
                c = ctab[b]
                total = halves(low1, c[h : h + 1, 127:128], c[h + 1 : h + 2, 127:128])
                starts[g, b] = state.astype(BF16)
                state = state * jnp.exp(total) + upd[g, b]
            ends.append(state)
        full = jnp.concatenate([ends[0], ends[1][0:64]], axis=0).astype(BF16)
        for q in range(NY):
            msg1[q, 0:QROWS] = full[q * QROWS : (q + 1) * QROWS]

    quarter = y * QROWS + lax.broadcasted_iota(jnp.int32, (QROWS, 128), 0)
    group_one = quarter < 128

    def factor(l0, l1):
        return jnp.where(group_one, jnp.exp(l0), jnp.exp(l1))

    def stage1():
        got["s1"] = []
        for j in range(1, NY):
            to = ymod(y + j)
            got["s1"].append(net.put(msg1.at[to], buf1.at[y], {"sp": z * NY + to}))
        buf1[y] = msg1[y]

    before = []

    def stage2():
        arrive(got["s1"])
        run = jnp.zeros((QROWS, 128), F32)
        sum0 = jnp.zeros((1, 128), F32)
        sum1 = jnp.zeros((1, 128), F32)
        for j in range(NY):
            before.append((run, sum0, sum1))
            l0, l1 = read_logs(buf1[j, QROWS:MROWS])
            run = run * factor(l0, l1) + buf1[j, 0:QROWS].astype(F32)
            sum0, sum1 = sum0 + l0, sum1 + l1
        msg2[0:QROWS] = run.astype(BF16)
        msg2[QROWS:MROWS] = log_rows(sum0, sum1)
        got["s2"] = []
        for j in range(1, NZ):
            got["s2"].append(net.put(msg2, buf2.at[z], {"sp": zmod(z + j) * NY + y}))
        buf2[z] = msg2[...]

    def stage3():
        arrive(got["s2"])
        run = jnp.zeros((QROWS, 128), F32)
        for j in range(NZ):
            l0, l1 = read_logs(buf2[j, QROWS:MROWS])
            new = run * factor(l0, l1) + buf2[j, 0:QROWS].astype(F32)
            run = jnp.where(j < z, new, run)
        for j in range(NY):
            part, l0, l1 = before[j]
            msg3[j] = (run * factor(l0, l1) + part).astype(BF16)
        mine = pl.ds(pl.multiple_of(y * QROWS, 16), QROWS)
        got["s3"] = []
        for j in range(1, NY):
            to = ymod(y + j)
            got["s3"].append(net.put(msg3.at[to], enter.at[mine], {"sp": z * NY + to}))
        enter[mine] = msg3[y]

    def inside(b, carry):
        at = pl.ds(pl.multiple_of(b * BLOCK, BLOCK), BLOCK)
        t = cols[b]
        c = ctab[b]
        queries[0, at] = conv(3, b).astype(BF16)
        for g in range(2):
            h = 2 * g
            qb, v = queries[g, at], values[g, at]
            scores = dot(qb, keys[g, at], 1, 1)
            weights = []
            for j in range(2):
                span = t[:, h + j : h + j + 1] - c[h + j : h + j + 1]
                weights.append((jnp.exp(jnp.where(causal, span, -jnp.inf)) * scores).astype(BF16))
            zero = jnp.zeros_like(v)
            two = jnp.concatenate([jnp.where(low, v, zero), jnp.where(low, zero, v)], axis=0)
            cum = halves(low, t[:, h : h + 1], t[:, h + 1 : h + 2])
            local[g, at] = dot(jnp.concatenate(weights, axis=1), two, 1, 0) + dot(
                qb, starts[g, b], 1, 0) * jnp.exp(cum)
        return carry

    def inside_a():
        own[8].wait()
        gf[...] = raw_g[...].astype(F32)
        for g in range(2):
            gates[g] = silu(gf[pl.ds(g, length, stride=2)])
        lax.fori_loop(0, blocks // 2, inside, 0, unroll=2)

    def inside_b():
        lax.fori_loop(blocks // 2, blocks, inside, 0, unroll=2)

    per = blocks // CHUNKS
    tokens = BLOCK * per

    def finish(k):
        need("s3")
        for i in range(per):
            b = k * per + i
            at = slice(b * BLOCK, (b + 1) * BLOCK)
            t = cols[b]
            for g in range(2):
                h = 8 + 2 * g
                if g == 0:
                    entering = enter[0:128]
                else:
                    entering = jnp.concatenate([enter[128:192], jnp.zeros((64, 128), BF16)], axis=0)
                m = local[g, at] + dot(queries[g, at], entering, 1, 0) * halves(
                    low, t[:, h : h + 1], t[:, h + 1 : h + 2])
                m = m * gates[g, at]
                square = m * m
                s0 = jnp.sum(jnp.where(low, square, 0.0), axis=1, keepdims=True)
                s1 = jnp.sum(jnp.where(low, 0.0, square), axis=1, keepdims=True)
                scale = lax.rsqrt(halves(low, s0, s1) * (1.0 / HEAD) + EPSILON)
                mx[k, tp, i, :, g * 128 : (g + 1) * 128] = (
                    m * scale * gain[g : g + 1]).astype(BF16)

    def project(k):
        need("share")
        tp_done("A", k)
        lhs = jnp.concatenate(
            [mx[k, s, odd, :, g * 128 : (g + 1) * 128] for g in range(2) for s in range(NTP)], axis=1)
        base = jnp.concatenate([res[k, odd], rn[0, k], rn[1, k]], axis=1)
        st[k, tp] = (dot(lhs, wo[...], 1, 0) + base.astype(F32)).astype(BF16)

    def stream_of(k, q, xx, cc):
        if xx % 2 == q:
            return st[k, 2 * xx + cc, :, 0:256]
        return jnp.concatenate(
            [st[k, 2 * ((xx - 1) % NX) + cc, :, 256:384], st[k, 2 * ((xx + 1) % NX) + cc, :, 384:512]],
            axis=1)

    def norm(k):
        tp_done("B", k)
        for q in range(2):
            square = jnp.zeros((BLOCK, 128), F32)
            for slot in (2 * q, 2 * q + 1, 2 * q + 4, 2 * q + 5):
                v = st[k, slot].astype(F32)
                for c in range(4):
                    piece = v[:, c * 128 : (c + 1) * 128]
                    square = square + piece * piece
            scale = lax.rsqrt(jnp.sum(square, axis=1, keepdims=True) * (1.0 / depth) + EPSILON)
            for slot in range(NTP):
                cut = slice(slot * 256, (slot + 1) * 256)
                v = stream_of(k, q, slot // 2, slot % 2).astype(F32)
                nb[k, q * BLOCK : (q + 1) * BLOCK, cut] = (v * scale * channel_gain[:, cut]).astype(BF16)

    def hidden_units(k):
        for j in (0, 1, -1, 2, -2, 3, -3, 4):
            need("gr", j)
        for c in range(NY):
            need("uz", c, 4)
        pair = dot(nb[k], gu[...].reshape(depth, 2 * width), 1, 0)
        hidden[k] = (silu(pair[:, :width]) * pair[:, width:]).astype(BF16)

    order = (2, 3, 1, 0)
    dests = {k: lax.rem(x + k, NX) * 2 for k in order}

    def down(k, d):
        return dot(hidden[k], dn[d].reshape(256, width), 1, 1).astype(BF16)

    def down_partner(k):
        need("dr", 0)
        need("dr", 1)
        need("ez", 4)
        for j in order:
            ps[k, j] = down(k, dests[j] + 1 - core)
        for j in order:
            got["P", k, j] = net.put(ps.at[k, j], pr.at[k, j], partner)

    def down_own(k):
        for j in order:
            po[k, j] = down(k, dests[j] + core)

    def pair_sum(k, j):
        got["P", k, j].wait_recv()
        return po[k, j].astype(F32) + pr[k, j].astype(F32)

    mid = tokens // 2
    outs = []

    def sum_first(k):
        qs[k, 2] = pair_sum(k, 2).astype(BF16)
        got["C1", k] = (net.put(qs.at[k, 2, 0:mid], relay_r.at[k], x_left),
                        net.put(qs.at[k, 2, mid:], relay_l.at[k], x_right))

    def sum_second(k):
        to_left, to_right = pair_sum(k, 3), pair_sum(k, 1)
        arrive(got["C1", k])
        qs[k, 3, 0:mid] = (to_left[0:mid] + relay_r[k].astype(F32)).astype(BF16)
        qs[k, 3, mid:] = to_left[mid:].astype(BF16)
        qs[k, 1, 0:mid] = to_right[0:mid].astype(BF16)
        qs[k, 1, mid:] = (to_right[mid:] + relay_l[k].astype(F32)).astype(BF16)
        got["C2", k] = (net.put(qs.at[k, 3], from_r.at[k], x_left),
                        net.put(qs.at[k, 1], from_l.at[k], x_right))

    def sum_third(k):
        total = pair_sum(k, 0)
        arrive(got["C2", k])
        total = total + from_l[k].astype(F32) + from_r[k].astype(F32)
        mine = st[k, tp, :, 0:256].astype(F32)
        other = jnp.concatenate(
            [st[k, slot_l, :, 256:384], st[k, slot_r, :, 384:512]], axis=1).astype(F32)
        for q in range(2):
            at = k * tokens + q * BLOCK
            stream = jnp.where(odd == q, mine, other)
            out[at : at + BLOCK] = (
                stream + 0.5 * total[q * BLOCK : (q + 1) * BLOCK]).astype(BF16)
        rows = pl.ds(k * tokens, tokens)
        copy = pltpu.make_async_copy(out.at[rows], hbm_out.at[rows], local_sem.at[19 + k])
        copy.start()
        outs.append(copy)

    run = {
        "tables": tables,
        "spread": spread,
        "bA": lambda: run_blocks(1, 5),
        "bB": lambda: run_blocks(5, 7),
        "b0": last_block,
        "s1": stage1,
        "s2": stage2,
        "s3": stage3,
        "ia": inside_a,
        "ib": inside_b,
        "gy0": lambda: gate_y(0),
        "gy1": lambda: gate_y(1, -1),
        "gy2": lambda: gate_y(2, -2),
        "gy3": lambda: gate_y(3, -3),
        "gy4": lambda: gate_y(4),
        "uy1": lambda: up_y(1),
        "uy2": lambda: up_y(2),
        "dy0": lambda: down_y(0),
        "dy1": lambda: down_y(1),
        "ey1": lambda: rest_y(1),
        "ey2": lambda: rest_y(2),
        "dr0": lambda: down_relay(0),
        "dr1": lambda: down_relay(1),
        "share": share,
    }
    for r in (1, 2, 3, 4):
        run[f"gz{r}"] = functools.partial(gate_z, r)
        for c in range(NY):
            run[f"u{c}{r}"] = functools.partial(up_z, c, r)
        run[f"dz{r}"] = functools.partial(down_z, r)
        run[f"ez{r}"] = functools.partial(rest_z, r)
    for k in (0, 1, -1, 2, -2, 3, -3, 4):
        run[f"gr{k}"] = functools.partial(gate_relay, k)
    for k in range(CHUNKS):
        run[f"fin{k}"] = functools.partial(finish, k)
        run[f"P{k}"] = functools.partial(project, k)
        run[f"N{k}"] = functools.partial(norm, k)
        run[f"H{k}"] = functools.partial(hidden_units, k)
        run[f"D{k}"] = functools.partial(down_partner, k)
        run[f"E{k}"] = functools.partial(down_own, k)
        run[f"C1{k}"] = functools.partial(sum_first, k)
        run[f"C2{k}"] = functools.partial(sum_second, k)
        run[f"C3{k}"] = functools.partial(sum_third, k)
        run[f"Ai{k}"] = functools.partial(mix_first, k)
        run[f"Ar{k}"] = functools.partial(mix_second, k)
        run[f"Af{k}"] = functools.partial(mix_third, k)
        run[f"Bi{k}"] = functools.partial(tp_first, st, "B", k)
        run[f"Br{k}"] = functools.partial(tp_second, st, "B", k)
        run[f"Bf{k}"] = functools.partial(tp_third, st, "B", k)
    for name in STEPS:
        mark(name)
        run.pop(name)()
    assert not run

    mark("sends")
    for copy in outs:
        copy.wait()
    for copy in net.sent:
        copy.wait_send()


def layer(small_args, hbm_args):
    length = hbm_args[2].shape[0]
    blocks = length // BLOCK
    tokens = length // CHUNKS
    width = hbm_args[8].shape[1]
    hbm = pl.BlockSpec(memory_space=pl.ANY)
    dma = pltpu.SemaphoreType.DMA

    def bf(*shape):
        return pltpu.VMEM(shape, BF16)

    def fl(*shape):
        return pltpu.VMEM(shape, F32)

    return pl.pallas_call(
        layer_kernel,
        out_shape=jax.ShapeDtypeStruct((length, 256), BF16),
        in_specs=[hbm] * (len(small_args) + len(hbm_args)),
        out_specs=hbm,
        scratch_shapes=[fl(*a.shape) for a in small_args]
        + [
            bf(length, 256),
            bf(2 * length, 128), bf(2 * length, 128), bf(length, 128), bf(length, 128),
            bf(128, length), fl(2 * length, 128), fl(2 * length, 128), fl(5, length + 8, 128),
            bf(16, 128), bf(16, 128), bf(16, 128), bf(128, 128),
            fl(blocks, 8, 128), fl(blocks, BLOCK, 16),
            bf(2, length, 128), bf(2, length, 128), bf(2, length, 128),
            fl(2, length, 128), fl(2, length, 128),
            fl(2, blocks, 128, 128), bf(2, blocks, 128, 128),
            bf(NY, MROWS, 128), bf(NY, MROWS, 128), bf(MROWS, 128), bf(NZ, MROWS, 128),
            bf(NY, QROWS, 128), bf(NY * QROWS, 128),
            bf(NZ, NY, 64, 2 * width), bf(NZ, NY, 64, width), bf(2048, 512),
            bf(CHUNKS, 2, BLOCK, 256), bf(2, CHUNKS, BLOCK, 128),
            bf(CHUNKS, NTP, 2, BLOCK, 256), bf(CHUNKS, NTP, BLOCK, 512),
            bf(CHUNKS, tokens, 2048), bf(CHUNKS, tokens, width),
            bf(CHUNKS, NX, tokens, 256), bf(CHUNKS, NX, tokens, 256), bf(CHUNKS, NX, tokens, 256),
            bf(CHUNKS, tokens // 2, 256), bf(CHUNKS, tokens // 2, 256),
            bf(CHUNKS, NX, tokens, 256), bf(CHUNKS, tokens, 256), bf(CHUNKS, tokens, 256),
            dma((19 + CHUNKS,)), dma((N_PUT,)), dma((N_PUT,)),
        ],
        compiler_params=pltpu.CompilerParams(
            collective_id=0, has_side_effects=True, vmem_limit_bytes=58 * 1024 * 1024),
        cost_estimate=pl.CostEstimate(
            flops=12_000_000_000, bytes_accessed=8_000_000, transcendentals=4_000_000),
        name="layer",
    )(*small_args, *hbm_args)


def shards(
    grouped_head_inputs,
    head_gate_inputs,
    unsmoothed_step,
    head_decay_rate,
    extra_log_decay,
    first_group_keys,
    first_group_queries,
    second_group_keys,
    second_group_queries,
    head_input_filter,
    first_group_filter,
    second_group_filter,
    head_norm_gain,
    output_weight,
    residual,
    channel_norm_gain,
    channel_gate_weight,
    channel_up_weight,
    channel_down_weight,
):
    length = grouped_head_inputs.shape[0]
    return layer(
        (
            unsmoothed_step.transpose(1, 2, 0),
            extra_log_decay.transpose(1, 2, 0),
            head_input_filter,
            first_group_filter,
            second_group_filter,
            head_norm_gain,
            channel_norm_gain[None],
            head_decay_rate,
        ),
        (
            grouped_head_inputs.reshape(2 * length, 128),
            head_gate_inputs.reshape(2 * length, 128),
            first_group_keys,
            first_group_queries,
            second_group_keys.T,
            second_group_queries.T,
            output_weight.reshape(-1, output_weight.shape[2]),
            residual.reshape(CHUNKS, 2, BLOCK, residual.shape[1]),
            channel_gate_weight,
            channel_up_weight,
            channel_down_weight,
        ),
    )


def solution(mesh):
    return jax.shard_map(
        shards,
        mesh=mesh,
        in_specs=(
            P("sp", None, "tp"),
            P("sp", None, "tp"),
            P("sp", None, "tp"),
            P(None, "tp"),
            P("sp", None, "tp"),
            P("sp", None),
            P("sp", None),
            P("sp", None),
            P("sp", None),
            P(None, None, "tp"),
            P(),
            P(),
            P(None, "tp"),
            P(None, None, "tp"),
            P("sp", "tp"),
            P(),
            P("sp", "tp"),
            P("sp", "tp"),
            P("sp", "tp"),
        ),
        out_specs=P("sp", "tp"),
        check_vma=False,
    )
```

```python
import functools

import jax
import jax.numpy as jnp
from jax import lax
from jax.experimental import pallas as pl
from jax.experimental.pallas import tpu as pltpu
from jax.sharding import PartitionSpec as P

HEAD = 64
CONV = 4
BLOCK = 128
EPSILON = 1e-06
MESH = pl.DeviceIdType.MESH
F32 = jnp.float32
BF16 = jnp.bfloat16
NY = 4
NZ = 8
NX = 4
NTP = 8
QROWS = 48
MROWS = 64
CHUNKS = 4
N_PUT = 236
SPLIT = 512
STEPS = (
    "dz1", "spread", "gy0", "gz1", "tables", "u01", "uy1", "bA", "bB", "b0", "dz2", "s1", "share",
    "ey1", "gz2", "gy1", "gr0", "s2", "uy2", "ey2", "ia", "gz3", "gy2", "gr1", "dz3", "ib", "u21",
    "gz4", "s3", "gy3", "gr-1", "u11", "ez1", "dz4", "u22", "u31", "fin0", "Ai0", "fin1", "fin2",
    "fin3", "Ai2", "gr3", "gy4", "ez2", "gr2", "u02", "dy0", "dy1", "Ar0", "u12", "Ai1", "u32",
    "Ar2", "gr-2", "Af0", "Ai3", "gr-3", "P0", "Ar1", "Af2", "Bi0", "u23", "P2", "u13", "ez3",
    "Bi2", "dr0", "Af1", "u33", "Br0", "u03", "gr4", "u24", "Ar3", "P1", "Br2", "dr1", "Bi1",
    "u14", "u34", "Bf0", "Af3", "u04", "P3", "N0", "ez4", "Bf2", "Bi3", "N2", "Br1", "H0", "D0",
    "H2", "Br3", "E0", "Bf1", "C10", "D2", "E2", "N1", "H1", "C12", "Bf3", "D1", "C20", "E1",
    "N3", "H3", "C11", "C22", "D3", "E3", "C30", "C13", "C21", "C32", "C23", "C31", "C33",
)


def mark(name):
    pass


def silu(v):
    return v * (0.5 * jnp.tanh(0.5 * v) + 0.5)


def halves(lane_low, a, b):
    return jnp.where(lane_low, a, b)


def dot(a, b, ca, cb):
    return lax.dot_general(a, b, (((ca,), (cb,)), ((), ())), preferred_element_type=F32)


def split_three(v):
    hi = v.astype(BF16)
    rest = v - hi.astype(F32)
    mid = rest.astype(BF16)
    low = (rest - mid.astype(F32)).astype(BF16)
    return hi, mid, low


def log_rows(l0, l1):
    rows = []
    for part0, part1 in zip(split_three(l0), split_three(l1)):
        rows += [part0.astype(F32), part1.astype(F32)]
    rows.append(jnp.zeros((10, 128), F32))
    return jnp.concatenate(rows, axis=0).astype(BF16)


def read_logs(rows):
    v = rows.astype(F32)
    return v[0:1] + v[2:3] + v[4:5], v[1:2] + v[3:4] + v[5:6]


class Net:
    def __init__(self, send, recv):
        self.send, self.recv, self.sent = send, recv, []

    def put(self, src, dst, to):
        index = len(self.sent)
        copy = pltpu.make_async_remote_copy(
            src_ref=src, dst_ref=dst, send_sem=self.send.at[index], recv_sem=self.recv.at[index],
            device_id=to, device_id_type=MESH)
        copy.start()
        self.sent.append(copy)
        return copy


def arrive(copies):
    for copy in copies:
        copy.wait_recv()


def layer_kernel(
    hbm_step, hbm_extra, hbm_head, hbm_taps1, hbm_taps2, hbm_gain, hbm_channel, hbm_rate,
    hx, hg, k1, q1, k2t, q2t, out_w, resid, gate_w, up_w, down_w,
    hbm_out,
    step_in, extra, head_taps, taps1, taps2, gain, channel_gain, rate, out,
    raw_x, raw_g, raw_k, raw_q, raw_t, xf, gf, pad, rim_x, rim_k, rim_q, rim_t,
    ctab, cols, keys, queries, values, local, gates, upd, starts,
    msg1, buf1, msg2, buf2, msg3, enter,
    gu, dn, wo, res, rn, mx, st, nb, hidden, ps, pr, po, relay_l, relay_r, qs, from_l, from_r,
    local_sem, send_sem, recv_sem,
):
    sp = lax.axis_index("sp")
    tp = lax.axis_index("tp")
    y = lax.rem(sp, NY)
    z = sp // NY
    core = lax.rem(tp, 2)
    x = tp // 2
    n_sp = NY * NZ
    length = k1.shape[0]
    blocks = length // BLOCK
    width = gate_w.shape[1]
    depth = wo.shape[0]
    right = lax.rem(sp + 1, n_sp)
    left = lax.rem(sp + n_sp - 1, n_sp)

    def zmod(v):
        return lax.rem(v + NZ, NZ)

    def ymod(v):
        return lax.rem(v + NY, NY)

    y_peers = [{"sp": z * NY + ymod(y + j)} for j in range(1, NY)]
    z_peers = [{"sp": zmod(z + j) * NY + y} for j in range(1, NZ)]
    to_up_y, to_down_y = {"sp": z * NY + ymod(y + 1)}, {"sp": z * NY + ymod(y - 1)}
    to_up_z, to_down_z = {"sp": zmod(z + 1) * NY + y}, {"sp": zmod(z - 1) * NY + y}
    odd = lax.rem(x, 2)
    even = 1 - odd
    slot_l = lax.rem(x + NX - 1, NX) * 2 + core
    slot_r = lax.rem(x + 1, NX) * 2 + core
    slot_o = lax.rem(x + 2, NX) * 2 + core
    partner, x_right, x_left = {"tp": x * 2 + 1 - core}, {"tp": slot_r}, {"tp": slot_l}

    mark("barrier")
    wanted = [
        (gate_w, gu.at[z, y, :, 0:width]),
        (up_w, gu.at[z, y, :, width:]),
        (down_w, dn.at[z, y]),
        (hx, raw_x),
        (k1, raw_k),
        (q1, raw_q),
        (k2t, raw_t.at[0:64]),
        (q2t, raw_t.at[64:128]),
        (hg, raw_g),
        (out_w, wo.at[:, 0:256]),
        (resid, res),
        (hbm_step, step_in),
        (hbm_extra, extra),
        (hbm_rate, rate),
        (hbm_head, head_taps),
        (hbm_taps1, taps1),
        (hbm_taps2, taps2),
        (hbm_gain, gain),
        (hbm_channel, channel_gain),
    ]
    barrier = pltpu.get_barrier_semaphore()
    greet = [{"sp": right}, {"sp": left}] + y_peers + z_peers + [partner, x_right, x_left]
    for peer in greet:
        pl.semaphore_signal(barrier, inc=1, device_id=peer, device_id_type=MESH)

    own = [pltpu.make_async_copy(a, b, local_sem.at[n]) for n, (a, b) in enumerate(wanted)]
    for copy in own:
        copy.start()

    row8 = lax.broadcasted_iota(jnp.int32, (8, 128), 0)
    low = lax.broadcasted_iota(jnp.int32, (BLOCK, 128), 1) < HEAD
    low1 = lax.broadcasted_iota(jnp.int32, (1, 128), 1) < HEAD
    at_row = lax.broadcasted_iota(jnp.int32, (BLOCK, BLOCK), 0)
    at_col = lax.broadcasted_iota(jnp.int32, (BLOCK, BLOCK), 1)
    causal = at_row >= at_col
    upper = jnp.where(at_row <= at_col, 1.0, 0.0).astype(BF16)

    mark("barwait")
    for copy in own[:8]:
        copy.wait()
    pl.semaphore_wait(barrier, len(greet))

    net = Net(send_sem, recv_sem)
    got = {}
    have = {("gz", 0)}

    def need(*key):
        if key not in have:
            have.add(key)
            arrive(got[key if len(key) > 1 else key[0]])

    tail = pl.ds(length - 16, 16)
    rims = [
        net.put(raw_x.at[pl.ds(2 * length - 16, 16)], rim_x, {"sp": right}),
        net.put(raw_k.at[tail], rim_k, {"sp": right}),
        net.put(raw_q.at[tail], rim_q, {"sp": right}),
        net.put(raw_t.at[:, pl.ds(length - BLOCK, BLOCK)], rim_t, {"sp": right}),
    ]

    def both(ref_a, ref_b, to_a, to_b):
        return net.put(ref_a, ref_a, to_a), net.put(ref_b, ref_b, to_b)

    def gate_z(r):
        need("gz", r - 1)
        a, b = zmod(z - (r - 1)), zmod(z + (r - 1))
        if r == 4:
            got["gz", r] = both(
                gu.at[a, y, 0:32, 0:width], gu.at[b, y, 32:64, 0:width], to_up_z, to_down_z)
        else:
            got["gz", r] = both(
                gu.at[a, y, :, 0:width], gu.at[b, y, :, 0:width], to_up_z, to_down_z)

    def gate_y(*ks):
        for k in ks:
            need("gz", abs(k))
            ref = gu.at[zmod(z + k), y, :, 0:width]
            got["gy", k] = both(ref, ref, to_up_y, to_down_y)

    def gate_relay(k):
        arrive(got["gy", k])
        zz = zmod(z + k)
        got["gr", k] = both(
            gu.at[zz, ymod(y - 1), 0:32, 0:width], gu.at[zz, ymod(y + 1), 32:64, 0:width],
            to_up_y, to_down_y)

    def up_y(r):
        if r == 1:
            ref = gu.at[z, y, :, width:]
            got["uy", 1] = both(ref, ref, to_up_y, to_down_y)
        else:
            need("uy", 1)
            got["uy", 2] = both(
                gu.at[z, ymod(y - 1), 0:32, width:], gu.at[z, ymod(y + 1), 32:64, width:],
                to_up_y, to_down_y)

    def up_z(c, r):
        if r > 1:
            arrive(got["uz", c, r - 1])
        elif c > 0:
            need("uy", 2 if c == 3 else 1)
        col = ymod(y + (0, -1, 1, 2)[c])
        a, b = zmod(z - (r - 1)), zmod(z + (r - 1))
        if r == 4:
            got["uz", c, r] = both(
                gu.at[a, col, 0:32, width:], gu.at[b, col, 32:64, width:], to_up_z, to_down_z)
        else:
            got["uz", c, r] = both(
                gu.at[a, col, :, width:], gu.at[b, col, :, width:], to_up_z, to_down_z)

    def down_z(r):
        if r > 1:
            arrive(got["dz", r - 1])
        a, b = zmod(z - (r - 1)), zmod(z + (r - 1))
        if r == 4:
            got["dz", r] = both(
                dn.at[a, y, 0:32, 0:SPLIT], dn.at[b, y, 32:64, 0:SPLIT], to_up_z, to_down_z)
        else:
            got["dz", r] = both(
                dn.at[a, y, :, 0:SPLIT], dn.at[b, y, :, 0:SPLIT], to_up_z, to_down_z)

    def down_y(h):
        need("dz", 4)
        ref = dn.at[4 * h : 4 * h + 4, y, :, 0:SPLIT]
        got["dy", h] = both(ref, ref, to_up_y, to_down_y)

    def down_relay(h):
        arrive(got["dy", h])
        part = pl.ds(4 * h, 4)
        got["dr", h] = both(
            dn.at[part, ymod(y - 1), 0:32, 0:SPLIT], dn.at[part, ymod(y + 1), 32:64, 0:SPLIT],
            to_up_y, to_down_y)

    def rest_y(r):
        if r == 1:
            ref = dn.at[z, y, :, SPLIT:]
            got["ey", 1] = both(ref, ref, to_up_y, to_down_y)
        else:
            need("ey", 1)
            got["ey", 2] = both(
                dn.at[z, ymod(y - 1), 0:32, SPLIT:], dn.at[z, ymod(y + 1), 32:64, SPLIT:],
                to_up_y, to_down_y)

    def rest_z(r):
        if r == 1:
            need("ey", 2)
        else:
            arrive(got["ez", r - 1])
        a, b = zmod(z - (r - 1)), zmod(z + (r - 1))
        if r == 4:
            got["ez", r] = both(
                dn.at[a, 0:2, :, SPLIT:], dn.at[b, 2:4, :, SPLIT:], to_up_z, to_down_z)
        else:
            got["ez", r] = both(
                dn.at[a, :, :, SPLIT:], dn.at[b, :, :, SPLIT:], to_up_z, to_down_z)

    def share():
        own[9].wait()
        own[10].wait()
        got["share"] = (
            net.put(res.at[:, even, :, 0:128], rn.at[0], x_left),
            net.put(res.at[:, even, :, 128:256], rn.at[1], x_right),
            net.put(wo.at[:, 0:128], wo.at[:, 256:384], x_left),
            net.put(wo.at[:, 128:256], wo.at[:, 384:512], x_right),
        )

    def mix_first(k):
        a, b = mx.at[k, tp, odd, 0:64], mx.at[k, tp, odd, 64:128]
        ref = mx.at[k, tp, even]
        got["A", k, 0] = (net.put(a, a, x_right), net.put(b, b, x_left),
                          net.put(ref, ref, x_right), net.put(ref, ref, x_left))
        ref = mx.at[k, tp, odd]
        got["A", k, 1] = [net.put(ref, ref, partner)]

    def mix_second(k):
        arrive(got["A", k, 0])
        a, b = mx.at[k, slot_l, even, 0:64], mx.at[k, slot_r, even, 64:128]
        got["A", k, 2] = (net.put(a, a, x_right), net.put(b, b, x_left))
        for slot in (slot_l, slot_r):
            ref = mx.at[k, slot, odd]
            got["A", k, 1] += [net.put(ref, ref, partner)]

    def mix_third(k):
        arrive(got["A", k, 2])
        ref = mx.at[k, slot_o, odd]
        got["A", k, 1] += [net.put(ref, ref, partner)]

    def tp_first(buf, key, k):
        ref = buf.at[k, tp]
        got[key, k, 0] = (net.put(ref, ref, x_right), net.put(ref, ref, x_left))
        got[key, k, 1] = [net.put(ref, ref, partner)]

    def tp_second(buf, key, k):
        arrive(got[key, k, 0])
        ref_l, ref_r = buf.at[k, slot_l], buf.at[k, slot_r]
        half = buf.shape[2] // 2
        a, b = ref_l.at[0:half], ref_r.at[half:]
        got[key, k, 2] = (net.put(a, a, x_right), net.put(b, b, x_left))
        got[key, k, 1] += [net.put(ref_l, ref_l, partner), net.put(ref_r, ref_r, partner)]

    def tp_third(buf, key, k):
        arrive(got[key, k, 2])
        ref = buf.at[k, slot_o]
        got[key, k, 1] += [net.put(ref, ref, partner)]

    def tp_done(key, k):
        arrive(got[key, k, 1])

    def tables():
        for copy in own[11:]:
            copy.wait()
        first_head = lax.broadcasted_iota(jnp.int32, (2, length), 0) == 0
        steps = [jax.nn.softplus(step_in[g]) for g in range(2)]
        logs = [extra[g] - steps[g] * jnp.where(first_head, rate[g : g + 1, 0:1], rate[g : g + 1, 1:2]) for g in range(2)]
        table = jnp.concatenate(
            [v[:, b * BLOCK : (b + 1) * BLOCK] for b in range(blocks) for v in logs + steps], axis=0)
        rows = table.shape[0]
        sums = dot(jnp.concatenate(split_three(table), axis=0), upper, 1, 0)
        sums = sums[0:rows] + sums[rows : 2 * rows] + sums[2 * rows :]
        offs = jnp.zeros((8, 1), F32)
        for b in range(blocks):
            cut = slice(8 * b, 8 * b + 8)
            c8 = jnp.where(row8 < 4, sums[cut], table[cut])
            ctab[b] = c8
            e8 = jnp.exp(jnp.where(row8 < 4, c8 + offs, 0.0))
            cols[b] = jnp.concatenate([c8, e8], axis=0).T
            offs = offs + c8[:, 127:128]
        log0 = halves(low1, offs[0:1], offs[1:2])
        log1 = halves(low1, offs[2:3], offs[3:4])
        my_logs = log_rows(log0, log1)
        for q in range(NY):
            msg1[q, QROWS:MROWS] = my_logs

    def spread():
        xf[0 : 2 * length] = raw_x[...].astype(F32)
        for g in range(2):
            pad[g, 8 : 8 + length] = xf[pl.ds(g, length, stride=2)]
        pad[2, 8 : 8 + length] = raw_k[...].astype(F32)
        pad[3, 8 : 8 + length] = raw_q[...].astype(F32)
        for b in range(blocks):
            pad[4, 8 + b * BLOCK : 8 + (b + 1) * BLOCK] = raw_t[:, b * BLOCK : (b + 1) * BLOCK].astype(F32).T

    def conv(n, b):
        full = pad[n, pl.ds(pl.multiple_of(b * BLOCK, BLOCK), BLOCK + 8)]
        if n < 2:
            taps = [head_taps[k, n : n + 1] for k in range(CONV)]
        elif n < 4:
            taps = [taps1[k, n - 2 : n - 1] for k in range(CONV)]
        else:
            taps = [jnp.concatenate([taps2[k, 0:1], taps2[k, 1:2]], axis=1) for k in range(CONV)]
        total = taps[0] * full[5 : 5 + BLOCK]
        for k in range(1, CONV):
            total = total + taps[k] * full[5 + k : 5 + k + BLOCK]
        return silu(total)

    def block(b, carry):
        at = pl.ds(pl.multiple_of(b * BLOCK, BLOCK), BLOCK)
        c = ctab[b]
        t = cols[b]
        key_one, mix_two = conv(2, b), conv(4, b)
        key_two = jnp.where(low, mix_two, 0.0)
        queries[1, at] = jnp.where(low, pltpu.roll(mix_two, 64, 1), 0.0).astype(BF16)
        for g, key in enumerate([key_one, key_two]):
            h = 2 * g
            v = conv(g, b) * halves(low, t[:, 4 + h : 5 + h], t[:, 5 + h : 6 + h])
            cum = halves(low, t[:, h : h + 1], t[:, h + 1 : h + 2])
            total = halves(low1, c[h : h + 1, 127:128], c[h + 1 : h + 2, 127:128])
            kb = key.astype(BF16)
            keys[g, at] = kb
            values[g, at] = v.astype(BF16)
            upd[g, b] = dot(kb, (v * jnp.exp(total - cum)).astype(BF16), 0, 0)
        return carry

    def run_blocks(lo, hi):
        lax.fori_loop(lo, hi, block, 0, unroll=2)

    def last_block():
        block(blocks - 1, 0)
        arrive(rims)
        has_left = sp > 0
        xf[0:16] = rim_x[...].astype(F32)
        for g in range(2):
            pad[g, 0:8] = jnp.where(has_left, xf[pl.ds(g, 8, stride=2)], 0.0)
        pad[2, 0:8] = jnp.where(has_left, rim_k[...].astype(F32)[8:16], 0.0)
        pad[3, 0:8] = jnp.where(has_left, rim_q[...].astype(F32)[8:16], 0.0)
        pad[4, 0:8] = jnp.where(has_left, rim_t[...].astype(F32).T[BLOCK - 8 :], 0.0)
        block(0, 0)
        ends = []
        for g in range(2):
            h = 2 * g
            state = jnp.zeros((BLOCK, 128), F32)
            for b in range(blocks):
                c = ctab[b]
                total = halves(low1, c[h : h + 1, 127:128], c[h + 1 : h + 2, 127:128])
                starts[g, b] = state.astype(BF16)
                state = state * jnp.exp(total) + upd[g, b]
            ends.append(state)
        full = jnp.concatenate([ends[0], ends[1][0:64]], axis=0).astype(BF16)
        for q in range(NY):
            msg1[q, 0:QROWS] = full[q * QROWS : (q + 1) * QROWS]

    quarter = y * QROWS + lax.broadcasted_iota(jnp.int32, (QROWS, 128), 0)
    group_one = quarter < 128

    def factor(l0, l1):
        return jnp.where(group_one, jnp.exp(l0), jnp.exp(l1))

    def stage1():
        got["s1"] = []
        for j in range(1, NY):
            to = ymod(y + j)
            got["s1"].append(net.put(msg1.at[to], buf1.at[y], {"sp": z * NY + to}))
        buf1[y] = msg1[y]

    before = []

    def stage2():
        arrive(got["s1"])
        run = jnp.zeros((QROWS, 128), F32)
        sum0 = jnp.zeros((1, 128), F32)
        sum1 = jnp.zeros((1, 128), F32)
        for j in range(NY):
            before.append((run, sum0, sum1))
            l0, l1 = read_logs(buf1[j, QROWS:MROWS])
            run = run * factor(l0, l1) + buf1[j, 0:QROWS].astype(F32)
            sum0, sum1 = sum0 + l0, sum1 + l1
        msg2[0:QROWS] = run.astype(BF16)
        msg2[QROWS:MROWS] = log_rows(sum0, sum1)
        got["s2"] = []
        for j in range(1, NZ):
            got["s2"].append(net.put(msg2, buf2.at[z], {"sp": zmod(z + j) * NY + y}))
        buf2[z] = msg2[...]

    def stage3():
        arrive(got["s2"])
        run = jnp.zeros((QROWS, 128), F32)
        for j in range(NZ):
            l0, l1 = read_logs(buf2[j, QROWS:MROWS])
            new = run * factor(l0, l1) + buf2[j, 0:QROWS].astype(F32)
            run = jnp.where(j < z, new, run)
        for j in range(NY):
            part, l0, l1 = before[j]
            msg3[j] = (run * factor(l0, l1) + part).astype(BF16)
        mine = pl.ds(pl.multiple_of(y * QROWS, 16), QROWS)
        got["s3"] = []
        for j in range(1, NY):
            to = ymod(y + j)
            got["s3"].append(net.put(msg3.at[to], enter.at[mine], {"sp": z * NY + to}))
        enter[mine] = msg3[y]

    def inside(b, carry):
        at = pl.ds(pl.multiple_of(b * BLOCK, BLOCK), BLOCK)
        t = cols[b]
        c = ctab[b]
        queries[0, at] = conv(3, b).astype(BF16)
        for g in range(2):
            h = 2 * g
            qb, v = queries[g, at], values[g, at]
            scores = dot(qb, keys[g, at], 1, 1)
            weights = []
            for j in range(2):
                span = t[:, h + j : h + j + 1] - c[h + j : h + j + 1]
                weights.append((jnp.exp(jnp.where(causal, span, -jnp.inf)) * scores).astype(BF16))
            zero = jnp.zeros_like(v)
            two = jnp.concatenate([jnp.where(low, v, zero), jnp.where(low, zero, v)], axis=0)
            cum = halves(low, t[:, h : h + 1], t[:, h + 1 : h + 2])
            local[g, at] = dot(jnp.concatenate(weights, axis=1), two, 1, 0) + dot(
                qb, starts[g, b], 1, 0) * jnp.exp(cum)
        return carry

    def inside_a():
        own[8].wait()
        gf[0 : 2 * length] = raw_g[...].astype(F32)
        for g in range(2):
            gates[g] = silu(gf[pl.ds(g, length, stride=2)])
        lax.fori_loop(0, blocks // 2, inside, 0, unroll=2)

    def inside_b():
        lax.fori_loop(blocks // 2, blocks, inside, 0, unroll=2)

    per = blocks // CHUNKS
    tokens = BLOCK * per

    def finish(k):
        need("s3")
        for i in range(per):
            b = k * per + i
            at = slice(b * BLOCK, (b + 1) * BLOCK)
            t = cols[b]
            for g in range(2):
                h = 8 + 2 * g
                if g == 0:
                    entering = enter[0:128]
                else:
                    entering = jnp.concatenate([enter[128:192], jnp.zeros((64, 128), BF16)], axis=0)
                m = local[g, at] + dot(queries[g, at], entering, 1, 0) * halves(
                    low, t[:, h : h + 1], t[:, h + 1 : h + 2])
                m = m * gates[g, at]
                square = m * m
                s0 = jnp.sum(jnp.where(low, square, 0.0), axis=1, keepdims=True)
                s1 = jnp.sum(jnp.where(low, 0.0, square), axis=1, keepdims=True)
                scale = lax.rsqrt(halves(low, s0, s1) * (1.0 / HEAD) + EPSILON)
                mx[k, tp, i, :, g * 128 : (g + 1) * 128] = (
                    m * scale * gain[g : g + 1]).astype(BF16)

    def project(k):
        need("share")
        tp_done("A", k)
        lhs = jnp.concatenate(
            [mx[k, s, odd, :, g * 128 : (g + 1) * 128] for g in range(2) for s in range(NTP)], axis=1)
        base = jnp.concatenate([res[k, odd], rn[0, k], rn[1, k]], axis=1)
        st[k, tp] = (dot(lhs, wo[...], 1, 0) + base.astype(F32)).astype(BF16)

    def stream_of(k, q, xx, cc):
        if xx % 2 == q:
            return st[k, 2 * xx + cc, :, 0:256]
        return jnp.concatenate(
            [st[k, 2 * ((xx - 1) % NX) + cc, :, 256:384], st[k, 2 * ((xx + 1) % NX) + cc, :, 384:512]],
            axis=1)

    def norm(k):
        tp_done("B", k)
        for q in range(2):
            square = jnp.zeros((BLOCK, 128), F32)
            for slot in (2 * q, 2 * q + 1, 2 * q + 4, 2 * q + 5):
                v = st[k, slot].astype(F32)
                for c in range(4):
                    piece = v[:, c * 128 : (c + 1) * 128]
                    square = square + piece * piece
            scale = lax.rsqrt(jnp.sum(square, axis=1, keepdims=True) * (1.0 / depth) + EPSILON)
            for slot in range(NTP):
                cut = slice(slot * 256, (slot + 1) * 256)
                v = stream_of(k, q, slot // 2, slot % 2).astype(F32)
                nb[k, q * BLOCK : (q + 1) * BLOCK, cut] = (v * scale * channel_gain[:, cut]).astype(BF16)

    def hidden_units(k):
        for j in (0, 1, -1, 2, -2, 3, -3, 4):
            need("gr", j)
        for c in range(NY):
            need("uz", c, 4)
        pair = dot(nb[k], gu[...].reshape(depth, 2 * width), 1, 0)
        hidden[k] = (silu(pair[:, :width]) * pair[:, width:]).astype(BF16)

    order = (2, 3, 1, 0)
    dests = {k: lax.rem(x + k, NX) * 2 for k in order}

    def down(k, d):
        return dot(hidden[k], dn[d].reshape(256, width), 1, 1).astype(BF16)

    def down_partner(k):
        need("dr", 0)
        need("dr", 1)
        need("ez", 4)
        for j in order:
            ps[k, j] = down(k, dests[j] + 1 - core)
        for j in order:
            got["P", k, j] = net.put(ps.at[k, j], pr.at[k, j], partner)

    def down_own(k):
        for j in order:
            po[k, j] = down(k, dests[j] + core)

    def pair_sum(k, j):
        got["P", k, j].wait_recv()
        return po[k, j].astype(F32) + pr[k, j].astype(F32)

    mid = tokens // 2
    outs = []

    def sum_first(k):
        qs[k, 2] = pair_sum(k, 2).astype(BF16)
        got["C1", k] = (net.put(qs.at[k, 2, 0:mid], relay_r.at[k], x_left),
                        net.put(qs.at[k, 2, mid:], relay_l.at[k], x_right))

    def sum_second(k):
        to_left, to_right = pair_sum(k, 3), pair_sum(k, 1)
        arrive(got["C1", k])
        qs[k, 3, 0:mid] = (to_left[0:mid] + relay_r[k].astype(F32)).astype(BF16)
        qs[k, 3, mid:] = to_left[mid:].astype(BF16)
        qs[k, 1, 0:mid] = to_right[0:mid].astype(BF16)
        qs[k, 1, mid:] = (to_right[mid:] + relay_l[k].astype(F32)).astype(BF16)
        got["C2", k] = (net.put(qs.at[k, 3], from_r.at[k], x_left),
                        net.put(qs.at[k, 1], from_l.at[k], x_right))

    def sum_third(k):
        total = pair_sum(k, 0)
        arrive(got["C2", k])
        total = total + from_l[k].astype(F32) + from_r[k].astype(F32)
        mine = st[k, tp, :, 0:256].astype(F32)
        other = jnp.concatenate(
            [st[k, slot_l, :, 256:384], st[k, slot_r, :, 384:512]], axis=1).astype(F32)
        for q in range(2):
            at = k * tokens + q * BLOCK
            stream = jnp.where(odd == q, mine, other)
            out[at : at + BLOCK] = (
                stream + 0.5 * total[q * BLOCK : (q + 1) * BLOCK]).astype(BF16)
        rows = pl.ds(k * tokens, tokens)
        copy = pltpu.make_async_copy(out.at[rows], hbm_out.at[rows], local_sem.at[19 + k])
        copy.start()
        outs.append(copy)

    run = {
        "tables": tables,
        "spread": spread,
        "bA": lambda: run_blocks(1, 5),
        "bB": lambda: run_blocks(5, 7),
        "b0": last_block,
        "s1": stage1,
        "s2": stage2,
        "s3": stage3,
        "ia": inside_a,
        "ib": inside_b,
        "gy0": lambda: gate_y(0),
        "gy1": lambda: gate_y(1, -1),
        "gy2": lambda: gate_y(2, -2),
        "gy3": lambda: gate_y(3, -3),
        "gy4": lambda: gate_y(4),
        "uy1": lambda: up_y(1),
        "uy2": lambda: up_y(2),
        "dy0": lambda: down_y(0),
        "dy1": lambda: down_y(1),
        "ey1": lambda: rest_y(1),
        "ey2": lambda: rest_y(2),
        "dr0": lambda: down_relay(0),
        "dr1": lambda: down_relay(1),
        "share": share,
    }
    for r in (1, 2, 3, 4):
        run[f"gz{r}"] = functools.partial(gate_z, r)
        for c in range(NY):
            run[f"u{c}{r}"] = functools.partial(up_z, c, r)
        run[f"dz{r}"] = functools.partial(down_z, r)
        run[f"ez{r}"] = functools.partial(rest_z, r)
    for k in (0, 1, -1, 2, -2, 3, -3, 4):
        run[f"gr{k}"] = functools.partial(gate_relay, k)
    for k in range(CHUNKS):
        run[f"fin{k}"] = functools.partial(finish, k)
        run[f"P{k}"] = functools.partial(project, k)
        run[f"N{k}"] = functools.partial(norm, k)
        run[f"H{k}"] = functools.partial(hidden_units, k)
        run[f"D{k}"] = functools.partial(down_partner, k)
        run[f"E{k}"] = functools.partial(down_own, k)
        run[f"C1{k}"] = functools.partial(sum_first, k)
        run[f"C2{k}"] = functools.partial(sum_second, k)
        run[f"C3{k}"] = functools.partial(sum_third, k)
        run[f"Ai{k}"] = functools.partial(mix_first, k)
        run[f"Ar{k}"] = functools.partial(mix_second, k)
        run[f"Af{k}"] = functools.partial(mix_third, k)
        run[f"Bi{k}"] = functools.partial(tp_first, st, "B", k)
        run[f"Br{k}"] = functools.partial(tp_second, st, "B", k)
        run[f"Bf{k}"] = functools.partial(tp_third, st, "B", k)
    for name in STEPS:
        mark(name)
        run.pop(name)()
    assert not run

    mark("sends")
    for copy in outs:
        copy.wait()
    for copy in net.sent:
        copy.wait_send()


def layer(small_args, hbm_args):
    length = hbm_args[2].shape[0]
    blocks = length // BLOCK
    tokens = length // CHUNKS
    width = hbm_args[8].shape[1]
    hbm = pl.BlockSpec(memory_space=pl.ANY)
    dma = pltpu.SemaphoreType.DMA

    def bf(*shape):
        return pltpu.VMEM(shape, BF16)

    def fl(*shape):
        return pltpu.VMEM(shape, F32)

    return pl.pallas_call(
        layer_kernel,
        out_shape=jax.ShapeDtypeStruct((length, 256), BF16),
        in_specs=[hbm] * (len(small_args) + len(hbm_args)),
        out_specs=hbm,
        scratch_shapes=[fl(*a.shape) for a in small_args]
        + [
            bf(length, 256),
            bf(2 * length, 128), bf(2 * length, 128), bf(length, 128), bf(length, 128),
            bf(128, length), fl(2 * length + 16, 128), fl(2 * length + 16, 128), fl(5, length + 8, 128),
            bf(16, 128), bf(16, 128), bf(16, 128), bf(128, 128),
            fl(blocks, 8, 128), fl(blocks, BLOCK, 16),
            bf(2, length, 128), bf(2, length, 128), bf(2, length, 128),
            fl(2, length, 128), fl(2, length, 128),
            fl(2, blocks, 128, 128), bf(2, blocks, 128, 128),
            bf(NY, MROWS, 128), bf(NY, MROWS, 128), bf(MROWS, 128), bf(NZ, MROWS, 128),
            bf(NY, QROWS, 128), bf(NY * QROWS, 128),
            bf(NZ, NY, 64, 2 * width), bf(NZ, NY, 64, width), bf(2048, 512),
            bf(CHUNKS, 2, BLOCK, 256), bf(2, CHUNKS, BLOCK, 128),
            bf(CHUNKS, NTP, 2, BLOCK, 256), bf(CHUNKS, NTP, BLOCK, 512),
            bf(CHUNKS, tokens, 2048), bf(CHUNKS, tokens, width),
            bf(CHUNKS, NX, tokens, 256), bf(CHUNKS, NX, tokens, 256), bf(CHUNKS, NX, tokens, 256),
            bf(CHUNKS, tokens // 2, 256), bf(CHUNKS, tokens // 2, 256),
            bf(CHUNKS, NX, tokens, 256), bf(CHUNKS, tokens, 256), bf(CHUNKS, tokens, 256),
            dma((19 + CHUNKS,)), dma((N_PUT,)), dma((N_PUT,)),
        ],
        compiler_params=pltpu.CompilerParams(
            collective_id=0, has_side_effects=True, vmem_limit_bytes=58 * 1024 * 1024),
        cost_estimate=pl.CostEstimate(
            flops=12_000_000_000, bytes_accessed=8_000_000, transcendentals=4_000_000),
        name="layer",
    )(*small_args, *hbm_args)


def shards(
    grouped_head_inputs,
    head_gate_inputs,
    unsmoothed_step,
    head_decay_rate,
    extra_log_decay,
    first_group_keys,
    first_group_queries,
    second_group_keys,
    second_group_queries,
    head_input_filter,
    first_group_filter,
    second_group_filter,
    head_norm_gain,
    output_weight,
    residual,
    channel_norm_gain,
    channel_gate_weight,
    channel_up_weight,
    channel_down_weight,
):
    length = grouped_head_inputs.shape[0]
    return layer(
        (
            unsmoothed_step.transpose(1, 2, 0),
            extra_log_decay.transpose(1, 2, 0),
            head_input_filter,
            first_group_filter,
            second_group_filter,
            head_norm_gain,
            channel_norm_gain[None],
            head_decay_rate,
        ),
        (
            grouped_head_inputs.reshape(2 * length, 128),
            head_gate_inputs.reshape(2 * length, 128),
            first_group_keys,
            first_group_queries,
            second_group_keys.T,
            second_group_queries.T,
            output_weight.reshape(-1, output_weight.shape[2]),
            residual.reshape(CHUNKS, 2, BLOCK, residual.shape[1]),
            channel_gate_weight,
            channel_up_weight,
            channel_down_weight,
        ),
    )


def solution(mesh):
    return jax.shard_map(
        shards,
        mesh=mesh,
        in_specs=(
            P("sp", None, "tp"),
            P("sp", None, "tp"),
            P("sp", None, "tp"),
            P(None, "tp"),
            P("sp", None, "tp"),
            P("sp", None),
            P("sp", None),
            P("sp", None),
            P("sp", None),
            P(None, None, "tp"),
            P(),
            P(),
            P(None, "tp"),
            P(None, None, "tp"),
            P("sp", "tp"),
            P(),
            P("sp", "tp"),
            P("sp", "tp"),
            P("sp", "tp"),
        ),
        out_specs=P("sp", "tp"),
        check_vma=False,
    )
```

```python
import functools

import jax
import jax.numpy as jnp
from jax import lax
from jax.experimental import pallas as pl
from jax.experimental.pallas import tpu as pltpu
from jax.sharding import PartitionSpec as P

HEAD = 64
CONV = 4
BLOCK = 128
EPSILON = 1e-06
MESH = pl.DeviceIdType.MESH
F32 = jnp.float32
BF16 = jnp.bfloat16
NY = 4
NZ = 8
NX = 4
NTP = 8
QROWS = 48
MROWS = 64
CHUNKS = 4
N_PUT = 236
SPLIT = 512
STEPS = (
    "gz1", "ey1", "dz1", "spread", "tables", "gy0", "uy1", "u01", "bA", "bB", "b0", "share",
    "gz2", "s1", "dz2", "ey2", "gr0", "gy1", "s2", "ia", "dz3", "gz3", "ez1", "uy2", "gy2", "gr1",
    "u21", "ib", "dz4", "u02", "s3", "gr-1", "u11", "gy3", "fin0", "Ai0", "fin1", "fin2", "dy1",
    "gr-2", "u22", "fin3", "gr2", "u31", "dy0", "Ai1", "Ar0", "Ai2", "gr3", "gz4", "gr-3", "u12",
    "Ar1", "u03", "Ai3", "ez2", "Af0", "P0", "Ar2", "u32", "Bi0", "gy4", "Af1", "u23", "P1",
    "Af2", "Bi1", "Ar3", "dr1", "u13", "u33", "Br0", "u24", "P2", "Br1", "u14", "Bi2", "ez3",
    "u04", "Af3", "gr4", "P3", "dr0", "u34", "Bi3", "Bf0", "Bf1", "ez4", "N0", "N1", "Br2", "H1",
    "D1", "Br3", "H0", "Bf2", "D0", "E1", "C11", "N2", "E0", "Bf3", "C10", "H2", "D2", "C21",
    "N3", "E2", "C12", "H3", "C20", "D3", "C31", "E3", "C13", "C22", "C30", "C23", "C32", "C33",
)


def mark(name):
    pass


def silu(v):
    return v * (0.5 * jnp.tanh(0.5 * v) + 0.5)


def halves(lane_low, a, b):
    return jnp.where(lane_low, a, b)


def dot(a, b, ca, cb):
    return lax.dot_general(a, b, (((ca,), (cb,)), ((), ())), preferred_element_type=F32)


def split_three(v):
    hi = v.astype(BF16)
    rest = v - hi.astype(F32)
    mid = rest.astype(BF16)
    low = (rest - mid.astype(F32)).astype(BF16)
    return hi, mid, low


def log_rows(l0, l1):
    rows = []
    for part0, part1 in zip(split_three(l0), split_three(l1)):
        rows += [part0.astype(F32), part1.astype(F32)]
    rows.append(jnp.zeros((10, 128), F32))
    return jnp.concatenate(rows, axis=0).astype(BF16)


def read_logs(rows):
    v = rows.astype(F32)
    return v[0:1] + v[2:3] + v[4:5], v[1:2] + v[3:4] + v[5:6]


class Net:
    def __init__(self, send, recv):
        self.send, self.recv, self.sent = send, recv, []

    def put(self, src, dst, to):
        index = len(self.sent)
        copy = pltpu.make_async_remote_copy(
            src_ref=src, dst_ref=dst, send_sem=self.send.at[index], recv_sem=self.recv.at[index],
            device_id=to, device_id_type=MESH)
        copy.start()
        self.sent.append(copy)
        return copy


def arrive(copies):
    for copy in copies:
        copy.wait_recv()


def layer_kernel(
    hbm_step, hbm_extra, hbm_head, hbm_taps1, hbm_taps2, hbm_gain, hbm_channel, hbm_rate,
    hx, hg, k1, q1, k2t, q2t, out_w, resid, gate_w, up_w, down_w,
    hbm_out,
    step_in, extra, head_taps, taps1, taps2, gain, channel_gain, rate, out,
    raw_x, raw_g, raw_k, raw_q, raw_t, xf, gf, pad, rim_x, rim_k, rim_q, rim_t,
    ctab, cols, keys, queries, values, local, gates, upd, starts,
    msg1, buf1, msg2, buf2, msg3, enter,
    gu, dn, wo, res, rn, mx, st, nb, hidden, ps, pr, po, relay_l, relay_r, qs, from_l, from_r,
    local_sem, send_sem, recv_sem,
):
    sp = lax.axis_index("sp")
    tp = lax.axis_index("tp")
    y = lax.rem(sp, NY)
    z = sp // NY
    core = lax.rem(tp, 2)
    x = tp // 2
    n_sp = NY * NZ
    length = k1.shape[0]
    blocks = length // BLOCK
    width = gate_w.shape[1]
    depth = wo.shape[0]
    right = lax.rem(sp + 1, n_sp)
    left = lax.rem(sp + n_sp - 1, n_sp)

    def zmod(v):
        return lax.rem(v + NZ, NZ)

    def ymod(v):
        return lax.rem(v + NY, NY)

    y_peers = [{"sp": z * NY + ymod(y + j)} for j in range(1, NY)]
    z_peers = [{"sp": zmod(z + j) * NY + y} for j in range(1, NZ)]
    to_up_y, to_down_y = {"sp": z * NY + ymod(y + 1)}, {"sp": z * NY + ymod(y - 1)}
    to_up_z, to_down_z = {"sp": zmod(z + 1) * NY + y}, {"sp": zmod(z - 1) * NY + y}
    odd = lax.rem(x, 2)
    even = 1 - odd
    slot_l = lax.rem(x + NX - 1, NX) * 2 + core
    slot_r = lax.rem(x + 1, NX) * 2 + core
    slot_o = lax.rem(x + 2, NX) * 2 + core
    partner, x_right, x_left = {"tp": x * 2 + 1 - core}, {"tp": slot_r}, {"tp": slot_l}

    mark("barrier")
    wanted = [
        (gate_w, gu.at[z, y, :, 0:width]),
        (up_w, gu.at[z, y, :, width:]),
        (down_w, dn.at[z, y]),
        (hx, raw_x),
        (k1, raw_k),
        (q1, raw_q),
        (k2t, raw_t.at[0:64]),
        (q2t, raw_t.at[64:128]),
        (hg, raw_g),
        (out_w, wo.at[:, 0:256]),
        (resid, res),
        (hbm_step, step_in),
        (hbm_extra, extra),
        (hbm_rate, rate),
        (hbm_head, head_taps),
        (hbm_taps1, taps1),
        (hbm_taps2, taps2),
        (hbm_gain, gain),
        (hbm_channel, channel_gain),
    ]
    barrier = pltpu.get_barrier_semaphore()
    greet = [{"sp": right}, {"sp": left}] + y_peers + z_peers + [partner, x_right, x_left]
    for peer in greet:
        pl.semaphore_signal(barrier, inc=1, device_id=peer, device_id_type=MESH)

    own = [pltpu.make_async_copy(a, b, local_sem.at[n]) for n, (a, b) in enumerate(wanted)]
    for copy in own:
        copy.start()

    row8 = lax.broadcasted_iota(jnp.int32, (8, 128), 0)
    low = lax.broadcasted_iota(jnp.int32, (BLOCK, 128), 1) < HEAD
    low1 = lax.broadcasted_iota(jnp.int32, (1, 128), 1) < HEAD
    at_row = lax.broadcasted_iota(jnp.int32, (BLOCK, BLOCK), 0)
    at_col = lax.broadcasted_iota(jnp.int32, (BLOCK, BLOCK), 1)
    causal = at_row >= at_col
    upper = jnp.where(at_row <= at_col, 1.0, 0.0).astype(BF16)

    mark("barwait")
    for copy in own[:8]:
        copy.wait()
    pl.semaphore_wait(barrier, len(greet))

    net = Net(send_sem, recv_sem)
    got = {}
    have = {("gz", 0)}

    def need(*key):
        if key not in have:
            have.add(key)
            arrive(got[key if len(key) > 1 else key[0]])

    tail = pl.ds(length - 16, 16)
    rims = [
        net.put(raw_x.at[pl.ds(2 * length - 16, 16)], rim_x, {"sp": right}),
        net.put(raw_k.at[tail], rim_k, {"sp": right}),
        net.put(raw_q.at[tail], rim_q, {"sp": right}),
        net.put(raw_t.at[:, pl.ds(length - BLOCK, BLOCK)], rim_t, {"sp": right}),
    ]

    def both(ref_a, ref_b, to_a, to_b):
        return net.put(ref_a, ref_a, to_a), net.put(ref_b, ref_b, to_b)

    def gate_z(r):
        need("gz", r - 1)
        a, b = zmod(z - (r - 1)), zmod(z + (r - 1))
        if r == 4:
            got["gz", r] = both(
                gu.at[a, y, 0:32, 0:width], gu.at[b, y, 32:64, 0:width], to_up_z, to_down_z)
        else:
            got["gz", r] = both(
                gu.at[a, y, :, 0:width], gu.at[b, y, :, 0:width], to_up_z, to_down_z)

    def gate_y(*ks):
        for k in ks:
            need("gz", abs(k))
            ref = gu.at[zmod(z + k), y, :, 0:width]
            got["gy", k] = both(ref, ref, to_up_y, to_down_y)

    def gate_relay(k):
        arrive(got["gy", k])
        zz = zmod(z + k)
        got["gr", k] = both(
            gu.at[zz, ymod(y - 1), 0:32, 0:width], gu.at[zz, ymod(y + 1), 32:64, 0:width],
            to_up_y, to_down_y)

    def up_y(r):
        if r == 1:
            ref = gu.at[z, y, :, width:]
            got["uy", 1] = both(ref, ref, to_up_y, to_down_y)
        else:
            need("uy", 1)
            got["uy", 2] = both(
                gu.at[z, ymod(y - 1), 0:32, width:], gu.at[z, ymod(y + 1), 32:64, width:],
                to_up_y, to_down_y)

    def up_z(c, r):
        if r > 1:
            arrive(got["uz", c, r - 1])
        elif c > 0:
            need("uy", 2 if c == 3 else 1)
        col = ymod(y + (0, -1, 1, 2)[c])
        a, b = zmod(z - (r - 1)), zmod(z + (r - 1))
        if r == 4:
            got["uz", c, r] = both(
                gu.at[a, col, 0:32, width:], gu.at[b, col, 32:64, width:], to_up_z, to_down_z)
        else:
            got["uz", c, r] = both(
                gu.at[a, col, :, width:], gu.at[b, col, :, width:], to_up_z, to_down_z)

    def down_z(r):
        if r > 1:
            arrive(got["dz", r - 1])
        a, b = zmod(z - (r - 1)), zmod(z + (r - 1))
        if r == 4:
            got["dz", r] = both(
                dn.at[a, y, 0:32, 0:SPLIT], dn.at[b, y, 32:64, 0:SPLIT], to_up_z, to_down_z)
        else:
            got["dz", r] = both(
                dn.at[a, y, :, 0:SPLIT], dn.at[b, y, :, 0:SPLIT], to_up_z, to_down_z)

    def down_y(h):
        need("dz", 4)
        ref = dn.at[4 * h : 4 * h + 4, y, :, 0:SPLIT]
        got["dy", h] = both(ref, ref, to_up_y, to_down_y)

    def down_relay(h):
        arrive(got["dy", h])
        part = pl.ds(4 * h, 4)
        got["dr", h] = both(
            dn.at[part, ymod(y - 1), 0:32, 0:SPLIT], dn.at[part, ymod(y + 1), 32:64, 0:SPLIT],
            to_up_y, to_down_y)

    def rest_y(r):
        if r == 1:
            ref = dn.at[z, y, :, SPLIT:]
            got["ey", 1] = both(ref, ref, to_up_y, to_down_y)
        else:
            need("ey", 1)
            got["ey", 2] = both(
                dn.at[z, ymod(y - 1), 0:32, SPLIT:], dn.at[z, ymod(y + 1), 32:64, SPLIT:],
                to_up_y, to_down_y)

    def rest_z(r):
        if r == 1:
            need("ey", 2)
        else:
            arrive(got["ez", r - 1])
        a, b = zmod(z - (r - 1)), zmod(z + (r - 1))
        if r == 4:
            got["ez", r] = both(
                dn.at[a, 0:2, :, SPLIT:], dn.at[b, 2:4, :, SPLIT:], to_up_z, to_down_z)
        else:
            got["ez", r] = both(
                dn.at[a, :, :, SPLIT:], dn.at[b, :, :, SPLIT:], to_up_z, to_down_z)

    def share():
        own[9].wait()
        own[10].wait()
        got["share"] = (
            net.put(res.at[:, even, :, 0:128], rn.at[0], x_left),
            net.put(res.at[:, even, :, 128:256], rn.at[1], x_right),
            net.put(wo.at[:, 0:128], wo.at[:, 256:384], x_left),
            net.put(wo.at[:, 128:256], wo.at[:, 384:512], x_right),
        )

    def mix_first(k):
        a, b = mx.at[k, tp, odd, 0:64], mx.at[k, tp, odd, 64:128]
        ref = mx.at[k, tp, even]
        got["A", k, 0] = (net.put(a, a, x_right), net.put(b, b, x_left),
                          net.put(ref, ref, x_right), net.put(ref, ref, x_left))
        ref = mx.at[k, tp, odd]
        got["A", k, 1] = [net.put(ref, ref, partner)]

    def mix_second(k):
        arrive(got["A", k, 0])
        a, b = mx.at[k, slot_l, even, 0:64], mx.at[k, slot_r, even, 64:128]
        got["A", k, 2] = (net.put(a, a, x_right), net.put(b, b, x_left))
        for slot in (slot_l, slot_r):
            ref = mx.at[k, slot, odd]
            got["A", k, 1] += [net.put(ref, ref, partner)]

    def mix_third(k):
        arrive(got["A", k, 2])
        ref = mx.at[k, slot_o, odd]
        got["A", k, 1] += [net.put(ref, ref, partner)]

    def tp_first(buf, key, k):
        ref = buf.at[k, tp]
        got[key, k, 0] = (net.put(ref, ref, x_right), net.put(ref, ref, x_left))
        got[key, k, 1] = [net.put(ref, ref, partner)]

    def tp_second(buf, key, k):
        arrive(got[key, k, 0])
        ref_l, ref_r = buf.at[k, slot_l], buf.at[k, slot_r]
        half = buf.shape[2] // 2
        a, b = ref_l.at[0:half], ref_r.at[half:]
        got[key, k, 2] = (net.put(a, a, x_right), net.put(b, b, x_left))
        got[key, k, 1] += [net.put(ref_l, ref_l, partner), net.put(ref_r, ref_r, partner)]

    def tp_third(buf, key, k):
        arrive(got[key, k, 2])
        ref = buf.at[k, slot_o]
        got[key, k, 1] += [net.put(ref, ref, partner)]

    def tp_done(key, k):
        arrive(got[key, k, 1])

    def tables():
        for copy in own[11:]:
            copy.wait()
        first_head = lax.broadcasted_iota(jnp.int32, (2, length), 0) == 0
        steps = [jax.nn.softplus(step_in[g]) for g in range(2)]
        logs = [extra[g] - steps[g] * jnp.where(first_head, rate[g : g + 1, 0:1], rate[g : g + 1, 1:2]) for g in range(2)]
        table = jnp.concatenate(
            [v[:, b * BLOCK : (b + 1) * BLOCK] for b in range(blocks) for v in logs + steps], axis=0)
        rows = table.shape[0]
        sums = dot(jnp.concatenate(split_three(table), axis=0), upper, 1, 0)
        sums = sums[0:rows] + sums[rows : 2 * rows] + sums[2 * rows :]
        offs = jnp.zeros((8, 1), F32)
        for b in range(blocks):
            cut = slice(8 * b, 8 * b + 8)
            c8 = jnp.where(row8 < 4, sums[cut], table[cut])
            ctab[b] = c8
            e8 = jnp.exp(jnp.where(row8 < 4, c8 + offs, 0.0))
            cols[b] = jnp.concatenate([c8, e8], axis=0).T
            offs = offs + c8[:, 127:128]
        log0 = halves(low1, offs[0:1], offs[1:2])
        log1 = halves(low1, offs[2:3], offs[3:4])
        my_logs = log_rows(log0, log1)
        for q in range(NY):
            msg1[q, QROWS:MROWS] = my_logs

    def spread():
        xf[0 : 2 * length] = raw_x[...].astype(F32)
        for g in range(2):
            pad[g, 8 : 8 + length] = xf[pl.ds(g, length, stride=2)]
        pad[2, 8 : 8 + length] = raw_k[...].astype(F32)
        pad[3, 8 : 8 + length] = raw_q[...].astype(F32)
        for b in range(blocks):
            pad[4, 8 + b * BLOCK : 8 + (b + 1) * BLOCK] = raw_t[:, b * BLOCK : (b + 1) * BLOCK].astype(F32).T

    def conv(n, b):
        full = pad[n, pl.ds(pl.multiple_of(b * BLOCK, BLOCK), BLOCK + 8)]
        if n < 2:
            taps = [head_taps[k, n : n + 1] for k in range(CONV)]
        elif n < 4:
            taps = [taps1[k, n - 2 : n - 1] for k in range(CONV)]
        else:
            taps = [jnp.concatenate([taps2[k, 0:1], taps2[k, 1:2]], axis=1) for k in range(CONV)]
        total = taps[0] * full[5 : 5 + BLOCK]
        for k in range(1, CONV):
            total = total + taps[k] * full[5 + k : 5 + k + BLOCK]
        return silu(total)

    def block(b, carry):
        at = pl.ds(pl.multiple_of(b * BLOCK, BLOCK), BLOCK)
        c = ctab[b]
        t = cols[b]
        key_one, mix_two = conv(2, b), conv(4, b)
        key_two = jnp.where(low, mix_two, 0.0)
        queries[1, at] = jnp.where(low, pltpu.roll(mix_two, 64, 1), 0.0).astype(BF16)
        for g, key in enumerate([key_one, key_two]):
            h = 2 * g
            v = conv(g, b) * halves(low, t[:, 4 + h : 5 + h], t[:, 5 + h : 6 + h])
            cum = halves(low, t[:, h : h + 1], t[:, h + 1 : h + 2])
            total = halves(low1, c[h : h + 1, 127:128], c[h + 1 : h + 2, 127:128])
            kb = key.astype(BF16)
            keys[g, at] = kb
            values[g, at] = v.astype(BF16)
            upd[g, b] = dot(kb, (v * jnp.exp(total - cum)).astype(BF16), 0, 0)
        return carry

    def run_blocks(lo, hi):
        lax.fori_loop(lo, hi, block, 0, unroll=2)

    def last_block():
        block(blocks - 1, 0)
        arrive(rims)
        has_left = sp > 0
        xf[0:16] = rim_x[...].astype(F32)
        for g in range(2):
            pad[g, 0:8] = jnp.where(has_left, xf[pl.ds(g, 8, stride=2)], 0.0)
        pad[2, 0:8] = jnp.where(has_left, rim_k[...].astype(F32)[8:16], 0.0)
        pad[3, 0:8] = jnp.where(has_left, rim_q[...].astype(F32)[8:16], 0.0)
        pad[4, 0:8] = jnp.where(has_left, rim_t[...].astype(F32).T[BLOCK - 8 :], 0.0)
        block(0, 0)
        ends = []
        for g in range(2):
            h = 2 * g
            state = jnp.zeros((BLOCK, 128), F32)
            for b in range(blocks):
                c = ctab[b]
                total = halves(low1, c[h : h + 1, 127:128], c[h + 1 : h + 2, 127:128])
                starts[g, b] = state.astype(BF16)
                state = state * jnp.exp(total) + upd[g, b]
            ends.append(state)
        full = jnp.concatenate([ends[0], ends[1][0:64]], axis=0).astype(BF16)
        for q in range(NY):
            msg1[q, 0:QROWS] = full[q * QROWS : (q + 1) * QROWS]

    quarter = y * QROWS + lax.broadcasted_iota(jnp.int32, (QROWS, 128), 0)
    group_one = quarter < 128

    def factor(l0, l1):
        return jnp.where(group_one, jnp.exp(l0), jnp.exp(l1))

    def stage1():
        got["s1"] = []
        for j in range(1, NY):
            to = ymod(y + j)
            got["s1"].append(net.put(msg1.at[to], buf1.at[y], {"sp": z * NY + to}))
        buf1[y] = msg1[y]

    before = []

    def stage2():
        arrive(got["s1"])
        run = jnp.zeros((QROWS, 128), F32)
        sum0 = jnp.zeros((1, 128), F32)
        sum1 = jnp.zeros((1, 128), F32)
        for j in range(NY):
            before.append((run, sum0, sum1))
            l0, l1 = read_logs(buf1[j, QROWS:MROWS])
            run = run * factor(l0, l1) + buf1[j, 0:QROWS].astype(F32)
            sum0, sum1 = sum0 + l0, sum1 + l1
        msg2[0:QROWS] = run.astype(BF16)
        msg2[QROWS:MROWS] = log_rows(sum0, sum1)
        got["s2"] = []
        for j in range(1, NZ):
            got["s2"].append(net.put(msg2, buf2.at[z], {"sp": zmod(z + j) * NY + y}))
        buf2[z] = msg2[...]

    def stage3():
        arrive(got["s2"])
        run = jnp.zeros((QROWS, 128), F32)
        for j in range(NZ):
            l0, l1 = read_logs(buf2[j, QROWS:MROWS])
            new = run * factor(l0, l1) + buf2[j, 0:QROWS].astype(F32)
            run = jnp.where(j < z, new, run)
        for j in range(NY):
            part, l0, l1 = before[j]
            msg3[j] = (run * factor(l0, l1) + part).astype(BF16)
        mine = pl.ds(pl.multiple_of(y * QROWS, 16), QROWS)
        got["s3"] = []
        for j in range(1, NY):
            to = ymod(y + j)
            got["s3"].append(net.put(msg3.at[to], enter.at[mine], {"sp": z * NY + to}))
        enter[mine] = msg3[y]

    def inside(b, carry):
        at = pl.ds(pl.multiple_of(b * BLOCK, BLOCK), BLOCK)
        t = cols[b]
        c = ctab[b]
        queries[0, at] = conv(3, b).astype(BF16)
        for g in range(2):
            h = 2 * g
            qb, v = queries[g, at], values[g, at]
            scores = dot(qb, keys[g, at], 1, 1)
            weights = []
            for j in range(2):
                span = t[:, h + j : h + j + 1] - c[h + j : h + j + 1]
                weights.append((jnp.exp(jnp.where(causal, span, -jnp.inf)) * scores).astype(BF16))
            zero = jnp.zeros_like(v)
            two = jnp.concatenate([jnp.where(low, v, zero), jnp.where(low, zero, v)], axis=0)
            cum = halves(low, t[:, h : h + 1], t[:, h + 1 : h + 2])
            local[g, at] = dot(jnp.concatenate(weights, axis=1), two, 1, 0) + dot(
                qb, starts[g, b], 1, 0) * jnp.exp(cum)
        return carry

    def inside_a():
        own[8].wait()
        gf[0 : 2 * length] = raw_g[...].astype(F32)
        for g in range(2):
            gates[g] = silu(gf[pl.ds(g, length, stride=2)])
        lax.fori_loop(0, blocks // 2, inside, 0, unroll=2)

    def inside_b():
        lax.fori_loop(blocks // 2, blocks, inside, 0, unroll=2)

    per = blocks // CHUNKS
    tokens = BLOCK * per

    def finish(k):
        need("s3")
        for i in range(per):
            b = k * per + i
            at = slice(b * BLOCK, (b + 1) * BLOCK)
            t = cols[b]
            for g in range(2):
                h = 8 + 2 * g
                if g == 0:
                    entering = enter[0:128]
                else:
                    entering = jnp.concatenate([enter[128:192], jnp.zeros((64, 128), BF16)], axis=0)
                m = local[g, at] + dot(queries[g, at], entering, 1, 0) * halves(
                    low, t[:, h : h + 1], t[:, h + 1 : h + 2])
                m = m * gates[g, at]
                square = m * m
                s0 = jnp.sum(jnp.where(low, square, 0.0), axis=1, keepdims=True)
                s1 = jnp.sum(jnp.where(low, 0.0, square), axis=1, keepdims=True)
                scale = lax.rsqrt(halves(low, s0, s1) * (1.0 / HEAD) + EPSILON)
                mx[k, tp, i, :, g * 128 : (g + 1) * 128] = (
                    m * scale * gain[g : g + 1]).astype(BF16)

    def project(k):
        need("share")
        tp_done("A", k)
        lhs = jnp.concatenate(
            [mx[k, s, odd, :, g * 128 : (g + 1) * 128] for g in range(2) for s in range(NTP)], axis=1)
        base = jnp.concatenate([res[k, odd], rn[0, k], rn[1, k]], axis=1)
        st[k, tp] = (dot(lhs, wo[...], 1, 0) + base.astype(F32)).astype(BF16)

    def stream_of(k, q, xx, cc):
        if xx % 2 == q:
            return st[k, 2 * xx + cc, :, 0:256]
        return jnp.concatenate(
            [st[k, 2 * ((xx - 1) % NX) + cc, :, 256:384], st[k, 2 * ((xx + 1) % NX) + cc, :, 384:512]],
            axis=1)

    def norm(k):
        tp_done("B", k)
        for q in range(2):
            square = jnp.zeros((BLOCK, 128), F32)
            for slot in (2 * q, 2 * q + 1, 2 * q + 4, 2 * q + 5):
                v = st[k, slot].astype(F32)
                for c in range(4):
                    piece = v[:, c * 128 : (c + 1) * 128]
                    square = square + piece * piece
            scale = lax.rsqrt(jnp.sum(square, axis=1, keepdims=True) * (1.0 / depth) + EPSILON)
            for slot in range(NTP):
                cut = slice(slot * 256, (slot + 1) * 256)
                v = stream_of(k, q, slot // 2, slot % 2).astype(F32)
                nb[k, q * BLOCK : (q + 1) * BLOCK, cut] = (v * scale * channel_gain[:, cut]).astype(BF16)

    def hidden_units(k):
        for j in (0, 1, -1, 2, -2, 3, -3, 4):
            need("gr", j)
        for c in range(NY):
            need("uz", c, 4)
        pair = dot(nb[k], gu[...].reshape(depth, 2 * width), 1, 0)
        hidden[k] = (silu(pair[:, :width]) * pair[:, width:]).astype(BF16)

    order = (2, 3, 1, 0)
    dests = {k: lax.rem(x + k, NX) * 2 for k in order}

    def down(k, d):
        return dot(hidden[k], dn[d].reshape(256, width), 1, 1).astype(BF16)

    def down_partner(k):
        need("dr", 0)
        need("dr", 1)
        need("ez", 4)
        for j in order:
            ps[k, j] = down(k, dests[j] + 1 - core)
        for j in order:
            got["P", k, j] = net.put(ps.at[k, j], pr.at[k, j], partner)

    def down_own(k):
        for j in order:
            po[k, j] = down(k, dests[j] + core)

    def pair_sum(k, j):
        got["P", k, j].wait_recv()
        return po[k, j].astype(F32) + pr[k, j].astype(F32)

    mid = tokens // 2
    outs = []

    def sum_first(k):
        qs[k, 2] = pair_sum(k, 2).astype(BF16)
        got["C1", k] = (net.put(qs.at[k, 2, 0:mid], relay_r.at[k], x_left),
                        net.put(qs.at[k, 2, mid:], relay_l.at[k], x_right))

    def sum_second(k):
        to_left, to_right = pair_sum(k, 3), pair_sum(k, 1)
        arrive(got["C1", k])
        qs[k, 3, 0:mid] = (to_left[0:mid] + relay_r[k].astype(F32)).astype(BF16)
        qs[k, 3, mid:] = to_left[mid:].astype(BF16)
        qs[k, 1, 0:mid] = to_right[0:mid].astype(BF16)
        qs[k, 1, mid:] = (to_right[mid:] + relay_l[k].astype(F32)).astype(BF16)
        got["C2", k] = (net.put(qs.at[k, 3], from_r.at[k], x_left),
                        net.put(qs.at[k, 1], from_l.at[k], x_right))

    def sum_third(k):
        total = pair_sum(k, 0)
        arrive(got["C2", k])
        total = total + from_l[k].astype(F32) + from_r[k].astype(F32)
        mine = st[k, tp, :, 0:256].astype(F32)
        other = jnp.concatenate(
            [st[k, slot_l, :, 256:384], st[k, slot_r, :, 384:512]], axis=1).astype(F32)
        for q in range(2):
            at = k * tokens + q * BLOCK
            stream = jnp.where(odd == q, mine, other)
            out[at : at + BLOCK] = (
                stream + 0.5 * total[q * BLOCK : (q + 1) * BLOCK]).astype(BF16)
        rows = pl.ds(k * tokens, tokens)
        copy = pltpu.make_async_copy(out.at[rows], hbm_out.at[rows], local_sem.at[19 + k])
        copy.start()
        outs.append(copy)

    run = {
        "tables": tables,
        "spread": spread,
        "bA": lambda: run_blocks(1, 5),
        "bB": lambda: run_blocks(5, 7),
        "b0": last_block,
        "s1": stage1,
        "s2": stage2,
        "s3": stage3,
        "ia": inside_a,
        "ib": inside_b,
        "gy0": lambda: gate_y(0),
        "gy1": lambda: gate_y(1, -1),
        "gy2": lambda: gate_y(2, -2),
        "gy3": lambda: gate_y(3, -3),
        "gy4": lambda: gate_y(4),
        "uy1": lambda: up_y(1),
        "uy2": lambda: up_y(2),
        "dy0": lambda: down_y(0),
        "dy1": lambda: down_y(1),
        "ey1": lambda: rest_y(1),
        "ey2": lambda: rest_y(2),
        "dr0": lambda: down_relay(0),
        "dr1": lambda: down_relay(1),
        "share": share,
    }
    for r in (1, 2, 3, 4):
        run[f"gz{r}"] = functools.partial(gate_z, r)
        for c in range(NY):
            run[f"u{c}{r}"] = functools.partial(up_z, c, r)
        run[f"dz{r}"] = functools.partial(down_z, r)
        run[f"ez{r}"] = functools.partial(rest_z, r)
    for k in (0, 1, -1, 2, -2, 3, -3, 4):
        run[f"gr{k}"] = functools.partial(gate_relay, k)
    for k in range(CHUNKS):
        run[f"fin{k}"] = functools.partial(finish, k)
        run[f"P{k}"] = functools.partial(project, k)
        run[f"N{k}"] = functools.partial(norm, k)
        run[f"H{k}"] = functools.partial(hidden_units, k)
        run[f"D{k}"] = functools.partial(down_partner, k)
        run[f"E{k}"] = functools.partial(down_own, k)
        run[f"C1{k}"] = functools.partial(sum_first, k)
        run[f"C2{k}"] = functools.partial(sum_second, k)
        run[f"C3{k}"] = functools.partial(sum_third, k)
        run[f"Ai{k}"] = functools.partial(mix_first, k)
        run[f"Ar{k}"] = functools.partial(mix_second, k)
        run[f"Af{k}"] = functools.partial(mix_third, k)
        run[f"Bi{k}"] = functools.partial(tp_first, st, "B", k)
        run[f"Br{k}"] = functools.partial(tp_second, st, "B", k)
        run[f"Bf{k}"] = functools.partial(tp_third, st, "B", k)
    for name in STEPS:
        mark(name)
        run.pop(name)()
    assert not run

    mark("sends")
    for copy in outs:
        copy.wait()
    for copy in net.sent:
        copy.wait_send()


def layer(small_args, hbm_args):
    length = hbm_args[2].shape[0]
    blocks = length // BLOCK
    tokens = length // CHUNKS
    width = hbm_args[8].shape[1]
    hbm = pl.BlockSpec(memory_space=pl.ANY)
    dma = pltpu.SemaphoreType.DMA

    def bf(*shape):
        return pltpu.VMEM(shape, BF16)

    def fl(*shape):
        return pltpu.VMEM(shape, F32)

    return pl.pallas_call(
        layer_kernel,
        out_shape=jax.ShapeDtypeStruct((length, 256), BF16),
        in_specs=[hbm] * (len(small_args) + len(hbm_args)),
        out_specs=hbm,
        scratch_shapes=[fl(*a.shape) for a in small_args]
        + [
            bf(length, 256),
            bf(2 * length, 128), bf(2 * length, 128), bf(length, 128), bf(length, 128),
            bf(128, length), fl(2 * length + 16, 128), fl(2 * length + 16, 128), fl(5, length + 8, 128),
            bf(16, 128), bf(16, 128), bf(16, 128), bf(128, 128),
            fl(blocks, 8, 128), fl(blocks, BLOCK, 16),
            bf(2, length, 128), bf(2, length, 128), bf(2, length, 128),
            fl(2, length, 128), fl(2, length, 128),
            fl(2, blocks, 128, 128), bf(2, blocks, 128, 128),
            bf(NY, MROWS, 128), bf(NY, MROWS, 128), bf(MROWS, 128), bf(NZ, MROWS, 128),
            bf(NY, QROWS, 128), bf(NY * QROWS, 128),
            bf(NZ, NY, 64, 2 * width), bf(NZ, NY, 64, width), bf(2048, 512),
            bf(CHUNKS, 2, BLOCK, 256), bf(2, CHUNKS, BLOCK, 128),
            bf(CHUNKS, NTP, 2, BLOCK, 256), bf(CHUNKS, NTP, BLOCK, 512),
            bf(CHUNKS, tokens, 2048), bf(CHUNKS, tokens, width),
            bf(CHUNKS, NX, tokens, 256), bf(CHUNKS, NX, tokens, 256), bf(CHUNKS, NX, tokens, 256),
            bf(CHUNKS, tokens // 2, 256), bf(CHUNKS, tokens // 2, 256),
            bf(CHUNKS, NX, tokens, 256), bf(CHUNKS, tokens, 256), bf(CHUNKS, tokens, 256),
            dma((19 + CHUNKS,)), dma((N_PUT,)), dma((N_PUT,)),
        ],
        compiler_params=pltpu.CompilerParams(
            collective_id=0, has_side_effects=True, vmem_limit_bytes=58 * 1024 * 1024),
        cost_estimate=pl.CostEstimate(
            flops=12_000_000_000, bytes_accessed=8_000_000, transcendentals=4_000_000),
        name="layer",
    )(*small_args, *hbm_args)


def shards(
    grouped_head_inputs,
    head_gate_inputs,
    unsmoothed_step,
    head_decay_rate,
    extra_log_decay,
    first_group_keys,
    first_group_queries,
    second_group_keys,
    second_group_queries,
    head_input_filter,
    first_group_filter,
    second_group_filter,
    head_norm_gain,
    output_weight,
    residual,
    channel_norm_gain,
    channel_gate_weight,
    channel_up_weight,
    channel_down_weight,
):
    length = grouped_head_inputs.shape[0]
    return layer(
        (
            unsmoothed_step.transpose(1, 2, 0),
            extra_log_decay.transpose(1, 2, 0),
            head_input_filter,
            first_group_filter,
            second_group_filter,
            head_norm_gain,
            channel_norm_gain[None],
            head_decay_rate,
        ),
        (
            grouped_head_inputs.reshape(2 * length, 128),
            head_gate_inputs.reshape(2 * length, 128),
            first_group_keys,
            first_group_queries,
            second_group_keys.T,
            second_group_queries.T,
            output_weight.reshape(-1, output_weight.shape[2]),
            residual.reshape(CHUNKS, 2, BLOCK, residual.shape[1]),
            channel_gate_weight,
            channel_up_weight,
            channel_down_weight,
        ),
    )


def solution(mesh):
    return jax.shard_map(
        shards,
        mesh=mesh,
        in_specs=(
            P("sp", None, "tp"),
            P("sp", None, "tp"),
            P("sp", None, "tp"),
            P(None, "tp"),
            P("sp", None, "tp"),
            P("sp", None),
            P("sp", None),
            P("sp", None),
            P("sp", None),
            P(None, None, "tp"),
            P(),
            P(),
            P(None, "tp"),
            P(None, None, "tp"),
            P("sp", "tp"),
            P(),
            P("sp", "tp"),
            P("sp", "tp"),
            P("sp", "tp"),
        ),
        out_specs=P("sp", "tp"),
        check_vma=False,
    )
```
